32 devices in a mesh: rep: 4 (over z), fs: 4 (over y, x), tp: 2 (over core).
Axes of the slice: x: 2, y: 2, z: 4, core: 2. Of those that a mesh axis runs over, the one named last changes fastest.
Arguments:
- residual: bfloat16 [16, 256, 2048], P(('rep', 'fs'), None, 'tp'), may hold values from -6 to 6
- queries: bfloat16 [16, 256, 2048], P(('rep', 'fs'), None, 'tp'), may hold values from -6 to 6
- key_matrix: bfloat16 [16, 256, 2048], P(('rep', 'fs'), None, 'tp'), may hold values from -6 to 6
- value_matrix: bfloat16 [16, 256, 2048], P(('rep', 'fs'), None, 'tp'), may hold values from -6 to 6
- decay_logodds: float32 [16, 256, 2048], P(('rep', 'fs'), None, 'tp'), may hold values from -3.4 to 8.9, as said below
- decay_surge: float32 [16, 256, 8], P(('rep', 'fs'), None, 'tp'), may hold values from -2.1 to 0, as said below
- head_norm_gain: float32 [256], replicated, may hold values from 0.1 to 1.9
- output_matrix: float32 [2048, 2048], P('fs', 'tp'), may hold values from -0.125 to 0.125
- output_column_scale: float32 [2048], P('tp'), may hold values from 0.5 to 2
- premix_norm_gain: float32 [2048], replicated, may hold values from 0.1 to 1.9
- gate_matrix: float32 [2048, 2816], P('fs', 'tp'), may hold values from -0.125 to 0.125
- gate_column_scale: float32 [2816], P('tp'), may hold values from 0.5 to 2
- up_matrix: float32 [2048, 2816], P('fs', 'tp'), may hold values from -0.125 to 0.125
- up_column_scale: float32 [2816], P('tp'), may hold values from 0.5 to 2
- down_matrix: float32 [2048, 2816], P('fs', 'tp'), may hold values from -0.109375 to 0.109375
- down_column_scale: float32 [2048], P('tp'), may hold values from 0.5 to 2
Outputs:
- layer_out: bfloat16 [16, 256, 2048], P(('rep', 'fs'), None, 'tp')
The draws below stay inside these ranges and needn't reach their ends.
Inputs may be any that keep to these rules, and one draw needn't show every extreme that they name: `decay_logodds`: log-odds of a key channel's decay. `decay_surge`: non-positive log-factors of a head's state.
All inputs are finite; a program needn't handle non-finite values.
Results may differ from the reference program's by a relative error of at most 0.018.
Values may be sent and summed in bfloat16 or wider, within the bound.
A program may use at most 128 MiB of HBM per device.

```python
import math
import jax
import jax.numpy as jnp
from jax import lax

D = 2048
HEAD_NUMBER = 8
HEAD_V = 256
FF = 2816
BLOCK = 64
SEQUENCE_LENGTH = 256
KEY_DIM = 2048
VALUE_DIM = 2048
BATCH_SIZE = 16
N_TP = 2


def draw_decay_logodds(key, part):
    residual_flows = jax.random.split(jax.random.fold_in(key, 11), 5)
    slow_share = 0.5
    jitter = jnp.clip(0.7 * jax.random.normal(residual_flows[4], (BATCH_SIZE, SEQUENCE_LENGTH, KEY_DIM), jnp.float32), -2.8, 2.8)
    slow_mask = jax.random.uniform(residual_flows[0], (KEY_DIM,), jnp.float32) < slow_share
    slow_base = jax.random.uniform(residual_flows[1], (KEY_DIM,), jnp.float32, 3.5, 5.5)
    fast_base = jax.random.uniform(residual_flows[2], (KEY_DIM,), jnp.float32, 0.0, 1.2)
    offset = jax.random.uniform(residual_flows[3], (BATCH_SIZE, 1, 1), jnp.float32, -0.6, 0.6)
    return jnp.where(slow_mask, slow_base, fast_base) + offset + jitter


def draw_decay_surge(key, part):
    residual_flows = jax.random.split(jax.random.fold_in(key, 23), 2)
    surge_position = jax.random.randint(residual_flows[0], (BATCH_SIZE, 3, HEAD_NUMBER), 0, SEQUENCE_LENGTH)
    strength = jnp.log(jax.random.uniform(residual_flows[1], (BATCH_SIZE, 3, HEAD_NUMBER), jnp.float32, 0.5, 0.8))
    match_scores = jnp.arange(SEQUENCE_LENGTH)[None, :, None, None] == surge_position[:, None, :, :]
    return jnp.sum(jnp.where(match_scores, strength[:, None, :, :], 0.0), axis=2)


def block_levels(own_key, shape, cuts, low, top_value):
    def one(position, shards_of):
        draws = jax.random.uniform(jax.random.fold_in(jax.random.fold_in(own_key, 6), position), (shards_of,), jnp.float32, low / len(cuts), top_value / len(cuts))
        return jnp.repeat(jnp.exp(draws), shape[position] // shards_of).reshape((-1,) + (1,) * (len(shape) - position - 1))

    loudness = one(*cuts[0])
    for cut in cuts[1:]:
        loudness = loudness * one(*cut)
    return loudness


def gaussian(stream_key, dims, scale, bound, cuts=(), kind=jnp.bfloat16):
    values = jax.random.normal(stream_key, dims, jnp.float32) * scale
    if len(cuts) > 0:
        values = block_levels(stream_key, dims, cuts, -0.22, 0.18) * values
    return jnp.clip(values, min=-bound, max=bound).astype(kind)


def setup_inputs(seed: int = 0) -> dict:
    arg_keys = jax.random.split(jax.random.key(seed), 17)
    return {
        "residual": gaussian(arg_keys[0], (BATCH_SIZE, SEQUENCE_LENGTH, D), 1.0, 6.0, ((0, 16), (2, 2))),
        "queries": gaussian(arg_keys[1], (BATCH_SIZE, SEQUENCE_LENGTH, KEY_DIM), 1.0, 6.0, ((0, 16), (2, 2))),
        "key_matrix": gaussian(arg_keys[2], (BATCH_SIZE, SEQUENCE_LENGTH, KEY_DIM), 1.0, 6.0, ((0, 16), (2, 2))),
        "value_matrix": gaussian(arg_keys[3], (BATCH_SIZE, SEQUENCE_LENGTH, VALUE_DIM), 1.0, 6.0, ((0, 16), (2, 2))),
        "decay_logodds": draw_decay_logodds(jax.random.fold_in(arg_keys[16], 71), 0),
        "decay_surge": draw_decay_surge(jax.random.fold_in(arg_keys[16], 71), 0),
        "head_norm_gain": jnp.clip(1.0 + 0.18 * jax.random.normal(arg_keys[6], (HEAD_V,), jnp.float32), 0.1, 1.9),
        "output_matrix": gaussian(arg_keys[7], (D, VALUE_DIM), VALUE_DIM ** -0.5, 0.125, ((0, 4), (1, 2)), jnp.float32),
        "output_column_scale": jnp.clip(jnp.exp(math.log(2.0) - 1.3862944 * jax.random.uniform(arg_keys[8], (D,), jnp.float32) ** block_levels(arg_keys[8], (D,), ((0, 2),), -0.2, 0.2)), 0.5, 2.0),
        "premix_norm_gain": jnp.clip(1.0 + 0.18 * jax.random.normal(arg_keys[9], (D,), jnp.float32), 0.1, 1.9),
        "gate_matrix": gaussian(arg_keys[10], (D, FF), D ** -0.5, 0.125, ((0, 4), (1, 2)), jnp.float32),
        "gate_column_scale": jnp.clip(jnp.exp(math.log(2.0) - 1.3862944 * jax.random.uniform(arg_keys[11], (FF,), jnp.float32) ** block_levels(arg_keys[11], (FF,), ((0, 2),), -0.2, 0.2)), 0.5, 2.0),
        "up_matrix": gaussian(arg_keys[12], (D, FF), D ** -0.5, 0.125, ((0, 4), (1, 2)), jnp.float32),
        "up_column_scale": jnp.clip(jnp.exp(math.log(2.0) - 1.3862944 * jax.random.uniform(arg_keys[13], (FF,), jnp.float32) ** block_levels(arg_keys[13], (FF,), ((0, 2),), -0.2, 0.2)), 0.5, 2.0),
        "down_matrix": gaussian(arg_keys[14], (D, FF), FF ** -0.5, 0.109375, ((0, 4), (1, 2)), jnp.float32),
        "down_column_scale": jnp.clip(jnp.exp(math.log(2.0) - 1.3862944 * jax.random.uniform(arg_keys[15], (D,), jnp.float32) ** block_levels(arg_keys[15], (D,), ((0, 2),), -0.2, 0.2)), 0.5, 2.0),
    }


epsilon = 1e-06
softness_factor = 16.0
highest = lax.Precision.HIGHEST

def one_direction(query_heads, key_heads, value_heads, log_decay_values):
    sequence_batch, head_total, token_length, key_channel_width = query_heads.shape
    value_width = value_heads.shape[-1]
    block_count = token_length // BLOCK

    def blocks(tensor):
        return tensor.reshape(sequence_batch, head_total, block_count, BLOCK, tensor.shape[-1])
    q_blocks = blocks(query_heads)
    k_blocks = blocks(key_heads)
    v_blocks = blocks(value_heads)
    running = jnp.cumsum(blocks(log_decay_values), axis=3)
    block_end = running[:, :, :, -1:, :]
    q_dec = q_blocks * jnp.exp(running)
    k_inv = k_blocks * jnp.exp(-running)
    k_end = k_blocks * jnp.exp(block_end - running)
    lower_mask = jnp.tril(jnp.ones((BLOCK, BLOCK), jnp.float32))
    scores = jnp.einsum('shnid,shnjd->shnij', q_dec, k_inv, precision=highest) * lower_mask
    inner_part = jnp.einsum('shnij,shnje->shnie', scores, v_blocks, precision=highest)
    fading = jnp.exp(block_end[:, :, :, 0, :])

    def advance(memory, pieces):
        q_piece, k_piece, v_piece, f_piece = pieces
        carried = jnp.einsum('shcd,shde->shce', q_piece, memory, precision=highest)
        memory = f_piece[..., None] * memory + jnp.einsum('shcd,shce->shde', k_piece, v_piece, precision=highest)
        return (memory, carried)
    pieces = tuple((jnp.moveaxis(tensor, 2, 0) for tensor in (q_dec, k_end, v_blocks, fading)))
    initial = jnp.zeros((sequence_batch, head_total, key_channel_width, value_width), jnp.float32)
    _, carried = lax.scan(advance, initial, pieces)
    summed = inner_part + jnp.moveaxis(carried, 0, 2)
    return summed.reshape(sequence_batch, head_total, token_length, value_width)

def backwards(tensor):
    return tensor[:, :, ::-1]

def linear_attend(queries, key_matrix, value_matrix, decay_logodds, decay_surge, head_norm_gain):
    sequence_batch, token_length, head_total = decay_surge.shape
    key_channel_width = queries.shape[-1] // head_total
    value_width = value_matrix.shape[-1] // head_total

    def split_heads(tensor, width):
        return jnp.transpose(tensor.astype(jnp.float32).reshape(sequence_batch, token_length, head_total, width), (0, 2, 1, 3))
    query_heads = split_heads(queries, key_channel_width) * key_channel_width ** (-0.5)
    key_heads = split_heads(key_matrix, key_channel_width)
    value_heads = split_heads(value_matrix, value_width)
    gate_values = jax.nn.log_sigmoid(decay_logodds).reshape(sequence_batch, token_length, head_total, key_channel_width) / softness_factor
    log_decay_values = jnp.transpose(gate_values + decay_surge[..., None], (0, 2, 1, 3))
    forward = one_direction(query_heads, key_heads, value_heads, log_decay_values)
    backward = backwards(one_direction(backwards(query_heads), backwards(key_heads), backwards(value_heads), backwards(log_decay_values)))
    attended = forward + backward
    scaled = attended * lax.rsqrt(lax.optimization_barrier(jnp.mean(attended * attended, axis=-1, keepdims=True)) + epsilon) * head_norm_gain
    merged = jnp.transpose(scaled, (0, 2, 1, 3)).reshape(sequence_batch * token_length, head_total * value_width)
    return merged.astype(jnp.bfloat16)

def grouped(left, right):
    width = left.shape[1] // N_TP
    left_parts = left.reshape(left.shape[0], N_TP, width).astype(jnp.float32)
    right_parts = right.reshape(right.shape[0], N_TP, width).astype(jnp.float32)
    terms = jnp.einsum('lgc,dgc->gld', left_parts, right_parts, precision=highest)
    rounded = lax.optimization_barrier(terms.astype(jnp.bfloat16))
    return lax.optimization_barrier(jnp.sum(rounded.astype(jnp.float32), axis=0))

def rms_scaled(rows_in, gain):
    wide_rows = rows_in.astype(jnp.float32)
    factor = lax.rsqrt(lax.optimization_barrier(jnp.mean(wide_rows * wide_rows, axis=-1, keepdims=True)) + epsilon)
    return (wide_rows * factor * gain).astype(jnp.bfloat16)

def reference(residual, queries, key_matrix, value_matrix, decay_logodds, decay_surge, head_norm_gain, output_matrix, output_column_scale, premix_norm_gain, gate_matrix, gate_column_scale, up_matrix, up_column_scale, down_matrix, down_column_scale):
    out_half = output_matrix.astype(jnp.bfloat16)
    gate_half = gate_matrix.astype(jnp.bfloat16)
    up_half = up_matrix.astype(jnp.bfloat16)
    down_half = down_matrix.astype(jnp.bfloat16)

    def single_sequence(input_rows):
        residual_sequence, query_sequence, key_sequence, value_sequence, logodds_sequence, surge_sequence = input_rows
        normalized_rows = linear_attend(query_sequence[None], key_sequence[None], value_sequence[None], logodds_sequence[None], surge_sequence[None], head_norm_gain)
        mix_total = grouped(normalized_rows, out_half)
        updated = (residual_sequence.astype(jnp.float32) + output_column_scale * mix_total).astype(jnp.bfloat16)
        normin = rms_scaled(updated, premix_norm_gain)
        gate_pre = jnp.dot(normin, gate_half, preferred_element_type=jnp.float32) * gate_column_scale
        up_pre = jnp.dot(normin, up_half, preferred_element_type=jnp.float32) * up_column_scale
        hidden = (jax.nn.silu(gate_pre) * up_pre).astype(jnp.bfloat16)
        down_total = grouped(hidden, down_half)
        return (updated.astype(jnp.float32) + down_column_scale * down_total).astype(jnp.bfloat16)
    return lax.map(single_sequence, (residual, queries, key_matrix, value_matrix, decay_logodds, decay_surge))
```

```python
import functools

import jax
import jax.numpy as jnp
from jax import lax
from jax.experimental import pallas as pl
from jax.experimental.pallas import tpu as pltpu
from jax.sharding import PartitionSpec as P

BLOCK = 64


epsilon = 1e-06
softness_factor = 16.0
highest = lax.Precision.HIGHEST


def attend_head(q, k, v, logodds, surge, gain):
    tokens, width = q.shape
    blocks = tokens // BLOCK
    mid = BLOCK // 2 - 1
    decay = (
        jnp.minimum(logodds, 0.0) - jnp.log1p(jnp.exp(-jnp.abs(logodds)))
    ) * (1.0 / softness_factor) + surge
    row = lax.broadcasted_iota(jnp.int32, (BLOCK, BLOCK), 0)
    col = lax.broadcasted_iota(jnp.int32, (BLOCK, BLOCK), 1)
    tri = jnp.where(row >= col, 1.0, 0.0).astype(jnp.bfloat16)
    q = q.astype(jnp.float32) * width ** (-0.5)
    k = k.astype(jnp.float32)
    high = decay.astype(jnp.bfloat16)
    low = (decay - high.astype(jnp.float32)).astype(jnp.bfloat16)
    pieces = []
    for n in range(blocks):
        rows = slice(n * BLOCK, (n + 1) * BLOCK)
        running = jnp.dot(tri, high[rows], preferred_element_type=jnp.float32) + jnp.dot(
            tri, low[rows], preferred_element_type=jnp.float32
        )
        before = running - decay[rows]
        center = running[mid : mid + 1]
        end = running[BLOCK - 1 : BLOCK]
        to_center = jnp.exp(center)
        from_center = jnp.exp(end - center)
        q_forward = q[rows] * jnp.exp(running - center)
        k_forward = k[rows] * jnp.exp(center - running)
        q_backward = q[rows] * jnp.exp(center - before)
        k_backward = k[rows] * jnp.exp(before - center)
        half = jnp.bfloat16
        scores = jnp.where(
            row >= col, by_rows(q_forward.astype(half), k_forward.astype(half)), 0.0
        ) + jnp.where(row <= col, by_rows(q_backward.astype(half), k_backward.astype(half)), 0.0)
        inner = jnp.dot(scores.astype(half), v[rows], preferred_element_type=jnp.float32)
        pieces.append(
            (
                inner,
                (q_forward * to_center).astype(half),
                (q_backward * from_center).astype(half),
                by_columns(v[rows], (k_forward * from_center).astype(half)),
                by_columns(v[rows], (k_backward * to_center).astype(half)),
                jnp.exp(end),
            )
        )
    totals = [piece[0] for piece in pieces]
    state = None
    for n in range(blocks):
        if state is not None:
            totals[n] = totals[n] + by_rows(pieces[n][1], state.astype(jnp.bfloat16))
        state = pieces[n][3] if state is None else pieces[n][5] * state + pieces[n][3]
    state = None
    for n in reversed(range(blocks)):
        if state is not None:
            totals[n] = totals[n] + by_rows(pieces[n][2], state.astype(jnp.bfloat16))
        state = pieces[n][4] if state is None else pieces[n][5] * state + pieces[n][4]
    attended = jnp.concatenate(totals, axis=0)
    scale = lax.rsqrt(jnp.mean(attended * attended, axis=-1, keepdims=True) + epsilon)
    return (attended * scale * gain).astype(jnp.bfloat16)


def by_columns(left, right):
    return lax.dot_general(
        left, right, (((0,), (0,)), ((), ())), preferred_element_type=jnp.float32
    )


def attend_kernel(head_total, q_ref, k_ref, v_ref, lo_ref, sg_ref, gain_ref, out_ref):
    width = q_ref.shape[1] // head_total
    value_width = v_ref.shape[1] // head_total
    for h in range(head_total):
        keys = slice(h * width, (h + 1) * width)
        values = slice(h * value_width, (h + 1) * value_width)
        out_ref[:, values] = attend_head(
            q_ref[:, keys],
            k_ref[:, keys],
            v_ref[:, values],
            lo_ref[:, keys],
            sg_ref[:, h : h + 1],
            gain_ref[...],
        )


def linear_attend(queries, key_matrix, value_matrix, decay_logodds, decay_surge, head_norm_gain):
    _, token_length, head_total = decay_surge.shape
    outs = [
        pl.pallas_call(
            functools.partial(attend_kernel, head_total),
            out_shape=jax.ShapeDtypeStruct(value_matrix.shape[1:], jnp.bfloat16),
            in_specs=[pl.BlockSpec(memory_space=pltpu.VMEM)] * 6,
            out_specs=pl.BlockSpec(memory_space=pltpu.VMEM),
            cost_estimate=pl.CostEstimate(
                flops=10**9, bytes_accessed=4 * 10**6, transcendentals=10**6
            ),
        )(
            queries[b], key_matrix[b], value_matrix[b], decay_logodds[b], decay_surge[b],
            head_norm_gain.reshape(1, -1),
        )
        for b in range(queries.shape[0])
    ]
    return jnp.concatenate(outs, axis=0)


def by_rows(left, right):
    return lax.dot_general(
        left, right, (((1,), (1,)), ((), ())), preferred_element_type=jnp.float32
    )


def body(
    residual,
    queries,
    key_matrix,
    value_matrix,
    decay_logodds,
    decay_surge,
    head_norm_gain,
    output_matrix,
    output_column_scale,
    premix_norm_gain,
    gate_matrix,
    gate_column_scale,
    up_matrix,
    up_column_scale,
    down_matrix,
    down_column_scale,
):
    sequence_batch, token_length, local_width = residual.shape
    row_count = sequence_batch * token_length
    normalized_rows = linear_attend(
        queries, key_matrix, value_matrix, decay_logodds, decay_surge, head_norm_gain
    )
    out_half = output_matrix.astype(jnp.bfloat16)
    out_full = lax.all_gather(out_half, "fs", axis=0, tiled=True)
    mix_terms = by_rows(normalized_rows, out_full)
    mix_total = lax.psum_scatter(
        mix_terms.astype(jnp.bfloat16), "tp", scatter_dimension=1, tiled=True
    ).astype(jnp.float32)
    own_rows = residual.reshape(row_count, local_width).astype(jnp.float32)
    updated = (own_rows + output_column_scale * mix_total).astype(jnp.bfloat16)
    features = lax.all_gather(updated, "tp", axis=1, tiled=True)
    wide_rows = features.astype(jnp.float32)
    factor = lax.rsqrt(jnp.mean(wide_rows * wide_rows, axis=-1, keepdims=True) + epsilon)
    normin = (wide_rows * factor * premix_norm_gain).astype(jnp.bfloat16)
    gate_half = gate_matrix.astype(jnp.bfloat16)
    up_half = up_matrix.astype(jnp.bfloat16)
    down_half = down_matrix.astype(jnp.bfloat16)
    gate_full, up_full, down_full = (
        lax.all_gather(gate_half, "fs", axis=0, tiled=True),
        lax.all_gather(up_half, "fs", axis=0, tiled=True),
        lax.all_gather(down_half, "fs", axis=0, tiled=True),
    )
    gate_pre = jnp.dot(normin, gate_full, preferred_element_type=jnp.float32)
    up_pre = jnp.dot(normin, up_full, preferred_element_type=jnp.float32)
    hidden = (jax.nn.silu(gate_pre * gate_column_scale) * (up_pre * up_column_scale)).astype(
        jnp.bfloat16
    )
    down_terms = by_rows(hidden, down_full)
    down_total = lax.psum_scatter(
        down_terms.astype(jnp.bfloat16), "tp", scatter_dimension=1, tiled=True
    ).astype(jnp.float32)
    result = (updated.astype(jnp.float32) + down_column_scale * down_total).astype(jnp.bfloat16)
    return result.reshape(sequence_batch, token_length, local_width)


def layer_kernel(
    q_hbm, k_hbm, v_hbm, lo_hbm, res_hbm, wo_hbm, gate_hbm, up_hbm, down_hbm,
    sg_ref, head_gain_ref, mlp_gain_ref, os_ref, gs_ref, us_ref, ds_ref,
    out_ref,
    q_v, k_v, v_v, lo_v, res_v, wo_f32, wo_half, wo_all,
    stage, own_f32, own_half, blocks, weights,
    normed, gathered, own_res, updated,
    os_all, gs_all, us_all, ds_all,
    own_down, to_p, to_p2, to_q, from_p, from_p2, from_q, result,
    load_sem, send_sem, recv_sem,
):
    r, f, t = lax.axis_index("rep"), lax.axis_index("fs"), lax.axis_index("tp")
    half = jnp.bfloat16
    x, y, c = f + 1 - 2 * lax.rem(f, 2), lax.rem(f + 2, 4), 3 - f
    p, q = x + t * (y - x), y + t * (x - y)
    fs_of = (f, x, y, c)
    m = lax.rem(r, 3)
    others = (lax.rem(m + 1, 3), lax.rem(m + 2, 3))
    mats = (gate_hbm, up_hbm, down_hbm)
    tokens, local_width = res_v.shape
    rows = tokens // 2
    own_width, total_units = stage.shape
    units = blocks.shape[2]
    part_rows = own_width // 2
    width = updated.shape[2]
    heads = sg_ref.shape[1]
    head_width = local_width // heads
    starts = [min(j * units, total_units - units) for j in range(4)]

    def lanes(start, size):
        return pl.ds(pl.multiple_of(start, 128), size)

    own_start = jnp.minimum(f * units, total_units - units)
    own_spill = f * units - own_start
    own_lanes = lanes(own_start, units)

    A, RES, CO, CX, CC = 0, 6, 10, 14, 30
    WO, SC, EP, EQ, EC, ZN, DN, FP, OUT = 38, 39, 43, 47, 51, 55, 73, 97, 103

    local_count = [0]
    waits = []

    def load(source, target):
        index = local_count[0]
        local_count[0] += 1
        copy = pltpu.make_async_copy(source, target, load_sem.at[index])
        return copy

    send_count = [0]
    sent = []

    def send(source, target, slot, device, when=None):
        index = send_count[0]
        send_count[0] += 1
        copy = pltpu.make_async_remote_copy(
            src_ref=source,
            dst_ref=target,
            send_sem=send_sem.at[index],
            recv_sem=recv_sem.at[slot],
            device_id=device,
            device_id_type=pl.DeviceIdType.MESH,
        )
        if when is None:
            copy.start()
        else:
            pl.when(when)(copy.start)
        sent.append((copy, when))

    def arrive(target, slot):
        pltpu.make_async_remote_copy(
            src_ref=target,
            dst_ref=target,
            send_sem=send_sem.at[0],
            recv_sem=recv_sem.at[slot],
            device_id=(r, f, 1 - t),
            device_id_type=pl.DeviceIdType.MESH,
        ).wait_recv()

    def part(n):
        return pl.ds(n * part_rows, part_rows)

    stage_loads = []
    for n in range(2):
        index = local_count[0]
        local_count[0] += 1
        for mm in range(3):
            @pl.when(m == mm)
            def _(mm=mm, n=n, index=index):
                pltpu.make_async_copy(
                    mats[mm].at[part(n)], stage.at[part(n)], load_sem.at[index]
                ).start()
        stage_loads.append(
            pltpu.make_async_copy(gate_hbm.at[part(n)], stage.at[part(n)], load_sem.at[index])
        )
    res_load = load(res_hbm, res_v)
    res_load.start()
    head_loads = []
    for h in range(heads):
        keys = slice(h * head_width, (h + 1) * head_width)
        loads = [
            load(a.at[:, keys], b.at[:, keys])
            for a, b in ((lo_hbm, lo_v), (q_hbm, q_v), (k_hbm, k_v), (v_hbm, v_v))
        ]
        for copy in loads:
            copy.start()
        head_loads.append(loads)
    wo_load = load(wo_hbm, wo_f32)
    wo_load.start()
    own_loads = []
    for n in range(2):
        index = local_count[0]
        local_count[0] += 1
        for mm in range(3):
            @pl.when(m == mm)
            def _(mm=mm, n=n, index=index):
                pltpu.make_async_copy(
                    mats[(mm + 1 + n) % 3].at[:, own_lanes], own_f32.at[n], load_sem.at[index]
                ).start()
        own_loads.append(
            pltpu.make_async_copy(gate_hbm.at[:, own_lanes], own_f32.at[n], load_sem.at[index])
        )

    partner = (r, f, 1 - t)
    peers = [partner]
    for other in (x, y, c):
        peers += [(r, other, 0), (r, other, 1)]
    peers += [(lax.rem(r + step, 4), f, t) for step in range(1, 4)]
    greet(peers)

    def weight_at(matrix, owner, n, core):
        return weights.at[
            matrix,
            pl.ds(owner * own_width + n * part_rows, part_rows),
            lanes(core * units, units),
        ]

    lane = lax.broadcasted_iota(jnp.int32, (part_rows, units), 1)
    for n in range(2):
        stage_loads[n].wait()
        span = slice(n * part_rows, (n + 1) * part_rows)
        for j in range(4):
            cut = stage[span, starts[j] : starts[j] + units]
            spill = j * units - starts[j]
            if spill > 0:
                cut = jnp.where((lane < spill) & (m == 2), 0.0, cut)
            blocks[j, span, :] = cut.astype(half)
        for rel in (1, 2, 3):
            send(
                blocks.at[fs_of[rel], part(n)], weight_at(m, f, n, t), A + n * 3 + rel - 1,
                (r, fs_of[rel], t),
            )
    own_copies = []
    for n in range(2):
        copy = load(blocks.at[f, part(n)], weight_at(m, f, n, t))
        copy.start()
        own_copies.append(copy)
        send(blocks.at[f, part(n)], weight_at(m, f, n, t), DN + m * 8 + n, partner)

    for n, (ref, both) in enumerate(
        ((os_ref, os_all), (gs_ref, gs_all), (us_ref, us_all), (ds_ref, ds_all))
    ):
        both[t] = ref[...]
        send(ref, both.at[t], SC + n, partner)

    res_load.wait()
    mine = jnp.where(lax.div(f, 2) == t, 1, 0)
    first = mine * x + (1 - mine) * c
    second = mine * f + (1 - mine) * y
    first_slot = RES + mine + (1 - mine) * 3
    second_slot = RES + (1 - mine) * 2
    target = own_res.at[f]
    for core in range(2):
        send(
            res_v.at[pl.ds(core * rows, rows), lanes((first - 2 * t) * own_width, own_width)],
            target, first_slot, (r, first, core),
        )
    second_lanes = lanes((second - 2 * t) * own_width, own_width)
    send(res_v.at[pl.ds((1 - t) * rows, rows), second_lanes], target, second_slot, (r, second, 1 - t))
    send(
        res_v.at[pl.ds(t * rows, rows), second_lanes], target, second_slot, (r, second, t),
        when=mine == 0,
    )
    kept_res = pltpu.make_async_copy(
        res_v.at[pl.ds(t * rows, rows), second_lanes], target, recv_sem.at[RES]
    )
    pl.when(mine == 1)(kept_res.start)

    def head_lanes(core, h):
        return lanes((core * heads + h) * head_width, head_width)

    def pump(n, rel):
        block = weight_at(m, fs_of[rel], n, t)
        arrive(block, A + n * 3 + rel - 1)
        send(block, block, DN + m * 8 + rel * 2 + n, partner)

    def along_z(n, rel, late):
        block = weight_at(m, fs_of[rel], n, t)
        for step in range(1, 4):
            to = lax.rem(r + step, 4)
            near = (to - r == 1) | (r - to == 1)
            if late:
                when = r == 2
            else:
                when = (r == 1) | (near & (r != 2))
            send(block, block, ZN + m * 6 + n * 3 + rel - 1, (to, f, t), when=when)

    for h in range(heads):
        keys = slice(h * head_width, (h + 1) * head_width)
        for copy in head_loads[h]:
            copy.wait()
        normed[h] = attend_head(
            q_v[:, keys], k_v[:, keys], v_v[:, keys], lo_v[:, keys],
            sg_ref[:, h : h + 1], head_gain_ref[...],
        )
        target = gathered.at[f, :, head_lanes(t, h)]
        for to, slot in ((x, CX), (y, CX + 8)):
            for core in range(2):
                send(
                    normed.at[h, pl.ds(core * rows, rows)], target, slot + t * 4 + h,
                    (r, to, core),
                )
        send(normed.at[h, pl.ds((1 - t) * rows, rows)], target, CO + h, partner)
        copy = load(normed.at[h, pl.ds(t * rows, rows)], target)
        copy.start()
        own_copies.append(copy)

    for rel in (1, 2):
        pump(0, rel)
        along_z(0, rel, False)

    wo_load.wait()
    wo_half[...] = wo_f32[...].astype(half)
    target = wo_all.at[:, lanes(t * local_width, local_width)]
    send(wo_half, target, WO, partner)
    copy = load(wo_half, target)
    copy.start()
    own_copies.append(copy)
    own_lane = lax.broadcasted_iota(jnp.int32, (own_width, units), 1)
    for n in range(2):
        own_loads[n].wait()
        cut = jnp.where((own_lane < own_spill) & (others[n] == 2), 0.0, own_f32[n])
        own_half[n] = cut.astype(half)
        target = weights.at[
            others[n], pl.ds(f * own_width, own_width), lanes(t * units, units)
        ]
        send(own_half.at[n], target, DN + others[n] * 8, partner)
        copy = load(own_half.at[n], target)
        copy.start()
        own_copies.append(copy)

    for n, rel in ((0, 3), (1, 1), (1, 2), (1, 3)):
        pump(n, rel)
        along_z(n, rel, False)

    from_p_slot, from_q_slot = CX + 8 * t, CX + 8 * (1 - t)
    for h in range(heads):
        for core in range(2):
            block = gathered.at[p, :, head_lanes(core, h)]
            arrive(block, from_p_slot + core * 4 + h)
            send(block, block, CC + core * 4 + h, (r, q, t))

    for n in range(2):
        for rel in (1, 2, 3):
            along_z(n, rel, True)

    for copy in own_copies:
        copy.wait()
    for n, both in enumerate((os_all, gs_all, us_all, ds_all)):
        arrive(both.at[1 - t], SC + n)
    arrive(wo_all.at[:, lanes((1 - t) * local_width, local_width)], WO)
    out_scale = os_all[lax.div(f, 2), :, lanes(lax.rem(f, 2) * own_width, own_width)]
    order = (f, p, q, c)
    res_slots = (RES, RES + 1 + t, RES + 2 - t, RES + 3)

    def feature_lanes(owner):
        return lanes(owner * own_width, own_width)

    for k in range(4):
        seq = order[k]
        if k == 0:
            for h in range(heads):
                arrive(gathered.at[f, :, head_lanes(1 - t, h)], CO + h)
        elif k > 1:
            slot = from_q_slot if k == 2 else CC
            for h in range(heads):
                for core in range(2):
                    arrive(gathered.at[seq, :, head_lanes(core, h)], slot + core * 4 + h)
        arrive(own_res.at[seq], res_slots[k])
        mixed = by_rows(gathered[seq], wo_all[...])
        updated[seq, :, feature_lanes(f)] = (
            own_res[seq].astype(jnp.float32) + out_scale * mixed
        ).astype(half)
        block = updated.at[seq, :, feature_lanes(f)]
        send(block, block, EP + (k ^ 1), (r, p, t))
        send(block, block, EQ + (k ^ 2), (r, q, t))

    def pump_z(matrix):
        for n in range(2):
            for rel in (1, 2, 3):
                block = weight_at(matrix, fs_of[rel], n, t)
                arrive(block, ZN + matrix * 6 + n * 3 + rel - 1)
                send(block, block, DN + matrix * 8 + rel * 2 + n, partner)

    zero, two = jnp.where(m == 0, 1, 0), jnp.where(m == 2, 1, 0)
    pump_z(zero)
    for k in range(4):
        block = updated.at[order[k], :, feature_lanes(p)]
        arrive(block, EP + k)
        send(block, block, EC + (k ^ 2), (r, q, t))
    pump_z(2 - two)

    arrive_whole = [
        weights.at[
            others[n], pl.ds(f * own_width, own_width), lanes((1 - t) * units, units)
        ]
        for n in range(2)
    ]
    for n in range(2):
        arrive(arrive_whole[n], DN + others[n] * 8)
        arrive(weight_at(m, f, n, 1 - t), DN + m * 8 + n)
    for matrix in range(3):
        for rel in (1, 2, 3):
            for n in range(2):
                arrive(
                    weight_at(matrix, fs_of[rel], n, 1 - t), DN + matrix * 8 + rel * 2 + n
                )

    gate_scale = jnp.concatenate([gs_all[0, :, own_lanes], gs_all[1, :, own_lanes]], axis=1)
    up_scale = jnp.concatenate([us_all[0, :, own_lanes], us_all[1, :, own_lanes]], axis=1)
    columns = width // 2

    def piece(n):
        return slice(n * columns, (n + 1) * columns)

    for k in (3, 1, 0, 2):
        seq = order[k]
        arrive(updated.at[seq, :, feature_lanes(q)], EQ + k)
        arrive(updated.at[seq, :, feature_lanes(c)], EC + k)
        wide = updated[seq].astype(jnp.float32)
        factor = lax.rsqrt(jnp.mean(wide * wide, axis=-1, keepdims=True) + epsilon)
        normin = (wide * factor * mlp_gain_ref[...]).astype(half)
        gate_pre = jnp.dot(normin, weights[0], preferred_element_type=jnp.float32) * gate_scale
        up_pre = jnp.dot(normin, weights[1], preferred_element_type=jnp.float32) * up_scale
        hidden = (jax.nn.silu(gate_pre) * up_pre).astype(half)
        for n in range(2):
            term = by_rows(hidden, weights[2, piece(n), :])
            if k == 3:
                to_p[:, piece(n)] = term.astype(half)
                send(to_p.at[:, piece(n)], from_p.at[:, piece(n)], FP + n, (r, p, t))
            elif k == 1:
                to_p2[:, piece(n)] = term.astype(half)
                send(to_p2.at[:, piece(n)], from_p2.at[:, piece(n)], FP + 2 + n, (r, p, t))
            elif k == 0:
                own_down[:, piece(n)] = term
            else:
                arrive(from_p.at[:, piece(n)], FP + n)
                total = term + from_p[:, piece(n)].astype(jnp.float32)
                to_q[:, piece(n)] = total.astype(half)
                send(to_q.at[:, piece(n)], from_q.at[:, piece(n)], FP + 4 + n, (r, q, t))

    down_scale = jnp.concatenate([ds_all[0], ds_all[1]], axis=1)
    for n in range(2):
        arrive(from_p2.at[:, piece(n)], FP + 2 + n)
        own_down[:, piece(n)] += from_p2[:, piece(n)].astype(jnp.float32)
    for n in range(2):
        arrive(from_q.at[:, piece(n)], FP + 4 + n)
        total = own_down[:, piece(n)] + from_q[:, piece(n)].astype(jnp.float32)
        result[:, piece(n)] = (
            updated[f, :, piece(n)].astype(jnp.float32) + down_scale[:, piece(n)] * total
        ).astype(half)
    mine_rows = pl.ds(t * rows, rows)
    send(
        result.at[:, lanes((1 - t) * local_width, local_width)], out_ref.at[mine_rows], OUT, partner
    )
    out_ref[mine_rows, :] = result[:, lanes(t * local_width, local_width)]
    arrive(out_ref.at[pl.ds((1 - t) * rows, rows)], OUT)
    for copy, when in sent:
        if when is None:
            copy.wait_send()
        else:
            pl.when(when)(copy.wait_send)


def one_kernel_body(
    sizes,
    residual,
    queries,
    key_matrix,
    value_matrix,
    decay_logodds,
    decay_surge,
    head_norm_gain,
    output_matrix,
    output_column_scale,
    premix_norm_gain,
    gate_matrix,
    gate_column_scale,
    up_matrix,
    up_column_scale,
    down_matrix,
    down_column_scale,
):
    half, full = jnp.bfloat16, jnp.float32
    _, tokens, local_width = residual.shape
    rows = tokens // 2
    own_width, total_units = gate_matrix.shape
    width = premix_norm_gain.shape[0]
    heads = decay_surge.shape[2]
    units = -(-total_units // (128 * 4)) * 128
    hbm, vmem = pl.BlockSpec(memory_space=pl.ANY), pl.BlockSpec(memory_space=pltpu.VMEM)
    out = pl.pallas_call(
        layer_kernel,
        out_shape=jax.ShapeDtypeStruct((tokens, local_width), half),
        in_specs=[hbm] * 9 + [vmem] * 7,
        out_specs=vmem,
        scratch_shapes=[
            pltpu.VMEM((tokens, local_width), half),
            pltpu.VMEM((tokens, local_width), half),
            pltpu.VMEM((tokens, local_width), half),
            pltpu.VMEM((tokens, local_width), full),
            pltpu.VMEM((tokens, local_width), half),
            pltpu.VMEM((own_width, local_width), full),
            pltpu.VMEM((own_width, local_width), half),
            pltpu.VMEM((own_width, width), half),
            pltpu.VMEM((own_width, total_units), full),
            pltpu.VMEM((2, own_width, units), full),
            pltpu.VMEM((2, own_width, units), half),
            pltpu.VMEM((4, own_width, units), half),
            pltpu.VMEM((3, width, 2 * units), half),
            pltpu.VMEM((heads, tokens, local_width // heads), half),
            pltpu.VMEM((4, rows, width), half),
            pltpu.VMEM((4, rows, own_width), half),
            pltpu.VMEM((4, rows, width), half),
            pltpu.VMEM((2, 1, local_width), full),
            pltpu.VMEM((2, 1, total_units), full),
            pltpu.VMEM((2, 1, total_units), full),
            pltpu.VMEM((2, 1, local_width), full),
            pltpu.VMEM((rows, width), full),
        ]
        + [pltpu.VMEM((rows, width), half)] * 7
        + [
            pltpu.SemaphoreType.DMA((64,)),
            pltpu.SemaphoreType.DMA((160,)),
            pltpu.SemaphoreType.DMA((104,)),
        ],
        compiler_params=pltpu.CompilerParams(
            collective_id=1, has_side_effects=True, vmem_limit_bytes=60 * 2**20
        ),
    )(
        queries[0], key_matrix[0], value_matrix[0], decay_logodds[0], residual[0],
        output_matrix, gate_matrix, up_matrix, down_matrix,
        decay_surge[0], head_norm_gain.reshape(1, -1), premix_norm_gain.reshape(1, -1),
        output_column_scale.reshape(1, -1), gate_column_scale.reshape(1, -1),
        up_column_scale.reshape(1, -1), down_column_scale.reshape(1, -1),
    )
    return out[None]


def greet(devices):
    barrier = pltpu.get_barrier_semaphore()
    for device in devices:
        pl.semaphore_signal(
            barrier, inc=1, device_id=device, device_id_type=pl.DeviceIdType.MESH
        )
    pl.semaphore_wait(barrier, len(devices))


def chosen_body(mesh):
    sizes = tuple(mesh.shape[name] for name in ("rep", "fs", "tp"))

    def run(*args):
        residual, surge, output_matrix, gate_matrix = args[0], args[5], args[7], args[10]
        sequences, tokens, local_width = residual.shape
        own_width, total_units = gate_matrix.shape
        fits = (
            sizes == (4, 4, 2)
            and sequences == 1
            and tokens % (2 * BLOCK) == 0
            and local_width == 2 * own_width
            and output_matrix.shape == (own_width, local_width)
            and own_width % 128 == 0
            and total_units % 128 == 0
            and total_units >= 512
            and (local_width // surge.shape[2]) % 128 == 0
            and surge.shape[2] == 4
        )
        if fits:
            return one_kernel_body(sizes, *args)
        return body(*args)

    return run


def solution(mesh):
    return jax.shard_map(
        chosen_body(mesh),
        mesh=mesh,
        in_specs=(
            P(("rep", "fs"), None, "tp"),
            P(("rep", "fs"), None, "tp"),
            P(("rep", "fs"), None, "tp"),
            P(("rep", "fs"), None, "tp"),
            P(("rep", "fs"), None, "tp"),
            P(("rep", "fs"), None, "tp"),
            P(),
            P("fs", "tp"),
            P("tp"),
            P(),
            P("fs", "tp"),
            P("tp"),
            P("fs", "tp"),
            P("tp"),
            P("fs", "tp"),
            P("tp"),
        ),
        out_specs=P(("rep", "fs"), None, "tp"),
        check_vma=False,
    )
```

```python
import functools

import jax
import jax.numpy as jnp
from jax import lax
from jax.experimental import pallas as pl
from jax.experimental.pallas import tpu as pltpu
from jax.sharding import PartitionSpec as P

BLOCK = 64


epsilon = 1e-06
softness_factor = 16.0
highest = lax.Precision.HIGHEST


def attend_head(q, k, v, logodds, surge, gain):
    tokens, width = q.shape
    blocks = tokens // BLOCK
    mid = BLOCK // 2 - 1
    decay = (
        jnp.minimum(logodds, 0.0) - jnp.log1p(jnp.exp(-jnp.abs(logodds)))
    ) * (1.0 / softness_factor) + surge
    row = lax.broadcasted_iota(jnp.int32, (BLOCK, BLOCK), 0)
    col = lax.broadcasted_iota(jnp.int32, (BLOCK, BLOCK), 1)
    tri = jnp.where(row >= col, 1.0, 0.0).astype(jnp.bfloat16)
    q = q.astype(jnp.float32) * width ** (-0.5)
    k = k.astype(jnp.float32)
    high = decay.astype(jnp.bfloat16)
    low = (decay - high.astype(jnp.float32)).astype(jnp.bfloat16)
    pieces = []
    for n in range(blocks):
        rows = slice(n * BLOCK, (n + 1) * BLOCK)
        running = jnp.dot(tri, high[rows], preferred_element_type=jnp.float32) + jnp.dot(
            tri, low[rows], preferred_element_type=jnp.float32
        )
        before = running - decay[rows]
        center = running[mid : mid + 1]
        end = running[BLOCK - 1 : BLOCK]
        to_center = jnp.exp(center)
        from_center = jnp.exp(end - center)
        q_forward = q[rows] * jnp.exp(running - center)
        k_forward = k[rows] * jnp.exp(center - running)
        q_backward = q[rows] * jnp.exp(center - before)
        k_backward = k[rows] * jnp.exp(before - center)
        half = jnp.bfloat16
        scores = jnp.where(
            row >= col, by_rows(q_forward.astype(half), k_forward.astype(half)), 0.0
        ) + jnp.where(row <= col, by_rows(q_backward.astype(half), k_backward.astype(half)), 0.0)
        inner = jnp.dot(scores.astype(half), v[rows], preferred_element_type=jnp.float32)
        pieces.append(
            (
                inner,
                (q_forward * to_center).astype(half),
                (q_backward * from_center).astype(half),
                by_columns(v[rows], (k_forward * from_center).astype(half)),
                by_columns(v[rows], (k_backward * to_center).astype(half)),
                jnp.exp(end),
            )
        )
    totals = [piece[0] for piece in pieces]
    state = None
    for n in range(blocks):
        if state is not None:
            totals[n] = totals[n] + by_rows(pieces[n][1], state.astype(jnp.bfloat16))
        state = pieces[n][3] if state is None else pieces[n][5] * state + pieces[n][3]
    state = None
    for n in reversed(range(blocks)):
        if state is not None:
            totals[n] = totals[n] + by_rows(pieces[n][2], state.astype(jnp.bfloat16))
        state = pieces[n][4] if state is None else pieces[n][5] * state + pieces[n][4]
    attended = jnp.concatenate(totals, axis=0)
    scale = lax.rsqrt(jnp.mean(attended * attended, axis=-1, keepdims=True) + epsilon)
    return (attended * scale * gain).astype(jnp.bfloat16)


def by_columns(left, right):
    return lax.dot_general(
        left, right, (((0,), (0,)), ((), ())), preferred_element_type=jnp.float32
    )


def attend_kernel(head_total, q_ref, k_ref, v_ref, lo_ref, sg_ref, gain_ref, out_ref):
    width = q_ref.shape[1] // head_total
    value_width = v_ref.shape[1] // head_total
    for h in range(head_total):
        keys = slice(h * width, (h + 1) * width)
        values = slice(h * value_width, (h + 1) * value_width)
        out_ref[:, values] = attend_head(
            q_ref[:, keys],
            k_ref[:, keys],
            v_ref[:, values],
            lo_ref[:, keys],
            sg_ref[:, h : h + 1],
            gain_ref[...],
        )


def linear_attend(queries, key_matrix, value_matrix, decay_logodds, decay_surge, head_norm_gain):
    _, token_length, head_total = decay_surge.shape
    outs = [
        pl.pallas_call(
            functools.partial(attend_kernel, head_total),
            out_shape=jax.ShapeDtypeStruct(value_matrix.shape[1:], jnp.bfloat16),
            in_specs=[pl.BlockSpec(memory_space=pltpu.VMEM)] * 6,
            out_specs=pl.BlockSpec(memory_space=pltpu.VMEM),
            cost_estimate=pl.CostEstimate(
                flops=10**9, bytes_accessed=4 * 10**6, transcendentals=10**6
            ),
        )(
            queries[b], key_matrix[b], value_matrix[b], decay_logodds[b], decay_surge[b],
            head_norm_gain.reshape(1, -1),
        )
        for b in range(queries.shape[0])
    ]
    return jnp.concatenate(outs, axis=0)


def by_rows(left, right):
    return lax.dot_general(
        left, right, (((1,), (1,)), ((), ())), preferred_element_type=jnp.float32
    )


def body(
    residual,
    queries,
    key_matrix,
    value_matrix,
    decay_logodds,
    decay_surge,
    head_norm_gain,
    output_matrix,
    output_column_scale,
    premix_norm_gain,
    gate_matrix,
    gate_column_scale,
    up_matrix,
    up_column_scale,
    down_matrix,
    down_column_scale,
):
    sequence_batch, token_length, local_width = residual.shape
    row_count = sequence_batch * token_length
    normalized_rows = linear_attend(
        queries, key_matrix, value_matrix, decay_logodds, decay_surge, head_norm_gain
    )
    out_half = output_matrix.astype(jnp.bfloat16)
    out_full = lax.all_gather(out_half, "fs", axis=0, tiled=True)
    mix_terms = by_rows(normalized_rows, out_full)
    mix_total = lax.psum_scatter(
        mix_terms.astype(jnp.bfloat16), "tp", scatter_dimension=1, tiled=True
    ).astype(jnp.float32)
    own_rows = residual.reshape(row_count, local_width).astype(jnp.float32)
    updated = (own_rows + output_column_scale * mix_total).astype(jnp.bfloat16)
    features = lax.all_gather(updated, "tp", axis=1, tiled=True)
    wide_rows = features.astype(jnp.float32)
    factor = lax.rsqrt(jnp.mean(wide_rows * wide_rows, axis=-1, keepdims=True) + epsilon)
    normin = (wide_rows * factor * premix_norm_gain).astype(jnp.bfloat16)
    gate_half = gate_matrix.astype(jnp.bfloat16)
    up_half = up_matrix.astype(jnp.bfloat16)
    down_half = down_matrix.astype(jnp.bfloat16)
    gate_full, up_full, down_full = (
        lax.all_gather(gate_half, "fs", axis=0, tiled=True),
        lax.all_gather(up_half, "fs", axis=0, tiled=True),
        lax.all_gather(down_half, "fs", axis=0, tiled=True),
    )
    gate_pre = jnp.dot(normin, gate_full, preferred_element_type=jnp.float32)
    up_pre = jnp.dot(normin, up_full, preferred_element_type=jnp.float32)
    hidden = (jax.nn.silu(gate_pre * gate_column_scale) * (up_pre * up_column_scale)).astype(
        jnp.bfloat16
    )
    down_terms = by_rows(hidden, down_full)
    down_total = lax.psum_scatter(
        down_terms.astype(jnp.bfloat16), "tp", scatter_dimension=1, tiled=True
    ).astype(jnp.float32)
    result = (updated.astype(jnp.float32) + down_column_scale * down_total).astype(jnp.bfloat16)
    return result.reshape(sequence_batch, token_length, local_width)


VMEM_MIB = 60
EARLY_PART = 4
EXTRA_PART = 8


def layer_kernel(
    q_hbm, k_hbm, v_hbm, lo_hbm, res_hbm, wo_hbm, gate_hbm, up_hbm, down_hbm,
    sg_ref, head_gain_ref, mlp_gain_ref, os_ref, gs_ref, us_ref, ds_ref,
    out_ref,
    q_v, k_v, v_v, lo_v, res_v, wo_f32, wo_half, wo_all,
    stage, own_f32, own_half, blocks, extra_stage, extra_blocks, weights,
    normed, gathered, own_res, updated, os_all, gs_all, us_all,
    own_down, other_down, other_updated, to_p, to_p2, to_q, from_p, from_p2, from_q,
    load_sem, send_sem, recv_sem,
):
    r, f, t = lax.axis_index("rep"), lax.axis_index("fs"), lax.axis_index("tp")
    half = jnp.bfloat16
    x, y, c = f + 1 - 2 * lax.rem(f, 2), lax.rem(f + 2, 4), 3 - f
    p, q = x + t * (y - x), y + t * (x - y)
    fs_of = (f, x, y, c)
    partner = (r, f, 1 - t)
    m = lax.rem(r, 3)
    zero, second = jnp.where(m == 0, 1, 0), jnp.where(m == 2, 1, 2)
    along = (zero, second)
    others = (lax.rem(m + 1, 3), lax.rem(m + 2, 3))
    mats = (gate_hbm, up_hbm, down_hbm)
    tokens, local_width = res_v.shape
    rows = tokens // 2
    own_width, total_units = stage.shape
    units = blocks.shape[2]
    width = updated.shape[2]
    heads = sg_ref.shape[0]
    head_width = local_width // heads
    starts = [min(j * units, total_units - units) for j in range(4)]
    early, extra = own_width // EARLY_PART, own_width // EXTRA_PART
    pieces = ((0, early), (early, own_width - early))
    kept = own_width - extra

    SA, SD, SS, SR, SX, SH, SZ, SWO, SC, SE, SF, SO = 0, 3, 4, 7, 11, 12, 15, 18, 19, 20, 23, 26
    A, RES, CP, CQ, CC, CO, WO, SCALE = 0, 6, 7, 15, 16, 17, 18, 19
    EP, EQ, EC, ZN, DN, XN, FP, OUT = 22, 26, 30, 34, 46, 47, 48, 54
    LSTAGE, LEXTRA, LRES, LHEAD, LWO, LOWN, LKEPT, LEND = 0, 2, 3, 4, 12, 13, 15, 18

    def lanes(start, size):
        return pl.ds(pl.multiple_of(start, 128), size)

    def part(n):
        return pl.ds(*pieces[n])

    def local(source, target, sem):
        return pltpu.make_async_copy(source, target, load_sem.at[sem])

    def send(source, target, sem, slot, device, when=None):
        copy = pltpu.make_async_remote_copy(
            src_ref=source,
            dst_ref=target,
            send_sem=send_sem.at[sem],
            recv_sem=recv_sem.at[slot],
            device_id=device,
            device_id_type=pl.DeviceIdType.MESH,
        )
        if when is None:
            copy.start()
        else:
            pl.when(when)(copy.start)

    def waiter(target, sem, slot):
        return pltpu.make_async_remote_copy(
            src_ref=target,
            dst_ref=target,
            send_sem=send_sem.at[sem],
            recv_sem=recv_sem.at[slot],
            device_id=partner,
            device_id_type=pl.DeviceIdType.MESH,
        )

    def arrive(target, slot):
        waiter(target, 0, slot).wait_recv()

    open_scope = []

    def phase(name):
        if open_scope:
            open_scope.pop().__exit__(None, None, None)
        if name:
            scope = jax.named_scope(name)
            scope.__enter__()
            open_scope.append(scope)

    phase("loads")
    own_start = jnp.minimum(f * units, total_units - units)
    own_spill = f * units - own_start
    own_lanes = lanes(own_start, units)
    extra_rows = pl.ds(kept, extra)
    for n in range(2):
        for mm in range(3):
            @pl.when(m == mm)
            def _(mm=mm, n=n):
                local(mats[mm].at[part(n)], stage.at[part(n)], LSTAGE + n).start()
    local(res_hbm, res_v, LRES).start()
    for mm in (1, 2):
        @pl.when(second == mm)
        def _(mm=mm):
            local(mats[mm].at[extra_rows], extra_stage, LEXTRA).start()
    for h in range(heads):
        keys = slice(h * head_width, (h + 1) * head_width)
        local(lo_hbm.at[:, keys], lo_v.at[:, keys], LHEAD + 2 * h).start()
        for a, b in ((q_hbm, q_v), (k_hbm, k_v), (v_hbm, v_v)):
            local(a.at[:, keys], b.at[:, keys], LHEAD + 2 * h + 1).start()
    local(wo_hbm, wo_f32, LWO).start()
    for n in range(2):
        for mm in range(3):
            @pl.when(m == mm)
            def _(mm=mm, n=n):
                local(
                    mats[(mm + 1 + n) % 3].at[:, own_lanes], own_f32.at[n], LOWN + n
                ).start()

    phase("greet")
    peers = [partner]
    for other in (x, y, c):
        peers += [(r, other, 0), (r, other, 1)]
    peers += [(lax.rem(r + step, 4), f, t) for step in range(1, 4)]
    greet(peers)

    def weight_rows(matrix, owner, start, size, core):
        return weights.at[
            matrix, pl.ds(owner * own_width + start, size), lanes(core * units, units)
        ]

    def weight_at(matrix, owner, n, size=None):
        return weight_rows(matrix, owner, pieces[n][0], size or pieces[n][1], t)

    def cut_blocks(source, target, start, size, matrix):
        lane = lax.broadcasted_iota(jnp.int32, (size, units), 1)
        span = slice(start, start + size)
        for j in range(4):
            cut = source[span, starts[j] : starts[j] + units]
            spill = j * units - starts[j]
            if spill > 0:
                cut = jnp.where((lane < spill) & (matrix == 2), 0.0, cut)
            target[j, span, :] = cut.astype(half)

    phase("cut_send")
    for n in range(2):
        local(gate_hbm.at[part(n)], stage.at[part(n)], LSTAGE + n).wait()
        cut_blocks(stage, blocks, *pieces[n], m)
        for rel in (1, 2, 3):
            send(
                blocks.at[fs_of[rel], part(n)], weight_at(m, f, n),
                SA + rel - 1, A + n * 3 + rel - 1, (r, fs_of[rel], t),
            )
    target = weight_rows(m, f, 0, own_width, t)
    local(blocks.at[f], target, LKEPT).start()
    send(blocks.at[f], target, SD, DN, partner)

    for n, (ref, both) in enumerate(((os_ref, os_all), (gs_ref, gs_all), (us_ref, us_all))):
        both[t] = ref[...].reshape(1, -1)
        send(both.at[t], both.at[t], SS + n, SCALE + n, partner)

    phase("residual")
    local(res_hbm, res_v, LRES).wait()
    mine = jnp.where(lax.div(f, 2) == t, 1, 0)
    first = mine * x + (1 - mine) * c
    other = mine * f + (1 - mine) * y
    target = own_res.at[f]
    first_lanes = lanes((first - 2 * t) * own_width, own_width)
    other_lanes = lanes((other - 2 * t) * own_width, own_width)
    my_rows, other_rows = pl.ds(t * rows, rows), pl.ds((1 - t) * rows, rows)
    for core in range(2):
        send(
            res_v.at[pl.ds(core * rows, rows), first_lanes], target, SR + core, RES,
            (r, first, core),
        )
    send(res_v.at[other_rows, other_lanes], target, SR + 2, RES, (r, other, 1 - t))
    send(res_v.at[my_rows, other_lanes], target, SR + 3, RES, (r, other, t), when=mine == 0)
    kept_res = pltpu.make_async_copy(res_v.at[my_rows, other_lanes], target, recv_sem.at[RES])
    pl.when(mine == 1)(kept_res.start)

    local(gate_hbm.at[extra_rows], extra_stage, LEXTRA).wait()
    cut_blocks(extra_stage, extra_blocks, 0, extra, second)
    for rel in (1, 2, 3):
        send(
            extra_blocks.at[fs_of[rel]], weight_rows(second, f, kept, extra, t), SX, XN,
            (r, fs_of[rel], t),
        )

    def head_lanes(core, h):
        return lanes((core * heads + h) * head_width, head_width)

    def z_moves():
        for step in range(1, 4):
            to = lax.rem(r + step, 4)
            near = (to - r == 1) | (r - to == 1)
            goes = (r == 1) | (r == 2) | near
            short = (r == 2) | ((r == 1) & (to == 2))
            yield step - 1, to, goes, short

    def pump(n, rel):
        block = weight_at(m, fs_of[rel], n)
        arrive(block, A + n * 3 + rel - 1)
        send(block, block, SD, DN, partner)
        for index, to, goes, short in z_moves():
            slot = ZN + n * 3 + rel - 1
            slot = slot + 6 * jnp.where(short, 1, 0)
            if n == 0:
                send(block, block, SZ + index, slot, (to, f, t), when=goes)
            else:
                send(
                    block, block, SZ + index, slot, (to, f, t),
                    when=goes & jnp.logical_not(short),
                )
                cut = weight_at(m, fs_of[rel], n, kept - early)
                send(cut, cut, SZ + index, slot, (to, f, t), when=goes & short)

    def pump_z(n, rel):
        for which in range(2):
            size = kept - early if n == 1 and which == 1 else None
            block = weight_at(along[which], fs_of[rel], n, size)
            arrive(block, ZN + which * 6 + n * 3 + rel - 1)
            send(block, block, SD, DN, partner)

    surge = jnp.transpose(sg_ref[...])
    for h in range(heads):
        phase("head")
        keys = slice(h * head_width, (h + 1) * head_width)
        local(lo_hbm.at[:, keys], lo_v.at[:, keys], LHEAD + 2 * h).wait()
        wide_keys = slice(0, 3 * head_width)
        local(q_hbm.at[:, wide_keys], q_v.at[:, wide_keys], LHEAD + 2 * h + 1).wait()
        normed[h] = attend_head(
            q_v[:, keys], k_v[:, keys], v_v[:, keys], lo_v[:, keys],
            surge[:, h : h + 1], head_gain_ref[...],
        )
        target = gathered.at[f, :, head_lanes(t, h)]
        for core in range(2):
            for n, to in enumerate((x, y)):
                send(
                    normed.at[h, pl.ds(core * rows, rows)], target, SH + n,
                    CP + t * 4 + h if n == core else CQ, (r, to, core),
                )
        send(normed.at[h, other_rows], target, SH + 2, CO, partner)
        local(normed.at[h, my_rows], target, LKEPT + 1).start()
        if h == heads - 2:
            phase("pump_a0")
            for rel in (1, 2):
                pump(0, rel)
    phase("pump_a0")
    pump(0, 3)

    phase("wo_own_cast")
    local(wo_hbm, wo_f32, LWO).wait()
    wo_half[...] = wo_f32[...].astype(half)
    target = wo_all.at[:, lanes(t * local_width, local_width)]
    send(wo_half, target, SWO, WO, partner)
    local(wo_half, target, LKEPT + 2).start()
    own_lane = lax.broadcasted_iota(jnp.int32, (own_width, units), 1)
    for n in range(2):
        local(gate_hbm.at[:, own_lanes], own_f32.at[n], LOWN + n).wait()
        cut = jnp.where((own_lane < own_spill) & (others[n] == 2), 0.0, own_f32[n])
        own_half[n] = cut.astype(half)
        target = weight_rows(others[n], f, 0, own_width, t)
        send(own_half.at[n], target, SD, DN, partner)
        local(own_half.at[n], target, LKEPT).start()

    phase("pump_a1")
    for rel in (1, 2, 3):
        pump(1, rel)
    arrive(extra_blocks.at[pl.ds(0, 3)], XN)
    for rel in (1, 2, 3):
        block = weight_rows(second, fs_of[rel], kept, extra, t)
        send(block, block, SD, DN, partner)

    phase("relay_c")
    for h in range(heads):
        for core in range(2):
            block = gathered.at[p, :, head_lanes(core, h)]
            arrive(block, CP + core * 4 + h)
            send(block, block, SC, CC, (r, q, t))
    phase("pump_z0")
    for rel in (1, 2, 3):
        pump_z(0, rel)
    pump_z(1, 1)

    phase("wait_small")
    local(own_half, own_half, LKEPT).wait()
    local(own_half.at[0], own_half.at[0], LKEPT).wait()
    target = gathered.at[f, :, lanes(t * local_width, local_width)]
    local(target, target, LKEPT + 1).wait()
    local(wo_half, wo_half, LKEPT + 2).wait()
    for n, both in enumerate((os_all, gs_all, us_all)):
        arrive(both.at[1 - t], SCALE + n)
    arrive(wo_half, WO)
    arrive(own_res, RES)
    out_scale = os_all[lax.div(f, 2), :, lanes(lax.rem(f, 2) * own_width, own_width)]
    order = (f, p, q, c)

    def feature_lanes(owner):
        return lanes(owner * own_width, own_width)

    def share(k, sem, slot, to):
        block = updated.at[order[k], :, feature_lanes(f)]
        send(block, block, sem, slot, (r, to, t))

    for k in range(4):
        seq = order[k]
        phase("wait_c")
        if k == 0:
            arrive(gathered.at[f, :, lanes((1 - t) * local_width, local_width)], CO)
        elif k > 1:
            arrive(gathered.at[seq], (CQ, CC)[k - 2])
        phase("outproj")
        mixed = by_rows(gathered[seq], wo_all[...])
        updated[seq, :, feature_lanes(f)] = (
            own_res[seq].astype(jnp.float32) + out_scale * mixed
        ).astype(half)
        if k == 2:
            for done in (2, 0, 1):
                share(done, SE, EP + (done ^ 1), p)
            for done in (1, 2, 0):
                share(done, SE + 1, EQ + (done ^ 2), q)
        elif k == 3:
            share(k, SE, EP + (k ^ 1), p)
            share(k, SE + 1, EQ + (k ^ 2), q)

    phase("pump_z1")
    pump_z(1, 2)
    phase("relay_e")
    for k in (1, 3, 0, 2):
        block = updated.at[order[k], :, feature_lanes(p)]
        arrive(block, EP + k)
        send(block, block, SE + 2, EC + (k ^ 2), (r, q, t))
    phase("pump_z2")
    pump_z(1, 3)
    phase("wait_w")
    arrive(weights.at[:, :, lanes((1 - t) * units, units)], DN)

    gate_scale = jnp.concatenate([gs_all[0, :, own_lanes], gs_all[1, :, own_lanes]], axis=1)
    up_scale = jnp.concatenate([us_all[0, :, own_lanes], us_all[1, :, own_lanes]], axis=1)

    def piece(n):
        return slice(n * local_width, (n + 1) * local_width)

    for k in (3, 1, 0, 2):
        seq = order[k]
        phase("wait_e")
        arrive(updated.at[seq, :, feature_lanes(q)], EQ + k)
        arrive(updated.at[seq, :, feature_lanes(c)], EC + k)
        phase("gate_up")
        wide = updated[seq].astype(jnp.float32)
        factor = lax.rsqrt(jnp.mean(wide * wide, axis=-1, keepdims=True) + epsilon)
        normin = (wide * factor * mlp_gain_ref[...]).astype(half)
        gate_pre = jnp.dot(normin, weights[0], preferred_element_type=jnp.float32) * gate_scale
        up_pre = jnp.dot(normin, weights[1], preferred_element_type=jnp.float32) * up_scale
        hidden = (jax.nn.silu(gate_pre) * up_pre).astype(half)
        phase("down")
        for n in range(2):
            term = by_rows(hidden, weights[2, piece(n), :])
            if k == 3:
                to_p[n] = term.astype(half)
                send(to_p.at[n], from_p.at[n], SF, FP + n, (r, p, t))
            elif k == 1:
                to_p2[n] = term.astype(half)
                send(to_p2.at[n], from_p2.at[t], SF + 1, FP + 2 + t, (r, p, n))
            elif k == 0:
                own_down[n] = term
            else:
                arrive(from_p.at[n], FP + n)
                to_q[n] = (term + from_p[n].astype(jnp.float32)).astype(half)
                send(to_q.at[n], from_q.at[t], SF + 2, FP + 4 + t, (r, q, n))
        if k == 0:
            send(own_down.at[1 - t], other_down, SO, OUT, partner)
            far_half = updated.at[f, :, lanes((1 - t) * local_width, local_width)]
            send(far_half, other_updated, SO + 1, OUT + 1, partner)

    phase("wait_other")
    arrive(other_down, OUT)
    arrive(other_updated, OUT + 1)
    phase("wait_p2")
    for core in range(2):
        arrive(from_p2.at[core], FP + 2 + core)
    own_sum = own_down[t] + from_p2[t].astype(jnp.float32)
    other_sum = other_down[...] + from_p2[1 - t].astype(jnp.float32)
    phase("wait_q")
    for core in range(2):
        arrive(from_q.at[core], FP + 4 + core)
    for n, (core, total, rows_in) in enumerate((
        (t, own_sum, updated[f, :, lanes(t * local_width, local_width)]),
        (1 - t, other_sum, other_updated[...]),
    )):
        total = total + from_q[core].astype(jnp.float32)
        target = pl.ds(core * rows, rows)
        q_v[target, :] = (rows_in.astype(jnp.float32) + ds_ref[...] * total).astype(half)
        local(q_v.at[target], out_ref.at[target], LEND + n).start()

    phase("drain")
    for rel in (1, 2, 3):
        waiter(blocks.at[0], SA + rel - 1, 0).wait_send()
    waiter(weights.at[:, :, lanes(t * units, units)], SD, 0).wait_send()
    for n, both in enumerate((os_all, gs_all, us_all)):
        waiter(both.at[t], SS + n, 0).wait_send()
    for n in range(3):
        waiter(own_res.at[0], SR + n, 0).wait_send()
    pl.when(mine == 0)(waiter(own_res.at[0], SR + 3, 0).wait_send)
    waiter(extra_blocks.at[pl.ds(0, 3)], SX, 0).wait_send()
    for n in range(2):
        waiter(normed, SH + n, 0).wait_send()
    waiter(normed.at[:, pl.ds(0, rows)], SH + 2, 0).wait_send()
    for index, to, goes, short in z_moves():
        for length, when in (
            (own_width, goes & jnp.logical_not(short)), (kept, goes & short),
        ):
            sent = weights.at[0, pl.ds(0, 3 * length), lanes(0, units)]
            pl.when(when)(waiter(sent, SZ + index, 0).wait_send)
    waiter(wo_half, SWO, 0).wait_send()
    waiter(gathered.at[0], SC, 0).wait_send()
    for n in range(3):
        waiter(updated.at[:, :, pl.ds(0, own_width)], SE + n, 0).wait_send()
    for n, sent in enumerate((to_p, to_p2, to_q)):
        waiter(sent, SF + n, 0).wait_send()
    waiter(other_down, SO, 0).wait_send()
    waiter(other_updated, SO + 1, 0).wait_send()
    for n, core in enumerate((t, 1 - t)):
        target = pl.ds(core * rows, rows)
        local(q_v.at[target], out_ref.at[target], LEND + n).wait()
    phase(None)


def one_kernel_body(
    sizes,
    residual,
    queries,
    key_matrix,
    value_matrix,
    decay_logodds,
    decay_surge,
    head_norm_gain,
    output_matrix,
    output_column_scale,
    premix_norm_gain,
    gate_matrix,
    gate_column_scale,
    up_matrix,
    up_column_scale,
    down_matrix,
    down_column_scale,
):
    half, full = jnp.bfloat16, jnp.float32
    _, tokens, local_width = residual.shape
    rows = tokens // 2
    own_width, total_units = gate_matrix.shape
    width = premix_norm_gain.shape[0]
    heads = decay_surge.shape[2]
    units = -(-total_units // (128 * 4)) * 128
    hbm, vmem = pl.BlockSpec(memory_space=pl.ANY), pl.BlockSpec(memory_space=pltpu.VMEM)
    out = pl.pallas_call(
        layer_kernel,
        out_shape=jax.ShapeDtypeStruct((tokens, local_width), half),
        in_specs=[hbm] * 9 + [vmem] * 7,
        out_specs=hbm,
        scratch_shapes=[
            pltpu.VMEM((tokens, local_width), half),
            pltpu.VMEM((tokens, local_width), half),
            pltpu.VMEM((tokens, local_width), half),
            pltpu.VMEM((tokens, local_width), full),
            pltpu.VMEM((tokens, local_width), half),
            pltpu.VMEM((own_width, local_width), full),
            pltpu.VMEM((own_width, local_width), half),
            pltpu.VMEM((own_width, width), half),
            pltpu.VMEM((own_width, total_units), full),
            pltpu.VMEM((2, own_width, units), full),
            pltpu.VMEM((2, own_width, units), half),
            pltpu.VMEM((4, own_width, units), half),
            pltpu.VMEM((own_width // EXTRA_PART, total_units), full),
            pltpu.VMEM((4, own_width // EXTRA_PART, units), half),
            pltpu.VMEM((3, width, 2 * units), half),
            pltpu.VMEM((heads, tokens, local_width // heads), half),
            pltpu.VMEM((4, rows, width), half),
            pltpu.VMEM((4, rows, own_width), half),
            pltpu.VMEM((4, rows, width), half),
            pltpu.VMEM((2, 1, local_width), full),
            pltpu.VMEM((2, 1, total_units), full),
            pltpu.VMEM((2, 1, total_units), full),
            pltpu.VMEM((2, rows, local_width), full),
            pltpu.VMEM((rows, local_width), full),
            pltpu.VMEM((rows, local_width), half),
        ]
        + [pltpu.VMEM((2, rows, local_width), half)] * 6
        + [
            pltpu.SemaphoreType.DMA((20,)),
            pltpu.SemaphoreType.DMA((28,)),
            pltpu.SemaphoreType.DMA((56,)),
        ],
        compiler_params=pltpu.CompilerParams(
            collective_id=1, has_side_effects=True, vmem_limit_bytes=VMEM_MIB * 2**20
        ),
    )(
        queries[0], key_matrix[0], value_matrix[0], decay_logodds[0], residual[0],
        output_matrix, gate_matrix, up_matrix, down_matrix,
        jnp.transpose(decay_surge[0]), head_norm_gain.reshape(1, -1), premix_norm_gain.reshape(1, -1),
        output_column_scale.reshape(1, -1), gate_column_scale,
        up_column_scale, down_column_scale.reshape(1, -1),
    )
    return out[None]


def greet(devices):
    barrier = pltpu.get_barrier_semaphore()
    for device in devices:
        pl.semaphore_signal(
            barrier, inc=1, device_id=device, device_id_type=pl.DeviceIdType.MESH
        )
    pl.semaphore_wait(barrier, len(devices))


def chosen_body(mesh):
    sizes = tuple(mesh.shape[name] for name in ("rep", "fs", "tp"))

    def run(*args):
        residual, surge, output_matrix, gate_matrix = args[0], args[5], args[7], args[10]
        sequences, tokens, local_width = residual.shape
        own_width, total_units = gate_matrix.shape
        fits = (
            sizes == (4, 4, 2)
            and sequences == 1
            and tokens % (2 * BLOCK) == 0
            and local_width == 2 * own_width
            and output_matrix.shape == (own_width, local_width)
            and own_width % 128 == 0
            and total_units % 128 == 0
            and total_units >= 512
            and (local_width // surge.shape[2]) % 128 == 0
            and surge.shape[2] == 4
        )
        if fits:
            return one_kernel_body(sizes, *args)
        return body(*args)

    return run


def solution(mesh):
    return jax.shard_map(
        chosen_body(mesh),
        mesh=mesh,
        in_specs=(
            P(("rep", "fs"), None, "tp"),
            P(("rep", "fs"), None, "tp"),
            P(("rep", "fs"), None, "tp"),
            P(("rep", "fs"), None, "tp"),
            P(("rep", "fs"), None, "tp"),
            P(("rep", "fs"), None, "tp"),
            P(),
            P("fs", "tp"),
            P("tp"),
            P(),
            P("fs", "tp"),
            P("tp"),
            P("fs", "tp"),
            P("tp"),
            P("fs", "tp"),
            P("tp"),
        ),
        out_specs=P(("rep", "fs"), None, "tp"),
        check_vma=False,
    )
```

```python
import functools

import jax
import jax.numpy as jnp
from jax import lax
from jax.experimental import pallas as pl
from jax.experimental.pallas import tpu as pltpu
from jax.sharding import PartitionSpec as P

BLOCK = 64


epsilon = 1e-06
softness_factor = 16.0
highest = lax.Precision.HIGHEST


def attend_head(q, k, v, logodds, surge, gain):
    tokens, width = q.shape
    blocks = tokens // BLOCK
    mid = BLOCK // 2 - 1
    decay = (
        jnp.minimum(logodds, 0.0) - jnp.log1p(jnp.exp(-jnp.abs(logodds)))
    ) * (1.0 / softness_factor) + surge
    row = lax.broadcasted_iota(jnp.int32, (BLOCK, BLOCK), 0)
    col = lax.broadcasted_iota(jnp.int32, (BLOCK, BLOCK), 1)
    tri = jnp.where(row >= col, 1.0, 0.0).astype(jnp.bfloat16)
    q = q.astype(jnp.float32) * width ** (-0.5)
    k = k.astype(jnp.float32)
    high = decay.astype(jnp.bfloat16)
    low = (decay - high.astype(jnp.float32)).astype(jnp.bfloat16)
    pieces = []
    for n in range(blocks):
        rows = slice(n * BLOCK, (n + 1) * BLOCK)
        running = jnp.dot(tri, high[rows], preferred_element_type=jnp.float32) + jnp.dot(
            tri, low[rows], preferred_element_type=jnp.float32
        )
        before = running - decay[rows]
        center = running[mid : mid + 1]
        end = running[BLOCK - 1 : BLOCK]
        to_center = jnp.exp(center)
        from_center = jnp.exp(end - center)
        q_forward = q[rows] * jnp.exp(running - center)
        k_forward = k[rows] * jnp.exp(center - running)
        q_backward = q[rows] * jnp.exp(center - before)
        k_backward = k[rows] * jnp.exp(before - center)
        half = jnp.bfloat16
        scores = jnp.where(
            row >= col, by_rows(q_forward.astype(half), k_forward.astype(half)), 0.0
        ) + jnp.where(row <= col, by_rows(q_backward.astype(half), k_backward.astype(half)), 0.0)
        inner = jnp.dot(scores.astype(half), v[rows], preferred_element_type=jnp.float32)
        pieces.append(
            (
                inner,
                (q_forward * to_center).astype(half),
                (q_backward * from_center).astype(half),
                by_columns(v[rows], (k_forward * from_center).astype(half)),
                by_columns(v[rows], (k_backward * to_center).astype(half)),
                jnp.exp(end),
            )
        )
    totals = [piece[0] for piece in pieces]
    state = None
    for n in range(blocks):
        if state is not None:
            totals[n] = totals[n] + by_rows(pieces[n][1], state.astype(jnp.bfloat16))
        state = pieces[n][3] if state is None else pieces[n][5] * state + pieces[n][3]
    state = None
    for n in reversed(range(blocks)):
        if state is not None:
            totals[n] = totals[n] + by_rows(pieces[n][2], state.astype(jnp.bfloat16))
        state = pieces[n][4] if state is None else pieces[n][5] * state + pieces[n][4]
    attended = jnp.concatenate(totals, axis=0)
    scale = lax.rsqrt(jnp.mean(attended * attended, axis=-1, keepdims=True) + epsilon)
    return (attended * scale * gain).astype(jnp.bfloat16)


def by_columns(left, right):
    return lax.dot_general(
        left, right, (((0,), (0,)), ((), ())), preferred_element_type=jnp.float32
    )


def attend_kernel(head_total, q_ref, k_ref, v_ref, lo_ref, sg_ref, gain_ref, out_ref):
    width = q_ref.shape[1] // head_total
    value_width = v_ref.shape[1] // head_total
    for h in range(head_total):
        keys = slice(h * width, (h + 1) * width)
        values = slice(h * value_width, (h + 1) * value_width)
        out_ref[:, values] = attend_head(
            q_ref[:, keys],
            k_ref[:, keys],
            v_ref[:, values],
            lo_ref[:, keys],
            sg_ref[:, h : h + 1],
            gain_ref[...],
        )


def linear_attend(queries, key_matrix, value_matrix, decay_logodds, decay_surge, head_norm_gain):
    _, token_length, head_total = decay_surge.shape
    outs = [
        pl.pallas_call(
            functools.partial(attend_kernel, head_total),
            out_shape=jax.ShapeDtypeStruct(value_matrix.shape[1:], jnp.bfloat16),
            in_specs=[pl.BlockSpec(memory_space=pltpu.VMEM)] * 6,
            out_specs=pl.BlockSpec(memory_space=pltpu.VMEM),
            cost_estimate=pl.CostEstimate(
                flops=10**9, bytes_accessed=4 * 10**6, transcendentals=10**6
            ),
        )(
            queries[b], key_matrix[b], value_matrix[b], decay_logodds[b], decay_surge[b],
            head_norm_gain.reshape(1, -1),
        )
        for b in range(queries.shape[0])
    ]
    return jnp.concatenate(outs, axis=0)


def by_rows(left, right):
    return lax.dot_general(
        left, right, (((1,), (1,)), ((), ())), preferred_element_type=jnp.float32
    )


def body(
    residual,
    queries,
    key_matrix,
    value_matrix,
    decay_logodds,
    decay_surge,
    head_norm_gain,
    output_matrix,
    output_column_scale,
    premix_norm_gain,
    gate_matrix,
    gate_column_scale,
    up_matrix,
    up_column_scale,
    down_matrix,
    down_column_scale,
):
    sequence_batch, token_length, local_width = residual.shape
    row_count = sequence_batch * token_length
    normalized_rows = linear_attend(
        queries, key_matrix, value_matrix, decay_logodds, decay_surge, head_norm_gain
    )
    out_half = output_matrix.astype(jnp.bfloat16)
    out_full = lax.all_gather(out_half, "fs", axis=0, tiled=True)
    mix_terms = by_rows(normalized_rows, out_full)
    mix_total = lax.psum_scatter(
        mix_terms.astype(jnp.bfloat16), "tp", scatter_dimension=1, tiled=True
    ).astype(jnp.float32)
    own_rows = residual.reshape(row_count, local_width).astype(jnp.float32)
    updated = (own_rows + output_column_scale * mix_total).astype(jnp.bfloat16)
    features = lax.all_gather(updated, "tp", axis=1, tiled=True)
    wide_rows = features.astype(jnp.float32)
    factor = lax.rsqrt(jnp.mean(wide_rows * wide_rows, axis=-1, keepdims=True) + epsilon)
    normin = (wide_rows * factor * premix_norm_gain).astype(jnp.bfloat16)
    gate_half = gate_matrix.astype(jnp.bfloat16)
    up_half = up_matrix.astype(jnp.bfloat16)
    down_half = down_matrix.astype(jnp.bfloat16)
    gate_full, up_full, down_full = (
        lax.all_gather(gate_half, "fs", axis=0, tiled=True),
        lax.all_gather(up_half, "fs", axis=0, tiled=True),
        lax.all_gather(down_half, "fs", axis=0, tiled=True),
    )
    gate_pre = jnp.dot(normin, gate_full, preferred_element_type=jnp.float32)
    up_pre = jnp.dot(normin, up_full, preferred_element_type=jnp.float32)
    hidden = (jax.nn.silu(gate_pre * gate_column_scale) * (up_pre * up_column_scale)).astype(
        jnp.bfloat16
    )
    down_terms = by_rows(hidden, down_full)
    down_total = lax.psum_scatter(
        down_terms.astype(jnp.bfloat16), "tp", scatter_dimension=1, tiled=True
    ).astype(jnp.float32)
    result = (updated.astype(jnp.float32) + down_column_scale * down_total).astype(jnp.bfloat16)
    return result.reshape(sequence_batch, token_length, local_width)


VMEM_MIB = 60
EXTRA_PART = 8
AFTER_HEAD = ((), ((0, 1), (0, 2)), ((0, 3),), ((1, 1), (1, 2)))


def layer_kernel(
    q_hbm, k_hbm, v_hbm, lo_hbm, res_hbm, wo_hbm, gate_hbm, up_hbm, down_hbm,
    sg_hbm, head_gain_hbm, mlp_gain_hbm, os_hbm, gs_hbm, us_hbm, ds_hbm,
    out_ref,
    sg_ref, head_gain_ref, mlp_gain_ref, os_ref, gs_ref, us_ref, ds_ref,
    q_v, k_v, v_v, lo_v, res_v, wo_f32, wo_half, wo_all,
    stage, own_f32, own_half, blocks, extra_stage, extra_blocks, weights,
    normed, gathered, own_res, updated, os_all, gs_all, us_all,
    own_down, other_down, other_updated, to_p, to_p2, to_q, from_p, from_p2, from_q,
    load_sem, send_sem, recv_sem,
):
    r, f, t = lax.axis_index("rep"), lax.axis_index("fs"), lax.axis_index("tp")
    half = jnp.bfloat16
    x, y, c = f + 1 - 2 * lax.rem(f, 2), lax.rem(f + 2, 4), 3 - f
    p, q = x + t * (y - x), y + t * (x - y)
    fs_of = (f, x, y, c)
    partner = (r, f, 1 - t)
    m = lax.rem(r, 3)
    zero, second = jnp.where(m == 0, 1, 0), jnp.where(m == 2, 1, 2)
    along = (zero, second)
    others = (lax.rem(m + 1, 3), lax.rem(m + 2, 3))
    mats = (gate_hbm, up_hbm, down_hbm)
    tokens, local_width = res_v.shape
    rows = tokens // 2
    own_width, total_units = stage.shape
    units = blocks.shape[2]
    width = updated.shape[2]
    heads = sg_ref.shape[0]
    head_width = local_width // heads
    starts = [min(j * units, total_units - units) for j in range(4)]
    eighth, extra = own_width // 8, own_width // EXTRA_PART
    pieces = (
        (0, eighth), (eighth, 3 * eighth), (4 * eighth, 4 * eighth - extra),
        (own_width - extra, extra),
    )
    last = len(pieces) - 1
    kept = own_width - extra

    SA, SD, SS, SR, SX, SH, SZ, SWO, SC, SE, SF, SO = 0, 3, 4, 7, 11, 12, 15, 18, 19, 20, 23, 26
    A, RES, CP, CQ, CC, CO, WO, SCALE = 0, 12, 13, 21, 22, 23, 24, 25
    EP, EQ, EC, ZN, DN, XN, FP, OUT = 28, 32, 36, 40, 64, 66, 67, 73
    LSTAGE, LEXTRA, LRES, LHEAD, LWO, LOWN, LKEPT, LEND, LSMALL = 0, 4, 5, 6, 14, 15, 17, 20, 22

    def lanes(start, size):
        return pl.ds(pl.multiple_of(start, 128), size)

    def part(n):
        return pl.ds(*pieces[n])

    def local(source, target, sem):
        return pltpu.make_async_copy(source, target, load_sem.at[sem])

    def send(source, target, sem, slot, device, when=None):
        copy = pltpu.make_async_remote_copy(
            src_ref=source,
            dst_ref=target,
            send_sem=send_sem.at[sem],
            recv_sem=recv_sem.at[slot],
            device_id=device,
            device_id_type=pl.DeviceIdType.MESH,
        )
        if when is None:
            copy.start()
        else:
            pl.when(when)(copy.start)

    def waiter(target, sem, slot):
        return pltpu.make_async_remote_copy(
            src_ref=target,
            dst_ref=target,
            send_sem=send_sem.at[sem],
            recv_sem=recv_sem.at[slot],
            device_id=partner,
            device_id_type=pl.DeviceIdType.MESH,
        )

    def arrive(target, slot):
        waiter(target, 0, slot).wait_recv()

    open_scope = []

    def phase(name):
        if open_scope:
            open_scope.pop().__exit__(None, None, None)
        if name:
            scope = jax.named_scope(name)
            scope.__enter__()
            open_scope.append(scope)

    phase("loads")
    own_start = jnp.minimum(f * units, total_units - units)
    own_spill = f * units - own_start
    own_lanes = lanes(own_start, units)
    extra_rows = pl.ds(kept, extra)
    for n in range(len(pieces)):
        for mm in range(3):
            @pl.when(m == mm)
            def _(mm=mm, n=n):
                local(mats[mm].at[part(n)], stage.at[part(n)], LSTAGE + n).start()
    small = (
        (os_hbm, os_ref), (gs_hbm, gs_ref), (us_hbm, us_ref), (sg_hbm, sg_ref),
        (head_gain_hbm, head_gain_ref), (mlp_gain_hbm, mlp_gain_ref), (ds_hbm, ds_ref),
    )
    for n, (source, target) in enumerate(small):
        local(source, target, LSMALL + n).start()
    local(res_hbm, res_v, LRES).start()
    for mm in (1, 2):
        @pl.when(second == mm)
        def _(mm=mm):
            local(mats[mm].at[extra_rows], extra_stage, LEXTRA).start()
    for h in range(heads):
        keys = slice(h * head_width, (h + 1) * head_width)
        local(lo_hbm.at[:, keys], lo_v.at[:, keys], LHEAD + 2 * h).start()
        for a, b in ((q_hbm, q_v), (k_hbm, k_v), (v_hbm, v_v)):
            local(a.at[:, keys], b.at[:, keys], LHEAD + 2 * h + 1).start()
    local(wo_hbm, wo_f32, LWO).start()
    for n in range(2):
        for mm in range(3):
            @pl.when(m == mm)
            def _(mm=mm, n=n):
                local(
                    mats[(mm + 1 + n) % 3].at[:, own_lanes], own_f32.at[n], LOWN + n
                ).start()

    phase("greet")
    peers = [partner]
    for other in (x, y, c):
        peers += [(r, other, 0), (r, other, 1)]
    middle = (r == 1) | (r == 2)
    beside = jnp.where(r < 2, r + 1, r - 1)
    away = jnp.where(r < 2, r + 2, r - 2)
    peers += [(beside, f, t), (away, f, t)]
    greet(peers, middle, (jnp.where(r < 2, 0, 3), f, t))

    def weight_rows(matrix, owner, start, size, core):
        return weights.at[
            matrix, pl.ds(owner * own_width + start, size), lanes(core * units, units)
        ]

    def weight_at(matrix, owner, n):
        return weight_rows(matrix, owner, *pieces[n], t)

    def dn(matrix):
        return DN + jnp.where(matrix == 2, 1, 0)

    def cut_blocks(source, target, start, size, matrix):
        lane = lax.broadcasted_iota(jnp.int32, (size, units), 1)
        span = slice(start, start + size)
        for j in range(4):
            cut = source[span, starts[j] : starts[j] + units]
            spill = j * units - starts[j]
            if spill > 0:
                cut = jnp.where((lane < spill) & (matrix == 2), 0.0, cut)
            target[j, span, :] = cut.astype(half)

    phase("cut_send")
    for n in range(len(pieces)):
        local(gate_hbm.at[part(n)], stage.at[part(n)], LSTAGE + n).wait()
        cut_blocks(stage, blocks, *pieces[n], m)
        for rel in (1, 2, 3):
            send(
                blocks.at[fs_of[rel], part(n)], weight_at(m, f, n),
                SA + rel - 1, A + n * 3 + rel - 1, (r, fs_of[rel], t),
            )
    target = weight_rows(m, f, 0, own_width, t)
    local(blocks.at[f], target, LKEPT).start()
    send(blocks.at[f], target, SD, dn(m), partner)

    for n, (source, target) in enumerate(small):
        local(source, target, LSMALL + n).wait()
    for n, (ref, both) in enumerate(((os_ref, os_all), (gs_ref, gs_all), (us_ref, us_all))):
        both[t] = ref[...].reshape(1, -1)
        send(both.at[t], both.at[t], SS + n, SCALE + n, partner)

    phase("residual")
    local(res_hbm, res_v, LRES).wait()
    mine = jnp.where(lax.div(f, 2) == t, 1, 0)
    first = mine * x + (1 - mine) * c
    other = mine * f + (1 - mine) * y
    target = own_res.at[f]
    first_lanes = lanes((first - 2 * t) * own_width, own_width)
    other_lanes = lanes((other - 2 * t) * own_width, own_width)
    my_rows, other_rows = pl.ds(t * rows, rows), pl.ds((1 - t) * rows, rows)
    for core in range(2):
        send(
            res_v.at[pl.ds(core * rows, rows), first_lanes], target, SR + core, RES,
            (r, first, core),
        )
    send(res_v.at[other_rows, other_lanes], target, SR + 2, RES, (r, other, 1 - t))
    send(res_v.at[my_rows, other_lanes], target, SR + 3, RES, (r, other, t), when=mine == 0)
    kept_res = pltpu.make_async_copy(res_v.at[my_rows, other_lanes], target, recv_sem.at[RES])
    pl.when(mine == 1)(kept_res.start)

    local(gate_hbm.at[extra_rows], extra_stage, LEXTRA).wait()
    cut_blocks(extra_stage, extra_blocks, 0, extra, second)
    for rel in (1, 2):
        send(
            extra_blocks.at[fs_of[rel]], weight_rows(second, f, kept, extra, t), SX, XN,
            (r, fs_of[rel], t),
        )

    def head_lanes(core, h):
        return lanes((core * heads + h) * head_width, head_width)

    def z_moves():
        for step in range(1, 4):
            to = lax.rem(r + step, 4)
            near = (to - r == 1) | (r - to == 1)
            goes = (r == 1) | (r == 2) | near
            short = (r == 2) | ((r == 1) & (to == 2))
            yield step - 1, to, goes, short

    def pump(n, rel):
        block = weight_at(m, fs_of[rel], n)
        arrive(block, A + n * 3 + rel - 1)
        send(block, block, SD, dn(m), partner)
        for index, to, goes, short in z_moves():
            slot = ZN + n * 3 + rel - 1
            slot = slot + 12 * jnp.where(short, 1, 0)
            if n == last and rel < 3:
                goes = goes & jnp.logical_not(short)
            send(block, block, SZ + index, slot, (to, f, t), when=goes)

    def pump_z(n, rel):
        for which in range(2):
            if which == 1 and n == last and rel < 3:
                continue
            block = weight_at(along[which], fs_of[rel], n)
            arrive(block, ZN + which * 12 + n * 3 + rel - 1)
            send(block, block, SD, dn(along[which]), partner)

    surge = jnp.transpose(sg_ref[...])
    for h in range(heads):
        phase("head")
        keys = slice(h * head_width, (h + 1) * head_width)
        local(lo_hbm.at[:, keys], lo_v.at[:, keys], LHEAD + 2 * h).wait()
        wide_keys = slice(0, 3 * head_width)
        local(q_hbm.at[:, wide_keys], q_v.at[:, wide_keys], LHEAD + 2 * h + 1).wait()
        normed[h] = attend_head(
            q_v[:, keys], k_v[:, keys], v_v[:, keys], lo_v[:, keys],
            surge[:, h : h + 1], head_gain_ref[...],
        )
        target = gathered.at[f, :, head_lanes(t, h)]
        for core in range(2):
            for n, to in enumerate((x, y)):
                send(
                    normed.at[h, pl.ds(core * rows, rows)], target, SH + n,
                    CP + t * 4 + h if n == core else CQ, (r, to, core),
                )
        send(normed.at[h, other_rows], target, SH + 2, CO, partner)
        local(normed.at[h, my_rows], target, LKEPT + 1).start()
        phase(f"pump_a#h={h}")
        for n, rel in AFTER_HEAD[h]:
            pump(n, rel)

    phase("wo_own_cast")
    local(wo_hbm, wo_f32, LWO).wait()
    wo_half[...] = jnp.transpose(wo_f32[...].astype(half))
    target = wo_all.at[pl.ds(t * local_width, local_width)]
    send(wo_half, target, SWO, WO, partner)
    local(wo_half, target, LKEPT + 2).start()
    own_lane = lax.broadcasted_iota(jnp.int32, (own_width, units), 1)
    for n in range(2):
        local(gate_hbm.at[:, own_lanes], own_f32.at[n], LOWN + n).wait()
        cut = jnp.where((own_lane < own_spill) & (others[n] == 2), 0.0, own_f32[n])
        own_half[n] = cut.astype(half)
        target = weight_rows(others[n], f, 0, own_width, t)
        send(own_half.at[n], target, SD, dn(others[n]), partner)
        local(own_half.at[n], target, LKEPT).start()

    phase("pump_a1")
    for n, rel in ((1, 3), (2, 1), (2, 2), (2, 3), (3, 1), (3, 2), (3, 3)):
        pump(n, rel)
    arrive(extra_blocks.at[pl.ds(0, 2)], XN)
    for rel in (1, 2):
        block = weight_rows(second, fs_of[rel], kept, extra, t)
        send(block, block, SD, dn(second), partner)

    phase("relay_c")
    for h in range(heads):
        for core in range(2):
            block = gathered.at[p, :, head_lanes(core, h)]
            arrive(block, CP + core * 4 + h)
            send(block, block, SC, CC, (r, q, t))
    phase("pump_z0")
    for n in (0, 1):
        for rel in (1, 2, 3):
            pump_z(n, rel)

    phase("wait_small")
    local(own_half, own_half, LKEPT).wait()
    local(own_half.at[0], own_half.at[0], LKEPT).wait()
    target = gathered.at[f, :, lanes(t * local_width, local_width)]
    local(target, target, LKEPT + 1).wait()
    local(wo_half, wo_half, LKEPT + 2).wait()
    for n, both in enumerate((os_all, gs_all, us_all)):
        arrive(both.at[1 - t], SCALE + n)
    arrive(wo_half, WO)
    arrive(own_res, RES)
    out_scale = os_all[lax.div(f, 2), :, lanes(lax.rem(f, 2) * own_width, own_width)]
    order = (f, p, q, c)

    def feature_lanes(owner):
        return lanes(owner * own_width, own_width)

    def share(k, sem, slot, to):
        block = updated.at[order[k], :, feature_lanes(f)]
        send(block, block, sem, slot, (r, to, t))

    def relay(k):
        block = updated.at[order[k], :, feature_lanes(p)]
        arrive(block, EP + k)
        send(block, block, SE + 2, EC + (k ^ 2), (r, q, t))

    for k in range(4):
        seq = order[k]
        phase("wait_c")
        if k == 0:
            arrive(gathered.at[f, :, lanes((1 - t) * local_width, local_width)], CO)
        elif k > 1:
            arrive(gathered.at[seq], (CQ, CC)[k - 2])
        phase("outproj")
        mixed = jnp.dot(gathered[seq], wo_all[...], preferred_element_type=jnp.float32)
        updated[seq, :, feature_lanes(f)] = (
            own_res[seq].astype(jnp.float32) + out_scale * mixed
        ).astype(half)
        if k == 2:
            for done in (2, 0, 1):
                share(done, SE, EP + (done ^ 1), p)
            for done in (1, 2):
                share(done, SE + 1, EQ + (done ^ 2), q)
        elif k == 3:
            share(3, SE, EP + 2, p)
            relay(1)
            for done in (3, 0):
                share(done, SE + 1, EQ + (done ^ 2), q)

    phase("pump_z1")
    pump_z(2, 1)
    phase("relay_e")
    relay(3)
    relay(0)
    phase("pump_z15")
    pump_z(2, 2)
    phase("relay_e")
    relay(2)
    phase("pump_z2")
    for n, rel in ((2, 3), (3, 1), (3, 2), (3, 3)):
        pump_z(n, rel)
    phase("wait_w")
    arrive(weights.at[pl.ds(0, 2), :, lanes((1 - t) * units, units)], DN)

    gate_scale = jnp.concatenate([gs_all[0, :, own_lanes], gs_all[1, :, own_lanes]], axis=1)
    up_scale = jnp.concatenate([us_all[0, :, own_lanes], us_all[1, :, own_lanes]], axis=1)

    def piece(n):
        return slice(n * local_width, (n + 1) * local_width)

    for k in (3, 1, 0, 2):
        seq = order[k]
        phase("wait_e")
        arrive(updated.at[seq, :, feature_lanes(q)], EQ + k)
        arrive(updated.at[seq, :, feature_lanes(c)], EC + k)
        phase("gate_up")
        wide = updated[seq].astype(jnp.float32)
        factor = lax.rsqrt(jnp.mean(wide * wide, axis=-1, keepdims=True) + epsilon)
        normin = (wide * factor * mlp_gain_ref[...]).astype(half)
        gate_pre = jnp.dot(normin, weights[0], preferred_element_type=jnp.float32) * gate_scale
        up_pre = jnp.dot(normin, weights[1], preferred_element_type=jnp.float32) * up_scale
        hidden = (jax.nn.silu(gate_pre) * up_pre).astype(half)
        phase("down")
        if k == 3:
            arrive(weights.at[2, :, lanes((1 - t) * units, units)], DN + 1)
        for n in range(2):
            term = by_rows(hidden, weights[2, piece(n), :])
            if k == 3:
                to_p[n] = term.astype(half)
                send(to_p.at[n], from_p.at[n], SF, FP + n, (r, p, t))
            elif k == 1:
                to_p2[n] = term.astype(half)
                send(to_p2.at[n], from_p2.at[t], SF + 1, FP + 2 + t, (r, p, n))
            elif k == 0:
                own_down[n] = term
            else:
                arrive(from_p.at[n], FP + n)
                to_q[n] = (term + from_p[n].astype(jnp.float32)).astype(half)
                send(to_q.at[n], from_q.at[t], SF + 2, FP + 4 + t, (r, q, n))
        if k == 0:
            send(own_down.at[1 - t], other_down, SO, OUT, partner)
            far_half = updated.at[f, :, lanes((1 - t) * local_width, local_width)]
            send(far_half, other_updated, SO + 1, OUT + 1, partner)

    phase("wait_other")
    arrive(other_down, OUT)
    arrive(other_updated, OUT + 1)
    phase("wait_p2")
    for core in range(2):
        arrive(from_p2.at[core], FP + 2 + core)
    own_sum = own_down[t] + from_p2[t].astype(jnp.float32)
    other_sum = other_down[...] + from_p2[1 - t].astype(jnp.float32)
    phase("wait_q")
    for core in range(2):
        arrive(from_q.at[core], FP + 4 + core)
    for n, (core, total, rows_in) in enumerate((
        (t, own_sum, updated[f, :, lanes(t * local_width, local_width)]),
        (1 - t, other_sum, other_updated[...]),
    )):
        total = total + from_q[core].astype(jnp.float32)
        target = pl.ds(core * rows, rows)
        q_v[target, :] = (rows_in.astype(jnp.float32) + ds_ref[...] * total).astype(half)
        local(q_v.at[target], out_ref.at[target], LEND + n).start()

    phase("drain")
    for rel in (1, 2, 3):
        waiter(blocks.at[0], SA + rel - 1, 0).wait_send()
    waiter(weights.at[:, :, lanes(t * units, units)], SD, 0).wait_send()
    for n, both in enumerate((os_all, gs_all, us_all)):
        waiter(both.at[t], SS + n, 0).wait_send()
    for n in range(3):
        waiter(own_res.at[0], SR + n, 0).wait_send()
    pl.when(mine == 0)(waiter(own_res.at[0], SR + 3, 0).wait_send)
    waiter(extra_blocks.at[pl.ds(0, 2)], SX, 0).wait_send()
    for n in range(2):
        waiter(normed, SH + n, 0).wait_send()
    waiter(normed.at[:, pl.ds(0, rows)], SH + 2, 0).wait_send()
    for index, to, goes, short in z_moves():
        for length, when in (
            (3 * own_width, goes & jnp.logical_not(short)),
            (3 * own_width - 2 * extra, goes & short),
        ):
            sent = weights.at[0, pl.ds(0, length), lanes(0, units)]
            pl.when(when)(waiter(sent, SZ + index, 0).wait_send)
    waiter(wo_half, SWO, 0).wait_send()
    waiter(gathered.at[0], SC, 0).wait_send()
    for n in range(3):
        waiter(updated.at[:, :, pl.ds(0, own_width)], SE + n, 0).wait_send()
    for n, sent in enumerate((to_p, to_p2, to_q)):
        waiter(sent, SF + n, 0).wait_send()
    waiter(other_down, SO, 0).wait_send()
    waiter(other_updated, SO + 1, 0).wait_send()
    for n, core in enumerate((t, 1 - t)):
        target = pl.ds(core * rows, rows)
        local(q_v.at[target], out_ref.at[target], LEND + n).wait()
    phase(None)


def one_kernel_body(
    sizes,
    residual,
    queries,
    key_matrix,
    value_matrix,
    decay_logodds,
    decay_surge,
    head_norm_gain,
    output_matrix,
    output_column_scale,
    premix_norm_gain,
    gate_matrix,
    gate_column_scale,
    up_matrix,
    up_column_scale,
    down_matrix,
    down_column_scale,
):
    half, full = jnp.bfloat16, jnp.float32
    _, tokens, local_width = residual.shape
    rows = tokens // 2
    own_width, total_units = gate_matrix.shape
    width = premix_norm_gain.shape[0]
    heads = decay_surge.shape[2]
    units = -(-total_units // (128 * 4)) * 128
    hbm = pl.BlockSpec(memory_space=pl.ANY)
    out = pl.pallas_call(
        layer_kernel,
        out_shape=jax.ShapeDtypeStruct((tokens, local_width), half),
        in_specs=[hbm] * 16,
        out_specs=hbm,
        scratch_shapes=[
            pltpu.VMEM((heads, tokens), full),
            pltpu.VMEM((1, head_norm_gain.shape[0]), full),
            pltpu.VMEM((1, width), full),
            pltpu.VMEM((1, local_width), full),
            pltpu.VMEM((total_units,), full),
            pltpu.VMEM((total_units,), full),
            pltpu.VMEM((1, local_width), full),
            pltpu.VMEM((tokens, local_width), half),
            pltpu.VMEM((tokens, local_width), half),
            pltpu.VMEM((tokens, local_width), half),
            pltpu.VMEM((tokens, local_width), full),
            pltpu.VMEM((tokens, local_width), half),
            pltpu.VMEM((own_width, local_width), full),
            pltpu.VMEM((local_width, own_width), half),
            pltpu.VMEM((width, own_width), half),
            pltpu.VMEM((own_width, total_units), full),
            pltpu.VMEM((2, own_width, units), full),
            pltpu.VMEM((2, own_width, units), half),
            pltpu.VMEM((4, own_width, units), half),
            pltpu.VMEM((own_width // EXTRA_PART, total_units), full),
            pltpu.VMEM((4, own_width // EXTRA_PART, units), half),
            pltpu.VMEM((3, width, 2 * units), half),
            pltpu.VMEM((heads, tokens, local_width // heads), half),
            pltpu.VMEM((4, rows, width), half),
            pltpu.VMEM((4, rows, own_width), half),
            pltpu.VMEM((4, rows, width), half),
            pltpu.VMEM((2, 1, local_width), full),
            pltpu.VMEM((2, 1, total_units), full),
            pltpu.VMEM((2, 1, total_units), full),
            pltpu.VMEM((2, rows, local_width), full),
            pltpu.VMEM((rows, local_width), full),
            pltpu.VMEM((rows, local_width), half),
        ]
        + [pltpu.VMEM((2, rows, local_width), half)] * 6
        + [
            pltpu.SemaphoreType.DMA((29,)),
            pltpu.SemaphoreType.DMA((28,)),
            pltpu.SemaphoreType.DMA((75,)),
        ],
        compiler_params=pltpu.CompilerParams(
            collective_id=1, has_side_effects=True, vmem_limit_bytes=VMEM_MIB * 2**20
        ),
    )(
        queries[0], key_matrix[0], value_matrix[0], decay_logodds[0], residual[0],
        output_matrix, gate_matrix, up_matrix, down_matrix,
        jnp.transpose(decay_surge[0]), head_norm_gain.reshape(1, -1), premix_norm_gain.reshape(1, -1),
        output_column_scale.reshape(1, -1), gate_column_scale,
        up_column_scale, down_column_scale.reshape(1, -1),
    )
    return out[None]


def greet(devices, more, extra):
    barrier = pltpu.get_barrier_semaphore()

    def signal(device):
        pl.semaphore_signal(
            barrier, inc=1, device_id=device, device_id_type=pl.DeviceIdType.MESH
        )

    for device in devices:
        signal(device)
    pl.when(more)(lambda: signal(extra))
    pl.semaphore_wait(barrier, len(devices) + jnp.where(more, 1, 0))


def chosen_body(mesh):
    sizes = tuple(mesh.shape[name] for name in ("rep", "fs", "tp"))

    def run(*args):
        residual, surge, output_matrix, gate_matrix = args[0], args[5], args[7], args[10]
        sequences, tokens, local_width = residual.shape
        own_width, total_units = gate_matrix.shape
        fits = (
            sizes == (4, 4, 2)
            and sequences == 1
            and tokens % (2 * BLOCK) == 0
            and local_width == 2 * own_width
            and output_matrix.shape == (own_width, local_width)
            and own_width % 128 == 0
            and total_units % 128 == 0
            and total_units >= 512
            and (local_width // surge.shape[2]) % 128 == 0
            and surge.shape[2] == 4
        )
        if fits:
            return one_kernel_body(sizes, *args)
        return body(*args)

    return run


def solution(mesh):
    return jax.shard_map(
        chosen_body(mesh),
        mesh=mesh,
        in_specs=(
            P(("rep", "fs"), None, "tp"),
            P(("rep", "fs"), None, "tp"),
            P(("rep", "fs"), None, "tp"),
            P(("rep", "fs"), None, "tp"),
            P(("rep", "fs"), None, "tp"),
            P(("rep", "fs"), None, "tp"),
            P(),
            P("fs", "tp"),
            P("tp"),
            P(),
            P("fs", "tp"),
            P("tp"),
            P("fs", "tp"),
            P("tp"),
            P("fs", "tp"),
            P("tp"),
        ),
        out_specs=P(("rep", "fs"), None, "tp"),
        check_vma=False,
    )
```

```python
import functools

import jax
import jax.numpy as jnp
from jax import lax
from jax.experimental import pallas as pl
from jax.experimental.pallas import tpu as pltpu
from jax.sharding import PartitionSpec as P

BLOCK = 64


epsilon = 1e-06
softness_factor = 16.0
highest = lax.Precision.HIGHEST


def attend_head(q, k, v, logodds, surge, gain):
    tokens, width = q.shape
    blocks = tokens // BLOCK
    mid = BLOCK // 2 - 1
    decay = (
        jnp.minimum(logodds, 0.0) - jnp.log1p(jnp.exp(-jnp.abs(logodds)))
    ) * (1.0 / softness_factor) + surge
    row = lax.broadcasted_iota(jnp.int32, (BLOCK, BLOCK), 0)
    col = lax.broadcasted_iota(jnp.int32, (BLOCK, BLOCK), 1)
    tri = jnp.where(row >= col, 1.0, 0.0).astype(jnp.bfloat16)
    q = q.astype(jnp.float32) * width ** (-0.5)
    k = k.astype(jnp.float32)
    high = decay.astype(jnp.bfloat16)
    low = (decay - high.astype(jnp.float32)).astype(jnp.bfloat16)
    pieces = []
    for n in range(blocks):
        rows = slice(n * BLOCK, (n + 1) * BLOCK)
        running = jnp.dot(tri, high[rows], preferred_element_type=jnp.float32) + jnp.dot(
            tri, low[rows], preferred_element_type=jnp.float32
        )
        before = running - decay[rows]
        center = running[mid : mid + 1]
        end = running[BLOCK - 1 : BLOCK]
        to_center = jnp.exp(center)
        from_center = jnp.exp(end - center)
        q_forward = q[rows] * jnp.exp(running - center)
        k_forward = k[rows] * jnp.exp(center - running)
        q_backward = q[rows] * jnp.exp(center - before)
        k_backward = k[rows] * jnp.exp(before - center)
        half = jnp.bfloat16
        scores = jnp.where(
            row >= col, by_rows(q_forward.astype(half), k_forward.astype(half)), 0.0
        ) + jnp.where(row <= col, by_rows(q_backward.astype(half), k_backward.astype(half)), 0.0)
        inner = jnp.dot(scores.astype(half), v[rows], preferred_element_type=jnp.float32)
        pieces.append(
            (
                inner,
                (q_forward * to_center).astype(half),
                (q_backward * from_center).astype(half),
                by_columns(v[rows], (k_forward * from_center).astype(half)),
                by_columns(v[rows], (k_backward * to_center).astype(half)),
                jnp.exp(end),
            )
        )
    totals = [piece[0] for piece in pieces]
    state = None
    for n in range(blocks):
        if state is not None:
            totals[n] = totals[n] + by_rows(pieces[n][1], state.astype(jnp.bfloat16))
        state = pieces[n][3] if state is None else pieces[n][5] * state + pieces[n][3]
    state = None
    for n in reversed(range(blocks)):
        if state is not None:
            totals[n] = totals[n] + by_rows(pieces[n][2], state.astype(jnp.bfloat16))
        state = pieces[n][4] if state is None else pieces[n][5] * state + pieces[n][4]
    attended = jnp.concatenate(totals, axis=0)
    scale = lax.rsqrt(jnp.mean(attended * attended, axis=-1, keepdims=True) + epsilon)
    return (attended * scale * gain).astype(jnp.bfloat16)


def by_columns(left, right):
    return lax.dot_general(
        left, right, (((0,), (0,)), ((), ())), preferred_element_type=jnp.float32
    )


def attend_kernel(head_total, q_ref, k_ref, v_ref, lo_ref, sg_ref, gain_ref, out_ref):
    width = q_ref.shape[1] // head_total
    value_width = v_ref.shape[1] // head_total
    for h in range(head_total):
        keys = slice(h * width, (h + 1) * width)
        values = slice(h * value_width, (h + 1) * value_width)
        out_ref[:, values] = attend_head(
            q_ref[:, keys],
            k_ref[:, keys],
            v_ref[:, values],
            lo_ref[:, keys],
            sg_ref[:, h : h + 1],
            gain_ref[...],
        )


def linear_attend(queries, key_matrix, value_matrix, decay_logodds, decay_surge, head_norm_gain):
    _, token_length, head_total = decay_surge.shape
    outs = [
        pl.pallas_call(
            functools.partial(attend_kernel, head_total),
            out_shape=jax.ShapeDtypeStruct(value_matrix.shape[1:], jnp.bfloat16),
            in_specs=[pl.BlockSpec(memory_space=pltpu.VMEM)] * 6,
            out_specs=pl.BlockSpec(memory_space=pltpu.VMEM),
            cost_estimate=pl.CostEstimate(
                flops=10**9, bytes_accessed=4 * 10**6, transcendentals=10**6
            ),
        )(
            queries[b], key_matrix[b], value_matrix[b], decay_logodds[b], decay_surge[b],
            head_norm_gain.reshape(1, -1),
        )
        for b in range(queries.shape[0])
    ]
    return jnp.concatenate(outs, axis=0)


def by_rows(left, right):
    return lax.dot_general(
        left, right, (((1,), (1,)), ((), ())), preferred_element_type=jnp.float32
    )


def body(
    residual,
    queries,
    key_matrix,
    value_matrix,
    decay_logodds,
    decay_surge,
    head_norm_gain,
    output_matrix,
    output_column_scale,
    premix_norm_gain,
    gate_matrix,
    gate_column_scale,
    up_matrix,
    up_column_scale,
    down_matrix,
    down_column_scale,
):
    sequence_batch, token_length, local_width = residual.shape
    row_count = sequence_batch * token_length
    normalized_rows = linear_attend(
        queries, key_matrix, value_matrix, decay_logodds, decay_surge, head_norm_gain
    )
    out_half = output_matrix.astype(jnp.bfloat16)
    out_full = lax.all_gather(out_half, "fs", axis=0, tiled=True)
    mix_terms = by_rows(normalized_rows, out_full)
    mix_total = lax.psum_scatter(
        mix_terms.astype(jnp.bfloat16), "tp", scatter_dimension=1, tiled=True
    ).astype(jnp.float32)
    own_rows = residual.reshape(row_count, local_width).astype(jnp.float32)
    updated = (own_rows + output_column_scale * mix_total).astype(jnp.bfloat16)
    features = lax.all_gather(updated, "tp", axis=1, tiled=True)
    wide_rows = features.astype(jnp.float32)
    factor = lax.rsqrt(jnp.mean(wide_rows * wide_rows, axis=-1, keepdims=True) + epsilon)
    normin = (wide_rows * factor * premix_norm_gain).astype(jnp.bfloat16)
    gate_half = gate_matrix.astype(jnp.bfloat16)
    up_half = up_matrix.astype(jnp.bfloat16)
    down_half = down_matrix.astype(jnp.bfloat16)
    gate_full, up_full, down_full = (
        lax.all_gather(gate_half, "fs", axis=0, tiled=True),
        lax.all_gather(up_half, "fs", axis=0, tiled=True),
        lax.all_gather(down_half, "fs", axis=0, tiled=True),
    )
    gate_pre = jnp.dot(normin, gate_full, preferred_element_type=jnp.float32)
    up_pre = jnp.dot(normin, up_full, preferred_element_type=jnp.float32)
    hidden = (jax.nn.silu(gate_pre * gate_column_scale) * (up_pre * up_column_scale)).astype(
        jnp.bfloat16
    )
    down_terms = by_rows(hidden, down_full)
    down_total = lax.psum_scatter(
        down_terms.astype(jnp.bfloat16), "tp", scatter_dimension=1, tiled=True
    ).astype(jnp.float32)
    result = (updated.astype(jnp.float32) + down_column_scale * down_total).astype(jnp.bfloat16)
    return result.reshape(sequence_batch, token_length, local_width)


VMEM_MIB = 60
EXTRA = (1,)
AFTER_HEAD = ((), ((0, 1), (0, 2)), ((0, 3),), ((1, 1), (1, 2)))


def layer_kernel(
    q_hbm, k_hbm, v_hbm, lo_hbm, res_hbm, wo_hbm, gate_hbm, up_hbm, down_hbm,
    sg_hbm, head_gain_hbm, mlp_gain_hbm, os_hbm, gs_hbm, us_hbm, ds_hbm,
    out_ref,
    sg_ref, head_gain_ref, mlp_gain_ref, os_ref, gs_ref, us_ref, ds_ref,
    q_v, k_v, v_v, lo_v, res_v, wo_f32, wo_half, wo_all,
    stage, own_f32, own_half, blocks, extra_stage, extra_blocks, weights,
    normed, gathered, own_res, updated, os_all, gs_all, us_all,
    own_down, other_down, other_updated, to_p, to_p2, to_q, from_p, from_p2, from_q,
    load_sem, send_sem, recv_sem,
):
    r, f, t = lax.axis_index("rep"), lax.axis_index("fs"), lax.axis_index("tp")
    half = jnp.bfloat16
    x, y, c = f + 1 - 2 * lax.rem(f, 2), lax.rem(f + 2, 4), 3 - f
    p, q = x + t * (y - x), y + t * (x - y)
    fs_of = (f, x, y, c)
    partner = (r, f, 1 - t)
    z_one = r + 1 - 2 * lax.rem(r, 2)
    z_two = jnp.where(r < 2, 2, 1)
    z_three = 6 - r - z_one - z_two
    middle = (r == 1) | (r == 2)
    end = jnp.logical_not(middle)
    pair = lax.div(f, 2)
    soon, next_, late = (
        (x + pair * (y - x), 1 + pair), (y + pair * (c - y), 2 + pair),
        (c + pair * (x - c), 3 - 2 * pair),
    )
    mats = (gate_hbm, up_hbm, down_hbm)
    tokens, local_width = res_v.shape
    rows = tokens // 2
    own_width, total_units = wo_f32.shape[0], stage.shape[2]
    units = blocks.shape[3]
    quarter = stage.shape[1]
    width = updated.shape[2]
    heads = sg_ref.shape[0]
    head_width = local_width // heads
    starts = [min(j * units, total_units - units) for j in range(4)]
    SA, SD, SS, SR, SH, SZ, SWO, SC, SE, SF, SO, SX = 0, 3, 4, 7, 11, 14, 17, 18, 19, 22, 25, 27
    A, RES, CP, CQ, CC, CO, WO, SCALE = 0, 9, 10, 18, 19, 20, 21, 22
    EP, EQ, EC, ZN, DN, FP, OUT = 25, 29, 33, 37, 73, 76, 82
    LSTAGE, LRES, LHEAD, LWO, LOWN, LKEPT, LEND, LSMALL, LEXTRA = 0, 3, 4, 12, 13, 16, 19, 21, 28

    def lanes(start, size):
        return pl.ds(pl.multiple_of(start, 128), size)

    def local(source, target, sem):
        return pltpu.make_async_copy(source, target, load_sem.at[sem])

    def send(source, target, sem, slot, device, when=None):
        copy = pltpu.make_async_remote_copy(
            src_ref=source,
            dst_ref=target,
            send_sem=send_sem.at[sem],
            recv_sem=recv_sem.at[slot],
            device_id=device,
            device_id_type=pl.DeviceIdType.MESH,
        )
        if when is None:
            copy.start()
        else:
            pl.when(when)(copy.start)

    def waiter(target, sem, slot):
        return pltpu.make_async_remote_copy(
            src_ref=target,
            dst_ref=target,
            send_sem=send_sem.at[sem],
            recv_sem=recv_sem.at[slot],
            device_id=partner,
            device_id_type=pl.DeviceIdType.MESH,
        )

    def arrive(target, slot):
        waiter(target, 0, slot).wait_recv()

    open_scope = []

    def phase(name):
        if open_scope:
            open_scope.pop().__exit__(None, None, None)
        if name:
            scope = jax.named_scope(name)
            scope.__enter__()
            open_scope.append(scope)

    phase("loads")
    own_start = jnp.minimum(f * units, total_units - units)
    own_spill = f * units - own_start
    own_lanes = lanes(own_start, units)
    my_quarter = pl.ds(pl.multiple_of(r * quarter, quarter), quarter)
    for mm in range(3):
        local(mats[mm].at[my_quarter], stage.at[mm], LSTAGE + mm).start()
    small = (
        (os_hbm, os_ref), (gs_hbm, gs_ref), (us_hbm, us_ref), (sg_hbm, sg_ref),
        (head_gain_hbm, head_gain_ref), (mlp_gain_hbm, mlp_gain_ref), (ds_hbm, ds_ref),
    )
    for n, (source, target) in enumerate(small):
        local(source, target, LSMALL + n).start()
    local(res_hbm, res_v, LRES).start()
    for h in range(heads):
        keys = slice(h * head_width, (h + 1) * head_width)
        local(lo_hbm.at[:, keys], lo_v.at[:, keys], LHEAD + 2 * h).start()
        for a, b in ((q_hbm, q_v), (k_hbm, k_v), (v_hbm, v_v)):
            local(a.at[:, keys], b.at[:, keys], LHEAD + 2 * h + 1).start()
    local(wo_hbm, wo_f32, LWO).start()
    for mm in range(3):
        local(mats[mm].at[:, own_lanes], own_f32.at[mm], LOWN + mm).start()
    far_quarter = pl.ds(pl.multiple_of(z_three * quarter, quarter), quarter)
    extra_loads = [
        local(mats[mm].at[far_quarter], extra_stage.at[n], LEXTRA + n)
        for n, mm in enumerate(EXTRA)
    ]
    for copy in extra_loads:
        pl.when(end)(copy.start)

    phase("greet")
    peers = [partner]
    for other in (x, y, c):
        peers += [(r, other, 0), (r, other, 1)]
    beside = jnp.where(r < 2, r + 1, r - 1)
    away = jnp.where(r < 2, r + 2, r - 2)
    peers += [(beside, f, t), (away, f, t)]
    greet(peers, middle, (jnp.where(r < 2, 0, 3), f, t))

    def weight_rows(matrix, owner, start, size, core):
        return weights.at[
            matrix, pl.ds(owner * own_width + start, size), lanes(core * units, units)
        ]

    def dn(matrix, owner):
        return DN if matrix < 2 else DN + 1 + lax.div(owner, 2)

    def cut_blocks(mm, source, target):
        lane = lax.broadcasted_iota(jnp.int32, (quarter, units), 1)
        for j in range(4):
            cut = source[:, starts[j] : starts[j] + units]
            spill = j * units - starts[j]
            if spill > 0 and mm == 2:
                cut = jnp.where(lane < spill, 0.0, cut)
            target[j] = cut.astype(half)

    phase("cut_send")
    for mm in range(3):
        local(mats[mm].at[my_quarter], stage.at[mm], LSTAGE + mm).wait()
        cut_blocks(mm, stage.at[mm], blocks.at[mm])
        for rel in (1, 2, 3):
            send(
                blocks.at[mm, fs_of[rel]], weight_rows(mm, f, r * quarter, quarter, t),
                SA + rel - 1, A + mm * 3 + rel - 1, (r, fs_of[rel], t),
            )

    for n, (source, target) in enumerate(small):
        local(source, target, LSMALL + n).wait()
    for n, (ref, both) in enumerate(((os_ref, os_all), (gs_ref, gs_all), (us_ref, us_all))):
        both[t] = ref[...].reshape(1, -1)
        send(both.at[t], both.at[t], SS + n, SCALE + n, partner)

    phase("residual")
    local(res_hbm, res_v, LRES).wait()
    mine = jnp.where(lax.div(f, 2) == t, 1, 0)
    first = mine * x + (1 - mine) * c
    other = mine * f + (1 - mine) * y
    target = own_res.at[f]
    first_lanes = lanes((first - 2 * t) * own_width, own_width)
    other_lanes = lanes((other - 2 * t) * own_width, own_width)
    my_rows, other_rows = pl.ds(t * rows, rows), pl.ds((1 - t) * rows, rows)
    for core in range(2):
        send(
            res_v.at[pl.ds(core * rows, rows), first_lanes], target, SR + core, RES,
            (r, first, core),
        )
    send(res_v.at[other_rows, other_lanes], target, SR + 2, RES, (r, other, 1 - t))
    send(res_v.at[my_rows, other_lanes], target, SR + 3, RES, (r, other, t), when=mine == 0)
    kept_res = pltpu.make_async_copy(res_v.at[my_rows, other_lanes], target, recv_sem.at[RES])
    pl.when(mine == 1)(kept_res.start)

    def head_lanes(core, h):
        return lanes((core * heads + h) * head_width, head_width)

    def piece_of(matrix, owner, plane):
        return weight_rows(matrix, owner, plane * quarter, quarter, t)

    def z_slot(matrix, rel, plane):
        return ZN + plane * 9 + matrix * 3 + rel - 1

    def pump(matrix, rel):
        block, slot = piece_of(matrix, fs_of[rel], r), z_slot(matrix, rel, r)
        arrive(block, A + matrix * 3 + rel - 1)
        when = end | (late[1] != rel) if matrix == 2 else None
        send(block, block, SZ, slot, (z_one, f, t), when)
        send(block, block, SZ + 1, slot, (z_two, f, t))
        send(block, block, SD, dn(matrix, fs_of[rel]), partner)

    def pump_late():
        owner, rel = late
        block = piece_of(2, owner, r)
        send(block, block, SZ, z_slot(2, rel, r), (z_one, f, t), middle)

    def pump_z(which, when, todo):
        for matrix, (owner, rel) in todo:
            for source in which:
                plane = (z_one, z_two, z_three)[source]
                block, slot = piece_of(matrix, owner, plane), z_slot(matrix, rel, plane)
                pl.when(when)(waiter(block, 0, slot).wait_recv)
                direct = source == 2 and matrix in EXTRA and rel < 3
                if when is middle and source > 0 and not direct:
                    send(block, block, SZ + 2, slot, (z_one, f, t), when)
                send(block, block, SD, dn(matrix, owner), partner, when)

    gates = [(0, (fs_of[rel], rel)) for rel in (1, 2, 3)]
    ups = [(1, (fs_of[rel], rel)) for rel in (1, 2, 3)]

    surge = jnp.transpose(sg_ref[...])
    for h in range(heads):
        phase("head")
        keys = slice(h * head_width, (h + 1) * head_width)
        local(lo_hbm.at[:, keys], lo_v.at[:, keys], LHEAD + 2 * h).wait()
        wide_keys = slice(0, 3 * head_width)
        local(q_hbm.at[:, wide_keys], q_v.at[:, wide_keys], LHEAD + 2 * h + 1).wait()
        normed[h] = attend_head(
            q_v[:, keys], k_v[:, keys], v_v[:, keys], lo_v[:, keys],
            surge[:, h : h + 1], head_gain_ref[...],
        )
        target = gathered.at[f, :, head_lanes(t, h)]
        for core in range(2):
            for n, to in enumerate((x, y)):
                send(
                    normed.at[h, pl.ds(core * rows, rows)], target, SH + n,
                    CP + t * 4 + h if n == core else CQ, (r, to, core),
                )
        send(normed.at[h, other_rows], target, SH + 2, CO, partner)
        local(normed.at[h, my_rows], target, LKEPT + 1).start()
        phase(f"pump_a#h={h}")
        for n, rel in AFTER_HEAD[h]:
            pump(n, rel)

    phase("wo_own_cast")
    local(wo_hbm, wo_f32, LWO).wait()
    wo_half[...] = jnp.transpose(wo_f32[...].astype(half))
    target = wo_all.at[pl.ds(t * local_width, local_width)]
    send(wo_half, target, SWO, WO, partner)
    local(wo_half, target, LKEPT + 2).start()
    own_lane = lax.broadcasted_iota(jnp.int32, (own_width, units), 1)
    for mm in range(3):
        local(mats[mm].at[:, own_lanes], own_f32.at[mm], LOWN + mm).wait()
        cut = own_f32[mm]
        if mm == 2:
            cut = jnp.where(own_lane < own_spill, 0.0, cut)
        own_half[mm] = cut.astype(half)
        target = weight_rows(mm, f, 0, own_width, t)
        send(own_half.at[mm], target, SD, dn(mm, f), partner)
        local(own_half.at[mm], target, LKEPT).start()

    phase("extras")
    @pl.when(end)
    def _():
        for n, mm in enumerate(EXTRA):
            extra_loads[n].wait()
            cut_blocks(mm, extra_stage.at[n], extra_blocks.at[n])
            for rel in (1, 2):
                send(
                    extra_blocks.at[n, fs_of[rel]], piece_of(mm, f, z_three),
                    SX, z_slot(mm, rel, z_three), (r, fs_of[rel], t),
                )

    phase("pump_a1")
    for n, rel in ((1, 3), (2, 1), (2, 2), (2, 3)):
        pump(n, rel)
    phase("z_gates")
    pump_z((1, 2), middle, gates)

    phase("relay_c")
    for h in range(heads):
        for core in range(2):
            block = gathered.at[p, :, head_lanes(core, h)]
            arrive(block, CP + core * 4 + h)
            send(block, block, SC, CC, (r, q, t))
    phase("pump_z0")
    phase("z_ups")
    pump_z((1, 2), middle, ups)
    phase("pump_z0")
    pump_z((0,), end, gates + ups + [(2, soon)])

    phase("wait_small")
    local(own_half, own_half, LKEPT).wait()
    target = gathered.at[f, :, lanes(t * local_width, local_width)]
    local(target, target, LKEPT + 1).wait()
    local(wo_half, wo_half, LKEPT + 2).wait()
    for n, both in enumerate((os_all, gs_all, us_all)):
        arrive(both.at[1 - t], SCALE + n)
    arrive(wo_half, WO)
    arrive(own_res, RES)
    out_scale = os_all[lax.div(f, 2), :, lanes(lax.rem(f, 2) * own_width, own_width)]
    order = (f, p, q, c)

    def feature_lanes(owner):
        return lanes(owner * own_width, own_width)

    def share(k, sem, slot, to):
        block = updated.at[order[k], :, feature_lanes(f)]
        send(block, block, sem, slot, (r, to, t))

    def relay(k):
        block = updated.at[order[k], :, feature_lanes(p)]
        arrive(block, EP + k)
        send(block, block, SE + 2, EC + (k ^ 2), (r, q, t))

    for k in range(4):
        seq = order[k]
        phase("wait_c")
        if k == 0:
            arrive(gathered.at[f, :, lanes((1 - t) * local_width, local_width)], CO)
        elif k > 1:
            arrive(gathered.at[seq], (CQ, CC)[k - 2])
        phase("outproj")
        mixed = jnp.dot(gathered[seq], wo_all[...], preferred_element_type=jnp.float32)
        updated[seq, :, feature_lanes(f)] = (
            own_res[seq].astype(jnp.float32) + out_scale * mixed
        ).astype(half)
        if k == 2:
            for done in (2, 0, 1):
                share(done, SE, EP + (done ^ 1), p)
            for done in (1, 2):
                share(done, SE + 1, EQ + (done ^ 2), q)
            phase("z_soon")
            pump_z((1, 2), middle, [(2, soon)])
            pump_z((1, 2), end, gates)
        elif k == 3:
            share(3, SE, EP + 2, p)
            relay(1)
            for done in (3, 0):
                share(done, SE + 1, EQ + (done ^ 2), q)

    phase("relay_e")
    relay(3)
    phase("z_downs")
    pump_z((1, 2), middle, [(2, next_), (2, late)])
    pump_late()
    pump_z((0,), middle, gates + ups)
    phase("relay_e")
    relay(0)
    relay(2)
    phase("pump_z2")
    pump_z((1, 2), end, ups)
    pump_z((0,), middle, [(2, soon), (2, next_), (2, late)])
    pump_z((0,), end, [(2, next_)])
    pump_z((1, 2), end, [(2, soon), (2, next_)])
    phase("wait_w")
    arrive(weights.at[pl.ds(0, 2), :, lanes((1 - t) * units, units)], DN)

    gate_scale = jnp.concatenate([gs_all[0, :, own_lanes], gs_all[1, :, own_lanes]], axis=1)
    up_scale = jnp.concatenate([us_all[0, :, own_lanes], us_all[1, :, own_lanes]], axis=1)

    def half_rows(n):
        return pl.ds(pl.multiple_of(n * local_width, local_width), local_width)

    partner_lanes = lanes((1 - t) * units, units)
    hiddens = {}

    def down_terms(k, n):
        term = by_rows(hiddens[k], weights[2, half_rows(n), :])
        if k == 3:
            to_p[n] = term.astype(half)
            send(to_p.at[n], from_p.at[n], SF, FP + n, (r, p, t))
        elif k == 1:
            to_p2[n] = term.astype(half)
            send(to_p2.at[n], from_p2.at[t], SF + 1, FP + 2 + t, (r, p, n))
        elif k == 0:
            own_down[n] = term
        else:
            arrive(from_p.at[n], FP + n)
            to_q[n] = (term + from_p[n].astype(jnp.float32)).astype(half)
            send(to_q.at[n], from_q.at[t], SF + 2, FP + 4 + t, (r, q, n))

    for k in (3, 1, 0, 2):
        seq = order[k]
        phase("wait_e")
        arrive(updated.at[seq, :, feature_lanes(q)], EQ + k)
        arrive(updated.at[seq, :, feature_lanes(c)], EC + k)
        phase("gate_up")
        wide = updated[seq].astype(jnp.float32)
        factor = lax.rsqrt(jnp.mean(wide * wide, axis=-1, keepdims=True) + epsilon)
        normin = (wide * factor * mlp_gain_ref[...]).astype(half)
        gate_pre = jnp.dot(normin, weights[0], preferred_element_type=jnp.float32) * gate_scale
        up_pre = jnp.dot(normin, weights[1], preferred_element_type=jnp.float32) * up_scale
        hiddens[k] = (jax.nn.silu(gate_pre) * up_pre).astype(half)
        if k == 3:
            phase("wait_half")
            arrive(weights.at[2, half_rows(0), partner_lanes], DN + 1)
        phase("down")
        down_terms(k, 0)
    phase("z_last")
    pump_z((0, 1, 2), end, [(2, late)])
    arrive(weights.at[2, half_rows(1), partner_lanes], DN + 2)
    phase("down_far")
    for k in (3, 1, 0):
        down_terms(k, 1)
    send(own_down.at[1 - t], other_down, SO, OUT, partner)
    other_half = updated.at[f, :, lanes((1 - t) * local_width, local_width)]
    send(other_half, other_updated, SO + 1, OUT + 1, partner)
    phase("down_q")
    down_terms(2, 1)

    phase("wait_other")
    arrive(other_down, OUT)
    arrive(other_updated, OUT + 1)
    phase("wait_p2")
    for core in range(2):
        arrive(from_p2.at[core], FP + 2 + core)
    own_sum = own_down[t] + from_p2[t].astype(jnp.float32)
    other_sum = other_down[...] + from_p2[1 - t].astype(jnp.float32)
    phase("wait_q")
    for core in range(2):
        arrive(from_q.at[core], FP + 4 + core)
    for n, (core, total, rows_in) in enumerate((
        (t, own_sum, updated[f, :, lanes(t * local_width, local_width)]),
        (1 - t, other_sum, other_updated[...]),
    )):
        total = total + from_q[core].astype(jnp.float32)
        target = pl.ds(core * rows, rows)
        q_v[target, :] = (rows_in.astype(jnp.float32) + ds_ref[...] * total).astype(half)
        local(q_v.at[target], out_ref.at[target], LEND + n).start()

    phase("drain")
    for rel in (1, 2, 3):
        waiter(blocks.at[:, 0], SA + rel - 1, 0).wait_send()
    waiter(weights.at[:, :, lanes(t * units, units)], SD, 0).wait_send()
    for n, both in enumerate((os_all, gs_all, us_all)):
        waiter(both.at[t], SS + n, 0).wait_send()
    for n in range(3):
        waiter(own_res.at[0], SR + n, 0).wait_send()
    pl.when(mine == 0)(waiter(own_res.at[0], SR + 3, 0).wait_send)
    for n in range(2):
        waiter(normed, SH + n, 0).wait_send()
    waiter(normed.at[:, pl.ds(0, rows)], SH + 2, 0).wait_send()
    for n in range(2):
        waiter(weights.at[0, pl.ds(0, 9 * quarter), lanes(0, units)], SZ + n, 0).wait_send()
    left = 18 - 2 * len(EXTRA)
    relayed = weights.at[0, pl.ds(0, left * quarter), lanes(0, units)]
    extras = extra_blocks.at[:, pl.ds(0, 2)]
    pl.when(end)(waiter(extras, SX, 0).wait_send)
    pl.when(middle)(waiter(relayed, SZ + 2, 0).wait_send)
    waiter(wo_half, SWO, 0).wait_send()
    waiter(gathered.at[0], SC, 0).wait_send()
    for n in range(3):
        waiter(updated.at[:, :, pl.ds(0, own_width)], SE + n, 0).wait_send()
    for n, sent in enumerate((to_p, to_p2, to_q)):
        waiter(sent, SF + n, 0).wait_send()
    waiter(other_down, SO, 0).wait_send()
    waiter(other_updated, SO + 1, 0).wait_send()
    for n, core in enumerate((t, 1 - t)):
        target = pl.ds(core * rows, rows)
        local(q_v.at[target], out_ref.at[target], LEND + n).wait()
    phase(None)


def one_kernel_body(
    sizes,
    residual,
    queries,
    key_matrix,
    value_matrix,
    decay_logodds,
    decay_surge,
    head_norm_gain,
    output_matrix,
    output_column_scale,
    premix_norm_gain,
    gate_matrix,
    gate_column_scale,
    up_matrix,
    up_column_scale,
    down_matrix,
    down_column_scale,
):
    half, full = jnp.bfloat16, jnp.float32
    _, tokens, local_width = residual.shape
    rows = tokens // 2
    own_width, total_units = gate_matrix.shape
    width = premix_norm_gain.shape[0]
    heads = decay_surge.shape[2]
    units = -(-total_units // (128 * 4)) * 128
    hbm = pl.BlockSpec(memory_space=pl.ANY)
    out = pl.pallas_call(
        layer_kernel,
        out_shape=jax.ShapeDtypeStruct((tokens, local_width), half),
        in_specs=[hbm] * 16,
        out_specs=hbm,
        scratch_shapes=[
            pltpu.VMEM((heads, tokens), full),
            pltpu.VMEM((1, head_norm_gain.shape[0]), full),
            pltpu.VMEM((1, width), full),
            pltpu.VMEM((1, local_width), full),
            pltpu.VMEM((total_units,), full),
            pltpu.VMEM((total_units,), full),
            pltpu.VMEM((1, local_width), full),
            pltpu.VMEM((tokens, local_width), half),
            pltpu.VMEM((tokens, local_width), half),
            pltpu.VMEM((tokens, local_width), half),
            pltpu.VMEM((tokens, local_width), full),
            pltpu.VMEM((tokens, local_width), half),
            pltpu.VMEM((own_width, local_width), full),
            pltpu.VMEM((local_width, own_width), half),
            pltpu.VMEM((width, own_width), half),
            pltpu.VMEM((3, own_width // 4, total_units), full),
            pltpu.VMEM((3, own_width, units), full),
            pltpu.VMEM((3, own_width, units), half),
            pltpu.VMEM((3, 4, own_width // 4, units), half),
            pltpu.VMEM((len(EXTRA), own_width // 4, total_units), full),
            pltpu.VMEM((len(EXTRA), 4, own_width // 4, units), half),
            pltpu.VMEM((3, width, 2 * units), half),
            pltpu.VMEM((heads, tokens, local_width // heads), half),
            pltpu.VMEM((4, rows, width), half),
            pltpu.VMEM((4, rows, own_width), half),
            pltpu.VMEM((4, rows, width), half),
            pltpu.VMEM((2, 1, local_width), full),
            pltpu.VMEM((2, 1, total_units), full),
            pltpu.VMEM((2, 1, total_units), full),
            pltpu.VMEM((2, rows, local_width), full),
            pltpu.VMEM((rows, local_width), full),
            pltpu.VMEM((rows, local_width), half),
        ]
        + [pltpu.VMEM((2, rows, local_width), half)] * 6
        + [
            pltpu.SemaphoreType.DMA((28 + len(EXTRA),)),
            pltpu.SemaphoreType.DMA((28,)),
            pltpu.SemaphoreType.DMA((84,)),
        ],
        compiler_params=pltpu.CompilerParams(
            collective_id=1, has_side_effects=True, vmem_limit_bytes=VMEM_MIB * 2**20
        ),
    )(
        queries[0], key_matrix[0], value_matrix[0], decay_logodds[0], residual[0],
        output_matrix, gate_matrix, up_matrix, down_matrix,
        jnp.transpose(decay_surge[0]), head_norm_gain.reshape(1, -1), premix_norm_gain.reshape(1, -1),
        output_column_scale.reshape(1, -1), gate_column_scale,
        up_column_scale, down_column_scale.reshape(1, -1),
    )
    return out[None]


def greet(devices, more, extra):
    barrier = pltpu.get_barrier_semaphore()

    def signal(device):
        pl.semaphore_signal(
            barrier, inc=1, device_id=device, device_id_type=pl.DeviceIdType.MESH
        )

    for device in devices:
        signal(device)
    pl.when(more)(lambda: signal(extra))
    pl.semaphore_wait(barrier, len(devices) + jnp.where(more, 1, 0))


def chosen_body(mesh):
    sizes = tuple(mesh.shape[name] for name in ("rep", "fs", "tp"))

    def run(*args):
        residual, surge, output_matrix, gate_matrix = args[0], args[5], args[7], args[10]
        sequences, tokens, local_width = residual.shape
        own_width, total_units = gate_matrix.shape
        fits = (
            sizes == (4, 4, 2)
            and sequences == 1
            and tokens % (2 * BLOCK) == 0
            and local_width == 2 * own_width
            and output_matrix.shape == (own_width, local_width)
            and own_width % 128 == 0
            and total_units % 128 == 0
            and total_units >= 512
            and (local_width // surge.shape[2]) % 128 == 0
            and surge.shape[2] == 4
        )
        if fits:
            return one_kernel_body(sizes, *args)
        return body(*args)

    return run


def solution(mesh):
    return jax.shard_map(
        chosen_body(mesh),
        mesh=mesh,
        in_specs=(
            P(("rep", "fs"), None, "tp"),
            P(("rep", "fs"), None, "tp"),
            P(("rep", "fs"), None, "tp"),
            P(("rep", "fs"), None, "tp"),
            P(("rep", "fs"), None, "tp"),
            P(("rep", "fs"), None, "tp"),
            P(),
            P("fs", "tp"),
            P("tp"),
            P(),
            P("fs", "tp"),
            P("tp"),
            P("fs", "tp"),
            P("tp"),
            P("fs", "tp"),
            P("tp"),
        ),
        out_specs=P(("rep", "fs"), None, "tp"),
        check_vma=False,
    )
```

```python
import functools

import jax
import jax.numpy as jnp
from jax import lax
from jax.experimental import pallas as pl
from jax.experimental.pallas import tpu as pltpu
from jax.sharding import PartitionSpec as P

BLOCK = 64


epsilon = 1e-06
softness_factor = 16.0
highest = lax.Precision.HIGHEST


def attend_head(q, k, v, logodds, surge, gain):
    tokens, width = q.shape
    blocks = tokens // BLOCK
    mid = BLOCK // 2 - 1
    decay = (
        jnp.minimum(logodds, 0.0) - jnp.log1p(jnp.exp(-jnp.abs(logodds)))
    ) * (1.0 / softness_factor) + surge
    row = lax.broadcasted_iota(jnp.int32, (BLOCK, BLOCK), 0)
    col = lax.broadcasted_iota(jnp.int32, (BLOCK, BLOCK), 1)
    tri = jnp.where(row >= col, 1.0, 0.0).astype(jnp.bfloat16)
    q = q.astype(jnp.float32) * width ** (-0.5)
    k = k.astype(jnp.float32)
    high = decay.astype(jnp.bfloat16)
    low = (decay - high.astype(jnp.float32)).astype(jnp.bfloat16)
    pieces = []
    for n in range(blocks):
        rows = slice(n * BLOCK, (n + 1) * BLOCK)
        running = jnp.dot(tri, high[rows], preferred_element_type=jnp.float32) + jnp.dot(
            tri, low[rows], preferred_element_type=jnp.float32
        )
        before = running - decay[rows]
        center = running[mid : mid + 1]
        end = running[BLOCK - 1 : BLOCK]
        to_center = jnp.exp(center)
        from_center = jnp.exp(end - center)
        q_forward = q[rows] * jnp.exp(running - center)
        k_forward = k[rows] * jnp.exp(center - running)
        q_backward = q[rows] * jnp.exp(center - before)
        k_backward = k[rows] * jnp.exp(before - center)
        half = jnp.bfloat16
        scores = jnp.where(
            row >= col, by_rows(q_forward.astype(half), k_forward.astype(half)), 0.0
        ) + jnp.where(row <= col, by_rows(q_backward.astype(half), k_backward.astype(half)), 0.0)
        inner = jnp.dot(scores.astype(half), v[rows], preferred_element_type=jnp.float32)
        pieces.append(
            (
                inner,
                (q_forward * to_center).astype(half),
                (q_backward * from_center).astype(half),
                by_columns(v[rows], (k_forward * from_center).astype(half)),
                by_columns(v[rows], (k_backward * to_center).astype(half)),
                jnp.exp(end),
            )
        )
    totals = [piece[0] for piece in pieces]
    state = None
    for n in range(blocks):
        if state is not None:
            totals[n] = totals[n] + by_rows(pieces[n][1], state.astype(jnp.bfloat16))
        state = pieces[n][3] if state is None else pieces[n][5] * state + pieces[n][3]
    state = None
    for n in reversed(range(blocks)):
        if state is not None:
            totals[n] = totals[n] + by_rows(pieces[n][2], state.astype(jnp.bfloat16))
        state = pieces[n][4] if state is None else pieces[n][5] * state + pieces[n][4]
    attended = jnp.concatenate(totals, axis=0)
    scale = lax.rsqrt(jnp.mean(attended * attended, axis=-1, keepdims=True) + epsilon)
    return (attended * scale * gain).astype(jnp.bfloat16)


def by_columns(left, right):
    return lax.dot_general(
        left, right, (((0,), (0,)), ((), ())), preferred_element_type=jnp.float32
    )


def attend_kernel(head_total, q_ref, k_ref, v_ref, lo_ref, sg_ref, gain_ref, out_ref):
    width = q_ref.shape[1] // head_total
    value_width = v_ref.shape[1] // head_total
    for h in range(head_total):
        keys = slice(h * width, (h + 1) * width)
        values = slice(h * value_width, (h + 1) * value_width)
        out_ref[:, values] = attend_head(
            q_ref[:, keys],
            k_ref[:, keys],
            v_ref[:, values],
            lo_ref[:, keys],
            sg_ref[:, h : h + 1],
            gain_ref[...],
        )


def linear_attend(queries, key_matrix, value_matrix, decay_logodds, decay_surge, head_norm_gain):
    _, token_length, head_total = decay_surge.shape
    outs = [
        pl.pallas_call(
            functools.partial(attend_kernel, head_total),
            out_shape=jax.ShapeDtypeStruct(value_matrix.shape[1:], jnp.bfloat16),
            in_specs=[pl.BlockSpec(memory_space=pltpu.VMEM)] * 6,
            out_specs=pl.BlockSpec(memory_space=pltpu.VMEM),
            cost_estimate=pl.CostEstimate(
                flops=10**9, bytes_accessed=4 * 10**6, transcendentals=10**6
            ),
        )(
            queries[b], key_matrix[b], value_matrix[b], decay_logodds[b], decay_surge[b],
            head_norm_gain.reshape(1, -1),
        )
        for b in range(queries.shape[0])
    ]
    return jnp.concatenate(outs, axis=0)


def by_rows(left, right):
    return lax.dot_general(
        left, right, (((1,), (1,)), ((), ())), preferred_element_type=jnp.float32
    )


def body(
    residual,
    queries,
    key_matrix,
    value_matrix,
    decay_logodds,
    decay_surge,
    head_norm_gain,
    output_matrix,
    output_column_scale,
    premix_norm_gain,
    gate_matrix,
    gate_column_scale,
    up_matrix,
    up_column_scale,
    down_matrix,
    down_column_scale,
):
    sequence_batch, token_length, local_width = residual.shape
    row_count = sequence_batch * token_length
    normalized_rows = linear_attend(
        queries, key_matrix, value_matrix, decay_logodds, decay_surge, head_norm_gain
    )
    out_half = output_matrix.astype(jnp.bfloat16)
    out_full = lax.all_gather(out_half, "fs", axis=0, tiled=True)
    mix_terms = by_rows(normalized_rows, out_full)
    mix_total = lax.psum_scatter(
        mix_terms.astype(jnp.bfloat16), "tp", scatter_dimension=1, tiled=True
    ).astype(jnp.float32)
    own_rows = residual.reshape(row_count, local_width).astype(jnp.float32)
    updated = (own_rows + output_column_scale * mix_total).astype(jnp.bfloat16)
    features = lax.all_gather(updated, "tp", axis=1, tiled=True)
    wide_rows = features.astype(jnp.float32)
    factor = lax.rsqrt(jnp.mean(wide_rows * wide_rows, axis=-1, keepdims=True) + epsilon)
    normin = (wide_rows * factor * premix_norm_gain).astype(jnp.bfloat16)
    gate_half = gate_matrix.astype(jnp.bfloat16)
    up_half = up_matrix.astype(jnp.bfloat16)
    down_half = down_matrix.astype(jnp.bfloat16)
    gate_full, up_full, down_full = (
        lax.all_gather(gate_half, "fs", axis=0, tiled=True),
        lax.all_gather(up_half, "fs", axis=0, tiled=True),
        lax.all_gather(down_half, "fs", axis=0, tiled=True),
    )
    gate_pre = jnp.dot(normin, gate_full, preferred_element_type=jnp.float32)
    up_pre = jnp.dot(normin, up_full, preferred_element_type=jnp.float32)
    hidden = (jax.nn.silu(gate_pre * gate_column_scale) * (up_pre * up_column_scale)).astype(
        jnp.bfloat16
    )
    down_terms = by_rows(hidden, down_full)
    down_total = lax.psum_scatter(
        down_terms.astype(jnp.bfloat16), "tp", scatter_dimension=1, tiled=True
    ).astype(jnp.float32)
    result = (updated.astype(jnp.float32) + down_column_scale * down_total).astype(jnp.bfloat16)
    return result.reshape(sequence_batch, token_length, local_width)


VMEM_MIB = 60
EXTRA = (1,)
AFTER_HEAD = ((), ((0, 1), (0, 2)), ((0, 3),), ((1, 1), (1, 2)))


def layer_kernel(
    q_hbm, k_hbm, v_hbm, lo_hbm, res_hbm, wo_hbm, gate_hbm, up_hbm, down_hbm,
    sg_hbm, head_gain_hbm, mlp_gain_hbm, os_hbm, gs_hbm, us_hbm, ds_hbm,
    out_ref,
    sg_ref, head_gain_ref, mlp_gain_ref, os_ref, gs_ref, us_ref, ds_ref,
    q_v, k_v, v_v, lo_v, res_v, wo_f32, wo_half, wo_all,
    stage, own_f32, own_half, blocks, extra_stage, extra_blocks, weights,
    normed, gathered, own_res, updated, os_all, gs_all, us_all,
    own_down, other_down, other_updated, to_p, to_p2, to_q, from_p, from_p2, from_q,
    load_sem, send_sem, recv_sem,
):
    r, f, t = lax.axis_index("rep"), lax.axis_index("fs"), lax.axis_index("tp")
    half = jnp.bfloat16
    x, y, c = f + 1 - 2 * lax.rem(f, 2), lax.rem(f + 2, 4), 3 - f
    p, q = x + t * (y - x), y + t * (x - y)
    fs_of = (f, x, y, c)
    partner = (r, f, 1 - t)
    z_one = r + 1 - 2 * lax.rem(r, 2)
    z_two = jnp.where(r < 2, 2, 1)
    z_three = 6 - r - z_one - z_two
    middle = (r == 1) | (r == 2)
    end = jnp.logical_not(middle)
    pair = lax.div(f, 2)
    soon, next_, late = (
        (x + pair * (y - x), 1 + pair), (y + pair * (c - y), 2 + pair),
        (c + pair * (x - c), 3 - 2 * pair),
    )
    mats = (gate_hbm, up_hbm, down_hbm)
    tokens, local_width = res_v.shape
    rows = tokens // 2
    own_width, total_units = wo_f32.shape[0], stage.shape[2]
    units = blocks.shape[3]
    quarter = stage.shape[1]
    width = updated.shape[2]
    heads = sg_ref.shape[0]
    head_width = local_width // heads
    starts = [min(j * units, total_units - units) for j in range(4)]
    SA, SD, SS, SR, SH, SZ, SWO, SC, SE, SF, SO, SX = 0, 3, 4, 7, 11, 14, 17, 18, 19, 22, 25, 27
    A, RES, CP, CQ, CC, CO, WO, SCALE = 0, 9, 10, 14, 15, 16, 17, 18
    EP, EQ, ZN, DN, FP, OUT = 21, 25, 29, 65, 68, 74
    LSTAGE, LRES, LHEAD, LWO, LOWN, LKEPT, LEND, LSMALL, LEXTRA = 0, 3, 4, 12, 13, 16, 19, 21, 28

    def lanes(start, size):
        return pl.ds(pl.multiple_of(start, 128), size)

    def local(source, target, sem):
        return pltpu.make_async_copy(source, target, load_sem.at[sem])

    def send(source, target, sem, slot, device, when=None):
        copy = pltpu.make_async_remote_copy(
            src_ref=source,
            dst_ref=target,
            send_sem=send_sem.at[sem],
            recv_sem=recv_sem.at[slot],
            device_id=device,
            device_id_type=pl.DeviceIdType.MESH,
        )
        if when is None:
            copy.start()
        else:
            pl.when(when)(copy.start)

    def waiter(target, sem, slot):
        return pltpu.make_async_remote_copy(
            src_ref=target,
            dst_ref=target,
            send_sem=send_sem.at[sem],
            recv_sem=recv_sem.at[slot],
            device_id=partner,
            device_id_type=pl.DeviceIdType.MESH,
        )

    def arrive(target, slot):
        waiter(target, 0, slot).wait_recv()

    open_scope = []

    def phase(name):
        if open_scope:
            open_scope.pop().__exit__(None, None, None)
        if name:
            scope = jax.named_scope(name)
            scope.__enter__()
            open_scope.append(scope)

    phase("loads")
    own_start = jnp.minimum(f * units, total_units - units)
    own_spill = f * units - own_start
    own_lanes = lanes(own_start, units)
    my_quarter = pl.ds(pl.multiple_of(r * quarter, quarter), quarter)
    for mm in range(3):
        local(mats[mm].at[my_quarter], stage.at[mm], LSTAGE + mm).start()
    small = (
        (os_hbm, os_ref), (gs_hbm, gs_ref), (us_hbm, us_ref), (sg_hbm, sg_ref),
        (head_gain_hbm, head_gain_ref), (mlp_gain_hbm, mlp_gain_ref), (ds_hbm, ds_ref),
    )
    for n, (source, target) in enumerate(small):
        local(source, target, LSMALL + n).start()
    local(res_hbm, res_v, LRES).start()
    for h in range(heads):
        keys = slice(h * head_width, (h + 1) * head_width)
        local(lo_hbm.at[:, keys], lo_v.at[:, keys], LHEAD + 2 * h).start()
        for a, b in ((q_hbm, q_v), (k_hbm, k_v), (v_hbm, v_v)):
            local(a.at[:, keys], b.at[:, keys], LHEAD + 2 * h + 1).start()
    local(wo_hbm, wo_f32, LWO).start()
    for mm in range(3):
        local(mats[mm].at[:, own_lanes], own_f32.at[mm], LOWN + mm).start()
    far_quarter = pl.ds(pl.multiple_of(z_three * quarter, quarter), quarter)
    extra_loads = [
        local(mats[mm].at[far_quarter], extra_stage.at[n], LEXTRA + n)
        for n, mm in enumerate(EXTRA)
    ]
    for copy in extra_loads:
        pl.when(end)(copy.start)

    phase("greet")
    peers = [partner]
    for other in (x, y, c):
        peers += [(r, other, 0), (r, other, 1)]
    beside = jnp.where(r < 2, r + 1, r - 1)
    away = jnp.where(r < 2, r + 2, r - 2)
    peers += [(beside, f, t), (away, f, t)]
    greet(peers, middle, (jnp.where(r < 2, 0, 3), f, t))

    def weight_rows(matrix, owner, start, size, core):
        return weights.at[
            matrix, pl.ds(owner * own_width + start, size), lanes(core * units, units)
        ]

    def dn(matrix, owner):
        return DN if matrix < 2 else DN + 1 + lax.div(owner, 2)

    def cut_blocks(mm, source, target):
        lane = lax.broadcasted_iota(jnp.int32, (quarter, units), 1)
        for j in range(4):
            cut = source[:, starts[j] : starts[j] + units]
            spill = j * units - starts[j]
            if spill > 0 and mm == 2:
                cut = jnp.where(lane < spill, 0.0, cut)
            target[j] = cut.astype(half)

    phase("cut_send")
    for mm in range(3):
        local(mats[mm].at[my_quarter], stage.at[mm], LSTAGE + mm).wait()
        cut_blocks(mm, stage.at[mm], blocks.at[mm])
        for rel in (1, 2, 3):
            send(
                blocks.at[mm, fs_of[rel]], weight_rows(mm, f, r * quarter, quarter, t),
                SA + rel - 1, A + mm * 3 + rel - 1, (r, fs_of[rel], t),
            )

    for n, (source, target) in enumerate(small):
        local(source, target, LSMALL + n).wait()
    for n, (ref, both) in enumerate(((os_ref, os_all), (gs_ref, gs_all), (us_ref, us_all))):
        both[t] = ref[...].reshape(1, -1)
        send(both.at[t], both.at[t], SS + n, SCALE + n, partner)

    phase("residual")
    local(res_hbm, res_v, LRES).wait()
    mine = jnp.where(lax.div(f, 2) == t, 1, 0)
    first = mine * x + (1 - mine) * c
    other = mine * f + (1 - mine) * y
    target = own_res.at[f]
    first_lanes = lanes((first - 2 * t) * own_width, own_width)
    other_lanes = lanes((other - 2 * t) * own_width, own_width)
    my_rows, other_rows = pl.ds(t * rows, rows), pl.ds((1 - t) * rows, rows)
    for core in range(2):
        send(
            res_v.at[pl.ds(core * rows, rows), first_lanes], target, SR + core, RES,
            (r, first, core),
        )
    send(res_v.at[other_rows, other_lanes], target, SR + 2, RES, (r, other, 1 - t))
    send(res_v.at[my_rows, other_lanes], target, SR + 3, RES, (r, other, t), when=mine == 0)
    kept_res = pltpu.make_async_copy(res_v.at[my_rows, other_lanes], target, recv_sem.at[RES])
    pl.when(mine == 1)(kept_res.start)

    def head_lanes(core, h):
        return lanes((core * heads + h) * head_width, head_width)

    def piece_of(matrix, owner, plane):
        return weight_rows(matrix, owner, plane * quarter, quarter, t)

    def z_slot(matrix, rel, plane):
        return ZN + plane * 9 + matrix * 3 + rel - 1

    def pump(matrix, rel):
        block, slot = piece_of(matrix, fs_of[rel], r), z_slot(matrix, rel, r)
        arrive(block, A + matrix * 3 + rel - 1)
        when = end | (late[1] != rel) if matrix == 2 else None
        send(block, block, SZ, slot, (z_one, f, t), when)
        send(block, block, SZ + 1, slot, (z_two, f, t))
        send(block, block, SD, dn(matrix, fs_of[rel]), partner)

    def pump_late():
        owner, rel = late
        block = piece_of(2, owner, r)
        send(block, block, SZ, z_slot(2, rel, r), (z_one, f, t), middle)

    def pump_z(which, when, todo):
        for matrix, (owner, rel) in todo:
            for source in which:
                plane = (z_one, z_two, z_three)[source]
                block, slot = piece_of(matrix, owner, plane), z_slot(matrix, rel, plane)
                pl.when(when)(waiter(block, 0, slot).wait_recv)
                direct = source == 2 and matrix in EXTRA and rel < 3
                if when is middle and source > 0 and not direct:
                    send(block, block, SZ + 2, slot, (z_one, f, t), when)
                send(block, block, SD, dn(matrix, owner), partner, when)

    gates = [(0, (fs_of[rel], rel)) for rel in (1, 2, 3)]
    ups = [(1, (fs_of[rel], rel)) for rel in (1, 2, 3)]

    surge = jnp.transpose(sg_ref[...])
    for h in range(heads):
        phase("head")
        keys = slice(h * head_width, (h + 1) * head_width)
        local(lo_hbm.at[:, keys], lo_v.at[:, keys], LHEAD + 2 * h).wait()
        wide_keys = slice(0, 3 * head_width)
        local(q_hbm.at[:, wide_keys], q_v.at[:, wide_keys], LHEAD + 2 * h + 1).wait()
        normed[h] = attend_head(
            q_v[:, keys], k_v[:, keys], v_v[:, keys], lo_v[:, keys],
            surge[:, h : h + 1], head_gain_ref[...],
        )
        target = gathered.at[f, :, head_lanes(t, h)]
        for core in range(2):
            for n, to in enumerate((x, y)):
                send(
                    normed.at[h, pl.ds(core * rows, rows)], target, SH + n,
                    CP + h if n == core else CQ, (r, to, core),
                )
        send(normed.at[h, other_rows], target, SH + 2, CO, partner)
        local(normed.at[h, my_rows], target, LKEPT + 1).start()
        phase(f"pump_a#h={h}")
        for n, rel in AFTER_HEAD[h]:
            pump(n, rel)

    phase("wo_own_cast")
    local(wo_hbm, wo_f32, LWO).wait()
    wo_half[...] = jnp.transpose(wo_f32[...].astype(half))
    target = wo_all.at[pl.ds(t * local_width, local_width)]
    send(wo_half, target, SWO, WO, partner)
    local(wo_half, target, LKEPT + 2).start()
    own_lane = lax.broadcasted_iota(jnp.int32, (own_width, units), 1)
    for mm in range(3):
        local(mats[mm].at[:, own_lanes], own_f32.at[mm], LOWN + mm).wait()
        cut = own_f32[mm]
        if mm == 2:
            cut = jnp.where(own_lane < own_spill, 0.0, cut)
        own_half[mm] = cut.astype(half)
        target = weight_rows(mm, f, 0, own_width, t)
        send(own_half.at[mm], target, SD, dn(mm, f), partner)
        local(own_half.at[mm], target, LKEPT).start()

    phase("extras")
    @pl.when(end)
    def _():
        for n, mm in enumerate(EXTRA):
            extra_loads[n].wait()
            cut_blocks(mm, extra_stage.at[n], extra_blocks.at[n])
            for rel in (1, 2):
                send(
                    extra_blocks.at[n, fs_of[rel]], piece_of(mm, f, z_three),
                    SX, z_slot(mm, rel, z_three), (r, fs_of[rel], t),
                )

    phase("pump_a1")
    for n, rel in ((1, 3), (2, 1), (2, 2), (2, 3)):
        pump(n, rel)
    phase("z_gates")
    pump_z((1, 2), middle, gates)

    phase("relay_c")
    for h in range(heads):
        arrive(gathered.at[p, :, lanes(0, 2 * head_width)], CP + h)
        for core in range(2):
            block = gathered.at[p, :, head_lanes(core, h)]
            send(block, block, SC, CC, (r, q, t))
    phase("pump_z0")
    phase("z_ups")
    pump_z((1, 2), middle, ups)
    phase("pump_z0")
    pump_z((0,), end, gates + ups + [(2, soon)])

    phase("wait_small")
    local(own_half, own_half, LKEPT).wait()
    target = gathered.at[f, :, lanes(t * local_width, local_width)]
    local(target, target, LKEPT + 1).wait()
    local(wo_half, wo_half, LKEPT + 2).wait()
    for n, both in enumerate((os_all, gs_all, us_all)):
        arrive(both.at[1 - t], SCALE + n)
    arrive(wo_half, WO)
    arrive(own_res, RES)
    out_scale = os_all[lax.div(f, 2), :, lanes(lax.rem(f, 2) * own_width, own_width)]
    order = (f, p, q, c)

    def feature_lanes(owner):
        return lanes(owner * own_width, own_width)

    def share(k, sem, slot, to):
        block = updated.at[order[k], :, feature_lanes(f)]
        send(block, block, sem, slot, (r, to, t))

    def relay(k):
        block = updated.at[order[k], :, feature_lanes(p)]
        arrive(block, EP + k)
        send(block, block, SE + 2, EQ + (k ^ 2), (r, q, t))

    for k in range(4):
        seq = order[k]
        phase("wait_c")
        if k == 0:
            arrive(gathered.at[f, :, lanes((1 - t) * local_width, local_width)], CO)
        elif k > 1:
            arrive(gathered.at[seq], (CQ, CC)[k - 2])
        phase("outproj")
        mixed = jnp.dot(gathered[seq], wo_all[...], preferred_element_type=jnp.float32)
        updated[seq, :, feature_lanes(f)] = (
            own_res[seq].astype(jnp.float32) + out_scale * mixed
        ).astype(half)
        if k == 2:
            for done in (2, 0, 1):
                share(done, SE, EP + (done ^ 1), p)
            for done in (1, 2):
                share(done, SE + 1, EQ + (done ^ 2), q)
            phase("z_soon")
            pump_z((1, 2), middle, [(2, soon)])
            pump_z((1, 2), end, gates)
        elif k == 3:
            share(3, SE, EP + 2, p)
            relay(1)
            for done in (3, 0):
                share(done, SE + 1, EQ + (done ^ 2), q)

    phase("relay_e")
    relay(3)
    phase("z_downs")
    pump_z((1, 2), middle, [(2, next_), (2, late)])
    pump_late()
    pump_z((0,), middle, gates + ups)
    phase("relay_e")
    relay(0)
    relay(2)
    phase("pump_z2")
    pump_z((1, 2), end, ups)
    pump_z((0,), middle, [(2, soon), (2, next_), (2, late)])
    phase("wait_w")
    arrive(weights.at[pl.ds(0, 2), :, lanes((1 - t) * units, units)], DN)

    gate_scale = jnp.concatenate([gs_all[0, :, own_lanes], gs_all[1, :, own_lanes]], axis=1)
    up_scale = jnp.concatenate([us_all[0, :, own_lanes], us_all[1, :, own_lanes]], axis=1)

    def half_rows(n):
        return pl.ds(pl.multiple_of(n * local_width, local_width), local_width)

    partner_lanes = lanes((1 - t) * units, units)
    hiddens = {}

    def down_terms(k, n):
        term = by_rows(hiddens[k], weights[2, half_rows(n), :])
        if k == 3:
            to_p[n] = term.astype(half)
            send(to_p.at[n], from_p.at[n], SF, FP + n, (r, p, t))
        elif k == 1:
            to_p2[n] = term.astype(half)
            send(to_p2.at[n], from_p2.at[t], SF + 1, FP + 2 + t, (r, p, n))
        elif k == 0:
            own_down[n] = term
        else:
            arrive(from_p.at[n], FP + n)
            to_q[n] = (term + from_p[n].astype(jnp.float32)).astype(half)
            send(to_q.at[n], from_q.at[t], SF + 2, FP + 4 + t, (r, q, n))

    for k in (3, 1, 0, 2):
        seq = order[k]
        phase("wait_e")
        arrive(updated.at[seq, :, lanes(0, 2 * own_width)], EQ + k)
        phase("gate_up")
        wide = updated[seq].astype(jnp.float32)
        factor = lax.rsqrt(jnp.mean(wide * wide, axis=-1, keepdims=True) + epsilon)
        normin = (wide * factor * mlp_gain_ref[...]).astype(half)
        gate_pre = jnp.dot(normin, weights[0], preferred_element_type=jnp.float32) * gate_scale
        up_pre = jnp.dot(normin, weights[1], preferred_element_type=jnp.float32) * up_scale
        hiddens[k] = (jax.nn.silu(gate_pre) * up_pre).astype(half)
        if k == 3:
            phase("z_half")
            pump_z((0,), end, [(2, next_)])
            pump_z((1, 2), end, [(2, soon), (2, next_)])
            phase("wait_half")
            arrive(weights.at[2, half_rows(0), partner_lanes], DN + 1)
        phase("down")
        down_terms(k, 0)
    phase("z_last")
    pump_z((0, 1, 2), end, [(2, late)])
    arrive(weights.at[2, half_rows(1), partner_lanes], DN + 2)
    phase("down_far")
    for k in (3, 1, 0):
        down_terms(k, 1)
    send(own_down.at[1 - t], other_down, SO, OUT, partner)
    other_half = updated.at[f, :, lanes((1 - t) * local_width, local_width)]
    send(other_half, other_updated, SO + 1, OUT + 1, partner)
    phase("down_q")
    down_terms(2, 1)

    phase("wait_other")
    arrive(other_down, OUT)
    arrive(other_updated, OUT + 1)
    phase("wait_p2")
    for core in range(2):
        arrive(from_p2.at[core], FP + 2 + core)
    own_sum = own_down[t] + from_p2[t].astype(jnp.float32)
    other_sum = other_down[...] + from_p2[1 - t].astype(jnp.float32)
    phase("wait_q")
    for core in range(2):
        arrive(from_q.at[core], FP + 4 + core)
    for n, (core, total, rows_in) in enumerate((
        (t, own_sum, updated[f, :, lanes(t * local_width, local_width)]),
        (1 - t, other_sum, other_updated[...]),
    )):
        total = total + from_q[core].astype(jnp.float32)
        target = pl.ds(core * rows, rows)
        q_v[target, :] = (rows_in.astype(jnp.float32) + ds_ref[...] * total).astype(half)
        local(q_v.at[target], out_ref.at[target], LEND + n).start()

    phase("drain")
    for rel in (1, 2, 3):
        waiter(blocks.at[:, 0], SA + rel - 1, 0).wait_send()
    waiter(weights.at[:, :, lanes(t * units, units)], SD, 0).wait_send()
    for n, both in enumerate((os_all, gs_all, us_all)):
        waiter(both.at[t], SS + n, 0).wait_send()
    for n in range(3):
        waiter(own_res.at[0], SR + n, 0).wait_send()
    pl.when(mine == 0)(waiter(own_res.at[0], SR + 3, 0).wait_send)
    for n in range(2):
        waiter(normed, SH + n, 0).wait_send()
    waiter(normed.at[:, pl.ds(0, rows)], SH + 2, 0).wait_send()
    for n in range(2):
        waiter(weights.at[0, pl.ds(0, 9 * quarter), lanes(0, units)], SZ + n, 0).wait_send()
    left = 18 - 2 * len(EXTRA)
    relayed = weights.at[0, pl.ds(0, left * quarter), lanes(0, units)]
    extras = extra_blocks.at[:, pl.ds(0, 2)]
    pl.when(end)(waiter(extras, SX, 0).wait_send)
    pl.when(middle)(waiter(relayed, SZ + 2, 0).wait_send)
    waiter(wo_half, SWO, 0).wait_send()
    waiter(gathered.at[0], SC, 0).wait_send()
    for n in range(3):
        waiter(updated.at[:, :, pl.ds(0, own_width)], SE + n, 0).wait_send()
    for n, sent in enumerate((to_p, to_p2, to_q)):
        waiter(sent, SF + n, 0).wait_send()
    waiter(other_down, SO, 0).wait_send()
    waiter(other_updated, SO + 1, 0).wait_send()
    for n, core in enumerate((t, 1 - t)):
        target = pl.ds(core * rows, rows)
        local(q_v.at[target], out_ref.at[target], LEND + n).wait()
    phase(None)


def one_kernel_body(
    sizes,
    residual,
    queries,
    key_matrix,
    value_matrix,
    decay_logodds,
    decay_surge,
    head_norm_gain,
    output_matrix,
    output_column_scale,
    premix_norm_gain,
    gate_matrix,
    gate_column_scale,
    up_matrix,
    up_column_scale,
    down_matrix,
    down_column_scale,
):
    half, full = jnp.bfloat16, jnp.float32
    _, tokens, local_width = residual.shape
    rows = tokens // 2
    own_width, total_units = gate_matrix.shape
    width = premix_norm_gain.shape[0]
    heads = decay_surge.shape[2]
    units = -(-total_units // (128 * 4)) * 128
    hbm = pl.BlockSpec(memory_space=pl.ANY)
    out = pl.pallas_call(
        layer_kernel,
        out_shape=jax.ShapeDtypeStruct((tokens, local_width), half),
        in_specs=[hbm] * 16,
        out_specs=hbm,
        scratch_shapes=[
            pltpu.VMEM((heads, tokens), full),
            pltpu.VMEM((1, head_norm_gain.shape[0]), full),
            pltpu.VMEM((1, width), full),
            pltpu.VMEM((1, local_width), full),
            pltpu.VMEM((total_units,), full),
            pltpu.VMEM((total_units,), full),
            pltpu.VMEM((1, local_width), full),
            pltpu.VMEM((tokens, local_width), half),
            pltpu.VMEM((tokens, local_width), half),
            pltpu.VMEM((tokens, local_width), half),
            pltpu.VMEM((tokens, local_width), full),
            pltpu.VMEM((tokens, local_width), half),
            pltpu.VMEM((own_width, local_width), full),
            pltpu.VMEM((local_width, own_width), half),
            pltpu.VMEM((width, own_width), half),
            pltpu.VMEM((3, own_width // 4, total_units), full),
            pltpu.VMEM((3, own_width, units), full),
            pltpu.VMEM((3, own_width, units), half),
            pltpu.VMEM((3, 4, own_width // 4, units), half),
            pltpu.VMEM((len(EXTRA), own_width // 4, total_units), full),
            pltpu.VMEM((len(EXTRA), 4, own_width // 4, units), half),
            pltpu.VMEM((3, width, 2 * units), half),
            pltpu.VMEM((heads, tokens, local_width // heads), half),
            pltpu.VMEM((4, rows, width), half),
            pltpu.VMEM((4, rows, own_width), half),
            pltpu.VMEM((4, rows, width), half),
            pltpu.VMEM((2, 1, local_width), full),
            pltpu.VMEM((2, 1, total_units), full),
            pltpu.VMEM((2, 1, total_units), full),
            pltpu.VMEM((2, rows, local_width), full),
            pltpu.VMEM((rows, local_width), full),
            pltpu.VMEM((rows, local_width), half),
        ]
        + [pltpu.VMEM((2, rows, local_width), half)] * 6
        + [
            pltpu.SemaphoreType.DMA((28 + len(EXTRA),)),
            pltpu.SemaphoreType.DMA((28,)),
            pltpu.SemaphoreType.DMA((76,)),
        ],
        compiler_params=pltpu.CompilerParams(
            collective_id=1, has_side_effects=True, vmem_limit_bytes=VMEM_MIB * 2**20
        ),
    )(
        queries[0], key_matrix[0], value_matrix[0], decay_logodds[0], residual[0],
        output_matrix, gate_matrix, up_matrix, down_matrix,
        jnp.transpose(decay_surge[0]), head_norm_gain.reshape(1, -1), premix_norm_gain.reshape(1, -1),
        output_column_scale.reshape(1, -1), gate_column_scale,
        up_column_scale, down_column_scale.reshape(1, -1),
    )
    return out[None]


def greet(devices, more, extra):
    barrier = pltpu.get_barrier_semaphore()

    def signal(device):
        pl.semaphore_signal(
            barrier, inc=1, device_id=device, device_id_type=pl.DeviceIdType.MESH
        )

    for device in devices:
        signal(device)
    pl.when(more)(lambda: signal(extra))
    pl.semaphore_wait(barrier, len(devices) + jnp.where(more, 1, 0))


def chosen_body(mesh):
    sizes = tuple(mesh.shape[name] for name in ("rep", "fs", "tp"))

    def run(*args):
        residual, surge, output_matrix, gate_matrix = args[0], args[5], args[7], args[10]
        sequences, tokens, local_width = residual.shape
        own_width, total_units = gate_matrix.shape
        fits = (
            sizes == (4, 4, 2)
            and sequences == 1
            and tokens % (2 * BLOCK) == 0
            and local_width == 2 * own_width
            and output_matrix.shape == (own_width, local_width)
            and own_width % 128 == 0
            and total_units % 128 == 0
            and total_units >= 512
            and (local_width // surge.shape[2]) % 128 == 0
            and surge.shape[2] == 4
        )
        if fits:
            return one_kernel_body(sizes, *args)
        return body(*args)

    return run


def solution(mesh):
    return jax.shard_map(
        chosen_body(mesh),
        mesh=mesh,
        in_specs=(
            P(("rep", "fs"), None, "tp"),
            P(("rep", "fs"), None, "tp"),
            P(("rep", "fs"), None, "tp"),
            P(("rep", "fs"), None, "tp"),
            P(("rep", "fs"), None, "tp"),
            P(("rep", "fs"), None, "tp"),
            P(),
            P("fs", "tp"),
            P("tp"),
            P(),
            P("fs", "tp"),
            P("tp"),
            P("fs", "tp"),
            P("tp"),
            P("fs", "tp"),
            P("tp"),
        ),
        out_specs=P(("rep", "fs"), None, "tp"),
        check_vma=False,
    )
```

```python
import functools

import jax
import jax.numpy as jnp
from jax import lax
from jax.experimental import pallas as pl
from jax.experimental.pallas import tpu as pltpu
from jax.sharding import PartitionSpec as P

BLOCK = 64


epsilon = 1e-06
softness_factor = 16.0
highest = lax.Precision.HIGHEST


def attend_head(q, k, v, logodds, surge, gain):
    tokens, width = q.shape
    blocks = tokens // BLOCK
    mid = BLOCK // 2 - 1
    decay = (
        jnp.minimum(logodds, 0.0) - jnp.log1p(jnp.exp(-jnp.abs(logodds)))
    ) * (1.0 / softness_factor) + surge
    row = lax.broadcasted_iota(jnp.int32, (BLOCK, BLOCK), 0)
    col = lax.broadcasted_iota(jnp.int32, (BLOCK, BLOCK), 1)
    tri = jnp.where(row >= col, 1.0, 0.0).astype(jnp.bfloat16)
    q = q.astype(jnp.float32) * width ** (-0.5)
    k = k.astype(jnp.float32)
    high = decay.astype(jnp.bfloat16)
    low = (decay - high.astype(jnp.float32)).astype(jnp.bfloat16)
    pieces = []
    for n in range(blocks):
        rows = slice(n * BLOCK, (n + 1) * BLOCK)
        running = jnp.dot(tri, high[rows], preferred_element_type=jnp.float32) + jnp.dot(
            tri, low[rows], preferred_element_type=jnp.float32
        )
        before = running - decay[rows]
        center = running[mid : mid + 1]
        end = running[BLOCK - 1 : BLOCK]
        to_center = jnp.exp(center)
        from_center = jnp.exp(end - center)
        q_forward = q[rows] * jnp.exp(running - center)
        k_forward = k[rows] * jnp.exp(center - running)
        q_backward = q[rows] * jnp.exp(center - before)
        k_backward = k[rows] * jnp.exp(before - center)
        half = jnp.bfloat16
        scores = jnp.where(
            row >= col, by_rows(q_forward.astype(half), k_forward.astype(half)), 0.0
        ) + jnp.where(row <= col, by_rows(q_backward.astype(half), k_backward.astype(half)), 0.0)
        inner = jnp.dot(scores.astype(half), v[rows], preferred_element_type=jnp.float32)
        pieces.append(
            (
                inner,
                (q_forward * to_center).astype(half),
                (q_backward * from_center).astype(half),
                by_columns(v[rows], (k_forward * from_center).astype(half)),
                by_columns(v[rows], (k_backward * to_center).astype(half)),
                jnp.exp(end),
            )
        )
    totals = [piece[0] for piece in pieces]
    state = None
    for n in range(blocks):
        if state is not None:
            totals[n] = totals[n] + by_rows(pieces[n][1], state.astype(jnp.bfloat16))
        state = pieces[n][3] if state is None else pieces[n][5] * state + pieces[n][3]
    state = None
    for n in reversed(range(blocks)):
        if state is not None:
            totals[n] = totals[n] + by_rows(pieces[n][2], state.astype(jnp.bfloat16))
        state = pieces[n][4] if state is None else pieces[n][5] * state + pieces[n][4]
    attended = jnp.concatenate(totals, axis=0)
    scale = lax.rsqrt(jnp.mean(attended * attended, axis=-1, keepdims=True) + epsilon)
    return (attended * scale * gain).astype(jnp.bfloat16)


def by_columns(left, right):
    return lax.dot_general(
        left, right, (((0,), (0,)), ((), ())), preferred_element_type=jnp.float32
    )


def attend_kernel(head_total, q_ref, k_ref, v_ref, lo_ref, sg_ref, gain_ref, out_ref):
    width = q_ref.shape[1] // head_total
    value_width = v_ref.shape[1] // head_total
    for h in range(head_total):
        keys = slice(h * width, (h + 1) * width)
        values = slice(h * value_width, (h + 1) * value_width)
        out_ref[:, values] = attend_head(
            q_ref[:, keys],
            k_ref[:, keys],
            v_ref[:, values],
            lo_ref[:, keys],
            sg_ref[:, h : h + 1],
            gain_ref[...],
        )


def linear_attend(queries, key_matrix, value_matrix, decay_logodds, decay_surge, head_norm_gain):
    _, token_length, head_total = decay_surge.shape
    outs = [
        pl.pallas_call(
            functools.partial(attend_kernel, head_total),
            out_shape=jax.ShapeDtypeStruct(value_matrix.shape[1:], jnp.bfloat16),
            in_specs=[pl.BlockSpec(memory_space=pltpu.VMEM)] * 6,
            out_specs=pl.BlockSpec(memory_space=pltpu.VMEM),
            cost_estimate=pl.CostEstimate(
                flops=10**9, bytes_accessed=4 * 10**6, transcendentals=10**6
            ),
        )(
            queries[b], key_matrix[b], value_matrix[b], decay_logodds[b], decay_surge[b],
            head_norm_gain.reshape(1, -1),
        )
        for b in range(queries.shape[0])
    ]
    return jnp.concatenate(outs, axis=0)


def by_rows(left, right):
    return lax.dot_general(
        left, right, (((1,), (1,)), ((), ())), preferred_element_type=jnp.float32
    )


def body(
    residual,
    queries,
    key_matrix,
    value_matrix,
    decay_logodds,
    decay_surge,
    head_norm_gain,
    output_matrix,
    output_column_scale,
    premix_norm_gain,
    gate_matrix,
    gate_column_scale,
    up_matrix,
    up_column_scale,
    down_matrix,
    down_column_scale,
):
    sequence_batch, token_length, local_width = residual.shape
    row_count = sequence_batch * token_length
    normalized_rows = linear_attend(
        queries, key_matrix, value_matrix, decay_logodds, decay_surge, head_norm_gain
    )
    out_half = output_matrix.astype(jnp.bfloat16)
    out_full = lax.all_gather(out_half, "fs", axis=0, tiled=True)
    mix_terms = by_rows(normalized_rows, out_full)
    mix_total = lax.psum_scatter(
        mix_terms.astype(jnp.bfloat16), "tp", scatter_dimension=1, tiled=True
    ).astype(jnp.float32)
    own_rows = residual.reshape(row_count, local_width).astype(jnp.float32)
    updated = (own_rows + output_column_scale * mix_total).astype(jnp.bfloat16)
    features = lax.all_gather(updated, "tp", axis=1, tiled=True)
    wide_rows = features.astype(jnp.float32)
    factor = lax.rsqrt(jnp.mean(wide_rows * wide_rows, axis=-1, keepdims=True) + epsilon)
    normin = (wide_rows * factor * premix_norm_gain).astype(jnp.bfloat16)
    gate_half = gate_matrix.astype(jnp.bfloat16)
    up_half = up_matrix.astype(jnp.bfloat16)
    down_half = down_matrix.astype(jnp.bfloat16)
    gate_full, up_full, down_full = (
        lax.all_gather(gate_half, "fs", axis=0, tiled=True),
        lax.all_gather(up_half, "fs", axis=0, tiled=True),
        lax.all_gather(down_half, "fs", axis=0, tiled=True),
    )
    gate_pre = jnp.dot(normin, gate_full, preferred_element_type=jnp.float32)
    up_pre = jnp.dot(normin, up_full, preferred_element_type=jnp.float32)
    hidden = (jax.nn.silu(gate_pre * gate_column_scale) * (up_pre * up_column_scale)).astype(
        jnp.bfloat16
    )
    down_terms = by_rows(hidden, down_full)
    down_total = lax.psum_scatter(
        down_terms.astype(jnp.bfloat16), "tp", scatter_dimension=1, tiled=True
    ).astype(jnp.float32)
    result = (updated.astype(jnp.float32) + down_column_scale * down_total).astype(jnp.bfloat16)
    return result.reshape(sequence_batch, token_length, local_width)


VMEM_MIB = 60
EXTRA = (1,)
AFTER_HEAD = ((), ((0, 1), (0, 2)), ((0, 3),), ((1, 1), (1, 2)))


def layer_kernel(
    q_hbm, k_hbm, v_hbm, lo_hbm, res_hbm, wo_hbm, gate_hbm, up_hbm, down_hbm,
    sg_hbm, head_gain_hbm, mlp_gain_hbm, os_hbm, gs_hbm, us_hbm, ds_hbm,
    out_ref,
    sg_ref, head_gain_ref, mlp_gain_ref, os_ref, gs_ref, us_ref, ds_ref,
    q_v, k_v, v_v, lo_v, res_v, wo_f32, wo_half, wo_all,
    stage, own_f32, own_half, blocks, extra_stage, extra_blocks, weights,
    normed, gathered, own_res, updated, os_all, gs_all, us_all,
    own_down, other_down, other_updated, to_p, to_p2, to_q, from_p, from_p2, from_q,
    load_sem, send_sem, recv_sem,
):
    r, f, t = lax.axis_index("rep"), lax.axis_index("fs"), lax.axis_index("tp")
    half = jnp.bfloat16
    x, y, c = f + 1 - 2 * lax.rem(f, 2), lax.rem(f + 2, 4), 3 - f
    p, q = x + t * (y - x), y + t * (x - y)
    fs_of = (f, x, y, c)
    partner = (r, f, 1 - t)
    z_one = r + 1 - 2 * lax.rem(r, 2)
    z_two = jnp.where(r < 2, 2, 1)
    z_three = 6 - r - z_one - z_two
    middle = (r == 1) | (r == 2)
    end = jnp.logical_not(middle)
    pair = lax.div(f, 2)
    soon, next_, late = (
        (x + pair * (y - x), 1 + pair), (y + pair * (c - y), 2 + pair),
        (c + pair * (x - c), 3 - 2 * pair),
    )
    mats = (gate_hbm, up_hbm, down_hbm)
    tokens, local_width = res_v.shape
    rows = tokens // 2
    own_width, total_units = wo_f32.shape[0], stage.shape[2]
    units = blocks.shape[3]
    quarter = stage.shape[1]
    width = updated.shape[2]
    heads = sg_ref.shape[0]
    head_width = local_width // heads
    starts = [min(j * units, total_units - units) for j in range(4)]
    SA, SD, SS, SR, SH, SZ, SWO, SC, SE, SF, SO, SX = 0, 3, 4, 7, 11, 14, 17, 18, 19, 22, 25, 27
    A, RES, CP, CQ, CC, CO, WO, SCALE = 0, 9, 10, 14, 15, 16, 17, 18
    EP, EQ, ZN, DN, FP, OUT = 21, 25, 29, 65, 68, 74
    LSTAGE, LRES, LHEAD, LWO, LOWN, LKEPT, LEND, LSMALL, LEXTRA = 0, 3, 4, 12, 13, 16, 19, 21, 28

    def lanes(start, size):
        return pl.ds(pl.multiple_of(start, 128), size)

    def local(source, target, sem):
        return pltpu.make_async_copy(source, target, load_sem.at[sem])

    def send(source, target, sem, slot, device, when=None):
        copy = pltpu.make_async_remote_copy(
            src_ref=source,
            dst_ref=target,
            send_sem=send_sem.at[sem],
            recv_sem=recv_sem.at[slot],
            device_id=device,
            device_id_type=pl.DeviceIdType.MESH,
        )
        if when is None:
            copy.start()
        else:
            pl.when(when)(copy.start)

    def waiter(target, sem, slot):
        return pltpu.make_async_remote_copy(
            src_ref=target,
            dst_ref=target,
            send_sem=send_sem.at[sem],
            recv_sem=recv_sem.at[slot],
            device_id=partner,
            device_id_type=pl.DeviceIdType.MESH,
        )

    def arrive(target, slot):
        waiter(target, 0, slot).wait_recv()

    open_scope = []

    def phase(name):
        if open_scope:
            open_scope.pop().__exit__(None, None, None)
        if name:
            scope = jax.named_scope(name)
            scope.__enter__()
            open_scope.append(scope)

    phase("loads")
    own_start = jnp.minimum(f * units, total_units - units)
    own_spill = f * units - own_start
    own_lanes = lanes(own_start, units)
    my_quarter = pl.ds(pl.multiple_of(r * quarter, quarter), quarter)
    for mm in range(3):
        local(mats[mm].at[my_quarter], stage.at[mm], LSTAGE + mm).start()
    small = (
        (os_hbm, os_ref), (gs_hbm, gs_ref), (us_hbm, us_ref), (sg_hbm, sg_ref),
        (head_gain_hbm, head_gain_ref), (mlp_gain_hbm, mlp_gain_ref), (ds_hbm, ds_ref),
    )
    for n, (source, target) in enumerate(small):
        local(source, target, LSMALL + n).start()
    local(res_hbm, res_v, LRES).start()
    for h in range(heads):
        keys = slice(h * head_width, (h + 1) * head_width)
        local(lo_hbm.at[:, keys], lo_v.at[:, keys], LHEAD + 2 * h).start()
        for a, b in ((q_hbm, q_v), (k_hbm, k_v), (v_hbm, v_v)):
            local(a.at[:, keys], b.at[:, keys], LHEAD + 2 * h + 1).start()
    local(wo_hbm, wo_f32, LWO).start()
    for mm in range(3):
        local(mats[mm].at[:, own_lanes], own_f32.at[mm], LOWN + mm).start()
    far_quarter = pl.ds(pl.multiple_of(z_three * quarter, quarter), quarter)
    extra_loads = [
        local(mats[mm].at[far_quarter], extra_stage.at[n], LEXTRA + n)
        for n, mm in enumerate(EXTRA)
    ]
    for copy in extra_loads:
        pl.when(end)(copy.start)

    phase("greet")
    peers = [partner]
    for other in (x, y, c):
        peers += [(r, other, 0), (r, other, 1)]
    beside = jnp.where(r < 2, r + 1, r - 1)
    away = jnp.where(r < 2, r + 2, r - 2)
    peers += [(beside, f, t), (away, f, t)]
    greet(peers, middle, (jnp.where(r < 2, 0, 3), f, t))

    def weight_rows(matrix, owner, start, size, core):
        return weights.at[
            matrix, pl.ds(owner * own_width + start, size), lanes(core * units, units)
        ]

    def dn(matrix, owner):
        return DN if matrix < 2 else DN + 1 + lax.div(owner, 2)

    def cut_blocks(mm, source, target):
        lane = lax.broadcasted_iota(jnp.int32, (quarter, units), 1)
        for j in range(4):
            cut = source[:, starts[j] : starts[j] + units]
            spill = j * units - starts[j]
            if spill > 0 and mm == 2:
                cut = jnp.where(lane < spill, 0.0, cut)
            target[j] = cut.astype(half)

    phase("cut_send")
    for mm in range(3):
        local(mats[mm].at[my_quarter], stage.at[mm], LSTAGE + mm).wait()
        cut_blocks(mm, stage.at[mm], blocks.at[mm])
        for rel in (1, 2, 3):
            send(
                blocks.at[mm, fs_of[rel]], weight_rows(mm, f, r * quarter, quarter, t),
                SA + rel - 1, A + mm * 3 + rel - 1, (r, fs_of[rel], t),
            )

    for n, (source, target) in enumerate(small):
        local(source, target, LSMALL + n).wait()
    for n, (ref, both) in enumerate(((os_ref, os_all), (gs_ref, gs_all), (us_ref, us_all))):
        both[t] = ref[...].reshape(1, -1)
        send(both.at[t], both.at[t], SS + n, SCALE + n, partner)

    phase("residual")
    local(res_hbm, res_v, LRES).wait()
    mine = jnp.where(lax.div(f, 2) == t, 1, 0)
    first = mine * x + (1 - mine) * c
    other = mine * f + (1 - mine) * y
    target = own_res.at[f]
    first_lanes = lanes((first - 2 * t) * own_width, own_width)
    other_lanes = lanes((other - 2 * t) * own_width, own_width)
    my_rows, other_rows = pl.ds(t * rows, rows), pl.ds((1 - t) * rows, rows)
    for core in range(2):
        send(
            res_v.at[pl.ds(core * rows, rows), first_lanes], target, SR + core, RES,
            (r, first, core),
        )
    send(res_v.at[other_rows, other_lanes], target, SR + 2, RES, (r, other, 1 - t))
    send(res_v.at[my_rows, other_lanes], target, SR + 3, RES, (r, other, t), when=mine == 0)
    kept_res = pltpu.make_async_copy(res_v.at[my_rows, other_lanes], target, recv_sem.at[RES])
    pl.when(mine == 1)(kept_res.start)

    def head_lanes(core, h):
        return lanes((core * heads + h) * head_width, head_width)

    def piece_of(matrix, owner, plane):
        return weight_rows(matrix, owner, plane * quarter, quarter, t)

    def z_slot(matrix, rel, plane):
        return ZN + plane * 9 + matrix * 3 + rel - 1

    def pump(matrix, rel):
        block, slot = piece_of(matrix, fs_of[rel], r), z_slot(matrix, rel, r)
        arrive(block, A + matrix * 3 + rel - 1)
        when = end | (late[1] != rel) if matrix == 2 else None
        send(block, block, SZ, slot, (z_one, f, t), when)
        send(block, block, SZ + 1, slot, (z_two, f, t))
        send(block, block, SD, dn(matrix, fs_of[rel]), partner)

    def pump_late():
        owner, rel = late
        block = piece_of(2, owner, r)
        send(block, block, SZ, z_slot(2, rel, r), (z_one, f, t), middle)

    def pump_z(which, when, todo):
        for matrix, (owner, rel) in todo:
            for source in which:
                plane = (z_one, z_two, z_three)[source]
                block, slot = piece_of(matrix, owner, plane), z_slot(matrix, rel, plane)
                pl.when(when)(waiter(block, 0, slot).wait_recv)
                direct = source == 2 and matrix in EXTRA and rel < 3
                if when is middle and source > 0 and not direct:
                    send(block, block, SZ + 2, slot, (z_one, f, t), when)
                send(block, block, SD, dn(matrix, owner), partner, when)

    gates = [(0, (fs_of[rel], rel)) for rel in (1, 2, 3)]
    ups = [(1, (fs_of[rel], rel)) for rel in (1, 2, 3)]

    surge = jnp.transpose(sg_ref[...])
    for h in range(heads):
        phase("head")
        keys = slice(h * head_width, (h + 1) * head_width)
        local(lo_hbm.at[:, keys], lo_v.at[:, keys], LHEAD + 2 * h).wait()
        wide_keys = slice(0, 3 * head_width)
        local(q_hbm.at[:, wide_keys], q_v.at[:, wide_keys], LHEAD + 2 * h + 1).wait()
        normed[h] = attend_head(
            q_v[:, keys], k_v[:, keys], v_v[:, keys], lo_v[:, keys],
            surge[:, h : h + 1], head_gain_ref[...],
        )
        target = gathered.at[f, :, head_lanes(t, h)]
        for core in range(2):
            for n, to in enumerate((x, y)):
                send(
                    normed.at[h, pl.ds(core * rows, rows)], target, SH + n,
                    CP + h if n == core else CQ, (r, to, core),
                )
        send(normed.at[h, other_rows], target, SH + 2, CO, partner)
        local(normed.at[h, my_rows], target, LKEPT + 1).start()
        phase(f"pump_a#h={h}")
        for n, rel in AFTER_HEAD[h]:
            pump(n, rel)

    phase("wo_own_cast")
    local(wo_hbm, wo_f32, LWO).wait()
    wo_half[...] = jnp.transpose(wo_f32[...].astype(half))
    target = wo_all.at[pl.ds(t * local_width, local_width)]
    send(wo_half, target, SWO, WO, partner)
    local(wo_half, target, LKEPT + 2).start()
    own_lane = lax.broadcasted_iota(jnp.int32, (own_width, units), 1)
    for mm in range(3):
        local(mats[mm].at[:, own_lanes], own_f32.at[mm], LOWN + mm).wait()
        cut = own_f32[mm]
        if mm == 2:
            cut = jnp.where(own_lane < own_spill, 0.0, cut)
        own_half[mm] = cut.astype(half)
        target = weight_rows(mm, f, 0, own_width, t)
        send(own_half.at[mm], target, SD, dn(mm, f), partner)
        local(own_half.at[mm], target, LKEPT).start()

    phase("extras")
    @pl.when(end)
    def _():
        for n, mm in enumerate(EXTRA):
            extra_loads[n].wait()
            cut_blocks(mm, extra_stage.at[n], extra_blocks.at[n])
            for rel in (1, 2):
                send(
                    extra_blocks.at[n, fs_of[rel]], piece_of(mm, f, z_three),
                    SX, z_slot(mm, rel, z_three), (r, fs_of[rel], t),
                )

    phase("pump_a1")
    for n, rel in ((1, 3), (2, 1), (2, 2), (2, 3)):
        pump(n, rel)
    phase("z_gates")
    pump_z((1, 2), middle, gates)

    phase("relay_c")
    for h in range(heads):
        arrive(gathered.at[p, :, lanes(0, 2 * head_width)], CP + h)
        for core in range(2):
            block = gathered.at[p, :, head_lanes(core, h)]
            send(block, block, SC, CC, (r, q, t))
    phase("pump_z0")
    phase("z_ups")
    pump_z((1, 2), middle, ups)
    phase("pump_z0")
    pump_z((0,), end, gates + ups + [(2, soon)])

    phase("wait_small")
    local(own_half, own_half, LKEPT).wait()
    target = gathered.at[f, :, lanes(t * local_width, local_width)]
    local(target, target, LKEPT + 1).wait()
    local(wo_half, wo_half, LKEPT + 2).wait()
    for n, both in enumerate((os_all, gs_all, us_all)):
        arrive(both.at[1 - t], SCALE + n)
    arrive(wo_half, WO)
    arrive(own_res, RES)
    out_scale = os_all[lax.div(f, 2), :, lanes(lax.rem(f, 2) * own_width, own_width)]
    order = (f, p, q, c)

    def feature_lanes(owner):
        return lanes(owner * own_width, own_width)

    def share(k, sem, slot, to):
        block = updated.at[order[k], :, feature_lanes(f)]
        send(block, block, sem, slot, (r, to, t))

    def relay(k):
        block = updated.at[order[k], :, feature_lanes(p)]
        arrive(block, EP + k)
        send(block, block, SE + 2, EQ + (k ^ 2), (r, q, t))

    for k in range(4):
        seq = order[k]
        phase("wait_c")
        if k == 0:
            arrive(gathered.at[f, :, lanes((1 - t) * local_width, local_width)], CO)
        elif k > 1:
            arrive(gathered.at[seq], (CQ, CC)[k - 2])
        phase("outproj")
        mixed = jnp.dot(gathered[seq], wo_all[...], preferred_element_type=jnp.float32)
        updated[seq, :, feature_lanes(f)] = (
            own_res[seq].astype(jnp.float32) + out_scale * mixed
        ).astype(half)
        if k == 2:
            for done in (2, 0, 1):
                share(done, SE, EP + (done ^ 1), p)
            for done in (1, 2):
                share(done, SE + 1, EQ + (done ^ 2), q)
            phase("z_soon")
            pump_z((1, 2), middle, [(2, soon)])
            pump_z((1, 2), end, gates)
        elif k == 3:
            share(3, SE, EP + 2, p)
            relay(1)
            for done in (3, 0):
                share(done, SE + 1, EQ + (done ^ 2), q)

    phase("relay_e")
    relay(3)
    phase("z_downs")
    pump_z((1, 2), middle, [(2, next_), (2, late)])
    pump_late()
    pump_z((0,), middle, gates + ups)
    phase("relay_e")
    relay(0)
    relay(2)
    phase("pump_z2")
    pump_z((1, 2), end, ups)
    pump_z((0,), middle, [(2, soon), (2, next_), (2, late)])
    phase("wait_w")
    arrive(weights.at[pl.ds(0, 2), :, lanes((1 - t) * units, units)], DN)

    gate_scale = jnp.concatenate([gs_all[0, :, own_lanes], gs_all[1, :, own_lanes]], axis=1)
    up_scale = jnp.concatenate([us_all[0, :, own_lanes], us_all[1, :, own_lanes]], axis=1)

    def half_rows(n):
        return pl.ds(pl.multiple_of(n * local_width, local_width), local_width)

    partner_lanes = lanes((1 - t) * units, units)
    hiddens = {}

    def down_terms(k, n):
        term = by_rows(hiddens[k], weights[2, half_rows(n), :])
        if k == 3:
            to_p[n] = term.astype(half)
            send(to_p.at[n], from_p.at[n], SF, FP + n, (r, p, t))
        elif k == 1:
            to_p2[n] = term.astype(half)
            send(to_p2.at[n], from_p2.at[t], SF + 1, FP + 2 + t, (r, p, n))
        elif k == 0:
            own_down[n] = term
        else:
            arrive(from_p.at[n], FP + n)
            to_q[n] = (term + from_p[n].astype(jnp.float32)).astype(half)
            send(to_q.at[n], from_q.at[t], SF + 2, FP + 4 + t, (r, q, n))

    for k in (3, 1, 0, 2):
        seq = order[k]
        phase("wait_e")
        arrive(updated.at[seq, :, lanes(0, 2 * own_width)], EQ + k)
        phase("gate_up")
        wide = updated[seq].astype(jnp.float32)
        factor = lax.rsqrt(jnp.mean(wide * wide, axis=-1, keepdims=True) + epsilon)
        normin = (wide * factor * mlp_gain_ref[...]).astype(half)
        gate_pre = jnp.dot(normin, weights[0], preferred_element_type=jnp.float32) * gate_scale
        up_pre = jnp.dot(normin, weights[1], preferred_element_type=jnp.float32) * up_scale
        hiddens[k] = (jax.nn.silu(gate_pre) * up_pre).astype(half)
        if k == 3:
            phase("z_half")
            pump_z((0,), end, [(2, next_)])
            pump_z((1, 2), end, [(2, soon), (2, next_)])
            phase("wait_half")
            arrive(weights.at[2, half_rows(0), partner_lanes], DN + 1)
        phase("down")
        down_terms(k, 0)
        if k == 0:
            pump_z((1, 2), end, [(2, late)])
    phase("z_last")
    pump_z((0,), end, [(2, late)])
    arrive(weights.at[2, half_rows(1), partner_lanes], DN + 2)
    phase("down_far")
    for k in (3, 1, 0):
        down_terms(k, 1)
    send(own_down.at[1 - t], other_down, SO, OUT, partner)
    other_half = updated.at[f, :, lanes((1 - t) * local_width, local_width)]
    send(other_half, other_updated, SO + 1, OUT + 1, partner)
    phase("down_q")
    down_terms(2, 1)

    phase("wait_other")
    arrive(other_down, OUT)
    arrive(other_updated, OUT + 1)
    phase("wait_p2")
    for core in range(2):
        arrive(from_p2.at[core], FP + 2 + core)
    own_sum = own_down[t] + from_p2[t].astype(jnp.float32)
    other_sum = other_down[...] + from_p2[1 - t].astype(jnp.float32)
    phase("wait_q")
    for core in range(2):
        arrive(from_q.at[core], FP + 4 + core)
    for n, (core, total, rows_in) in enumerate((
        (t, own_sum, updated[f, :, lanes(t * local_width, local_width)]),
        (1 - t, other_sum, other_updated[...]),
    )):
        total = total + from_q[core].astype(jnp.float32)
        target = pl.ds(core * rows, rows)
        q_v[target, :] = (rows_in.astype(jnp.float32) + ds_ref[...] * total).astype(half)
        local(q_v.at[target], out_ref.at[target], LEND + n).start()

    phase("drain")
    for rel in (1, 2, 3):
        waiter(blocks.at[:, 0], SA + rel - 1, 0).wait_send()
    waiter(weights.at[:, :, lanes(t * units, units)], SD, 0).wait_send()
    for n, both in enumerate((os_all, gs_all, us_all)):
        waiter(both.at[t], SS + n, 0).wait_send()
    for n in range(3):
        waiter(own_res.at[0], SR + n, 0).wait_send()
    pl.when(mine == 0)(waiter(own_res.at[0], SR + 3, 0).wait_send)
    for n in range(2):
        waiter(normed, SH + n, 0).wait_send()
    waiter(normed.at[:, pl.ds(0, rows)], SH + 2, 0).wait_send()
    for n in range(2):
        waiter(weights.at[0, pl.ds(0, 9 * quarter), lanes(0, units)], SZ + n, 0).wait_send()
    left = 18 - 2 * len(EXTRA)
    relayed = weights.at[0, pl.ds(0, left * quarter), lanes(0, units)]
    extras = extra_blocks.at[:, pl.ds(0, 2)]
    pl.when(end)(waiter(extras, SX, 0).wait_send)
    pl.when(middle)(waiter(relayed, SZ + 2, 0).wait_send)
    waiter(wo_half, SWO, 0).wait_send()
    waiter(gathered.at[0], SC, 0).wait_send()
    for n in range(3):
        waiter(updated.at[:, :, pl.ds(0, own_width)], SE + n, 0).wait_send()
    for n, sent in enumerate((to_p, to_p2, to_q)):
        waiter(sent, SF + n, 0).wait_send()
    waiter(other_down, SO, 0).wait_send()
    waiter(other_updated, SO + 1, 0).wait_send()
    for n, core in enumerate((t, 1 - t)):
        target = pl.ds(core * rows, rows)
        local(q_v.at[target], out_ref.at[target], LEND + n).wait()
    phase(None)


def one_kernel_body(
    sizes,
    residual,
    queries,
    key_matrix,
    value_matrix,
    decay_logodds,
    decay_surge,
    head_norm_gain,
    output_matrix,
    output_column_scale,
    premix_norm_gain,
    gate_matrix,
    gate_column_scale,
    up_matrix,
    up_column_scale,
    down_matrix,
    down_column_scale,
):
    half, full = jnp.bfloat16, jnp.float32
    _, tokens, local_width = residual.shape
    rows = tokens // 2
    own_width, total_units = gate_matrix.shape
    width = premix_norm_gain.shape[0]
    heads = decay_surge.shape[2]
    units = -(-total_units // (128 * 4)) * 128
    hbm = pl.BlockSpec(memory_space=pl.ANY)
    out = pl.pallas_call(
        layer_kernel,
        out_shape=jax.ShapeDtypeStruct((tokens, local_width), half),
        in_specs=[hbm] * 16,
        out_specs=hbm,
        scratch_shapes=[
            pltpu.VMEM((heads, tokens), full),
            pltpu.VMEM((1, head_norm_gain.shape[0]), full),
            pltpu.VMEM((1, width), full),
            pltpu.VMEM((1, local_width), full),
            pltpu.VMEM((total_units,), full),
            pltpu.VMEM((total_units,), full),
            pltpu.VMEM((1, local_width), full),
            pltpu.VMEM((tokens, local_width), half),
            pltpu.VMEM((tokens, local_width), half),
            pltpu.VMEM((tokens, local_width), half),
            pltpu.VMEM((tokens, local_width), full),
            pltpu.VMEM((tokens, local_width), half),
            pltpu.VMEM((own_width, local_width), full),
            pltpu.VMEM((local_width, own_width), half),
            pltpu.VMEM((width, own_width), half),
            pltpu.VMEM((3, own_width // 4, total_units), full),
            pltpu.VMEM((3, own_width, units), full),
            pltpu.VMEM((3, own_width, units), half),
            pltpu.VMEM((3, 4, own_width // 4, units), half),
            pltpu.VMEM((len(EXTRA), own_width // 4, total_units), full),
            pltpu.VMEM((len(EXTRA), 4, own_width // 4, units), half),
            pltpu.VMEM((3, width, 2 * units), half),
            pltpu.VMEM((heads, tokens, local_width // heads), half),
            pltpu.VMEM((4, rows, width), half),
            pltpu.VMEM((4, rows, own_width), half),
            pltpu.VMEM((4, rows, width), half),
            pltpu.VMEM((2, 1, local_width), full),
            pltpu.VMEM((2, 1, total_units), full),
            pltpu.VMEM((2, 1, total_units), full),
            pltpu.VMEM((2, rows, local_width), full),
            pltpu.VMEM((rows, local_width), full),
            pltpu.VMEM((rows, local_width), half),
        ]
        + [pltpu.VMEM((2, rows, local_width), half)] * 6
        + [
            pltpu.SemaphoreType.DMA((28 + len(EXTRA),)),
            pltpu.SemaphoreType.DMA((28,)),
            pltpu.SemaphoreType.DMA((76,)),
        ],
        compiler_params=pltpu.CompilerParams(
            collective_id=1, has_side_effects=True, vmem_limit_bytes=VMEM_MIB * 2**20
        ),
    )(
        queries[0], key_matrix[0], value_matrix[0], decay_logodds[0], residual[0],
        output_matrix, gate_matrix, up_matrix, down_matrix,
        jnp.transpose(decay_surge[0]), head_norm_gain.reshape(1, -1), premix_norm_gain.reshape(1, -1),
        output_column_scale.reshape(1, -1), gate_column_scale,
        up_column_scale, down_column_scale.reshape(1, -1),
    )
    return out[None]


def greet(devices, more, extra):
    barrier = pltpu.get_barrier_semaphore()

    def signal(device):
        pl.semaphore_signal(
            barrier, inc=1, device_id=device, device_id_type=pl.DeviceIdType.MESH
        )

    for device in devices:
        signal(device)
    pl.when(more)(lambda: signal(extra))
    pl.semaphore_wait(barrier, len(devices) + jnp.where(more, 1, 0))


def chosen_body(mesh):
    sizes = tuple(mesh.shape[name] for name in ("rep", "fs", "tp"))

    def run(*args):
        residual, surge, output_matrix, gate_matrix = args[0], args[5], args[7], args[10]
        sequences, tokens, local_width = residual.shape
        own_width, total_units = gate_matrix.shape
        fits = (
            sizes == (4, 4, 2)
            and sequences == 1
            and tokens % (2 * BLOCK) == 0
            and local_width == 2 * own_width
            and output_matrix.shape == (own_width, local_width)
            and own_width % 128 == 0
            and total_units % 128 == 0
            and total_units >= 512
            and (local_width // surge.shape[2]) % 128 == 0
            and surge.shape[2] == 4
        )
        if fits:
            return one_kernel_body(sizes, *args)
        return body(*args)

    return run


def solution(mesh):
    return jax.shard_map(
        chosen_body(mesh),
        mesh=mesh,
        in_specs=(
            P(("rep", "fs"), None, "tp"),
            P(("rep", "fs"), None, "tp"),
            P(("rep", "fs"), None, "tp"),
            P(("rep", "fs"), None, "tp"),
            P(("rep", "fs"), None, "tp"),
            P(("rep", "fs"), None, "tp"),
            P(),
            P("fs", "tp"),
            P("tp"),
            P(),
            P("fs", "tp"),
            P("tp"),
            P("fs", "tp"),
            P("tp"),
            P("fs", "tp"),
            P("tp"),
        ),
        out_specs=P(("rep", "fs"), None, "tp"),
        check_vma=False,
    )
```
